256 devices in a mesh: ep: 32 (over z, x), tp: 8 (over y, core).
Axes of the slice: x: 4, y: 4, z: 8, core: 2. Of those that a mesh axis runs over, the one named last changes fastest.
Arguments:
- tokens: bfloat16 [768, 4096], P('ep'), may hold values from -6 to 6
- delta_state: float32 [768, 16, 128, 128], P('ep', 'tp'), may hold values from -0.625 to 0.625
- attn_gain: float32 [4096], replicated, may hold values from 0.1 to 1.9
- query_weight: bfloat16 [4096, 2048], P('ep', 'tp'), may hold values from -0.09375 to 0.09375
- key_weight: bfloat16 [4096, 2048], P('ep', 'tp'), may hold values from -0.09375 to 0.09375
- value_weight: bfloat16 [4096, 2048], P('ep', 'tp'), may hold values from -0.09375 to 0.09375
- decay_weight: bfloat16 [4096, 16], replicated, may hold values from -0.09375 to 0.09375
- beta_weight: bfloat16 [4096, 16], replicated, may hold values from -0.09375 to 0.09375
- decay_rate: float32 [16], P('tp'), may hold values from 0.05 to 3
- head_gain: float32 [128], replicated, may hold values from 0.1 to 1.9
- output_weight: bfloat16 [2048, 4096], P('tp'), may hold values from -0.125 to 0.125
- ffn_gain: float32 [4096], replicated, may hold values from 0.1 to 1.9
- expert_ids: int32 [768, 2], P('ep'), may hold values from 0 to 31, all different within a row; in each aligned block of 24 rows (0 to 23, 24 to 47, ...) at most 3 rows name the same one
- group_prob: float32 [768], P('ep'), may hold values from 0.3 to 1
- expert_logit: float32 [768, 2], P('ep'), may hold values from -8 to 8
- expert_gate: bfloat16 [32, 4096, 1024], P('ep', None, 'tp'), may hold values from -0.09375 to 0.09375
- expert_up: bfloat16 [32, 4096, 1024], P('ep', None, 'tp'), may hold values from -0.09375 to 0.09375
- expert_down: bfloat16 [32, 1024, 4096], P('ep', 'tp'), may hold values from -0.1875 to 0.1875
- dense_gate: bfloat16 [4096, 4096], P('tp', 'ep'), may hold values from -0.09375 to 0.09375
- dense_up: bfloat16 [4096, 4096], P('tp', 'ep'), may hold values from -0.09375 to 0.09375
- dense_down: bfloat16 [4096, 4096], P('ep', 'tp'), may hold values from -0.09375 to 0.09375
- dense_mix: float32 [4096], P('tp'), may hold values from -3 to 3
Outputs:
- mixed_out: bfloat16 [768, 4096], P('ep', 'tp')
- new_state: float32 [768, 16, 128, 128], P('ep', 'tp')
The draws below stay inside these ranges and needn't reach their ends.
Inputs may be any that keep to these rules, and one draw needn't show every extreme that they name: `expert_ids`: each row names 2 different experts. Among the rows of one device (aligned blocks of 24 rows) no expert is named by more than 3 rows, and in every draw some expert reaches 3 in some block.
All inputs are finite; a program needn't handle non-finite values.
Results may differ from the reference program's by a relative error of at most 0.02.
Values may be sent and summed in bfloat16 or wider, within the bound.
No kernel may reach another device: no remote copies, remote signals or barrier semaphores. Data moves between devices by JAX's collectives and lax.ppermute only.
A program may use at most 64 MiB of HBM per device.

```python
import math
import jax
import jax.numpy as jnp
import numpy as np
from jax import lax

D = 4096
HEADS = 16
HEAD = 128
FE = 1024
FD = 4096
TOPK = 2
SEQ_DEV = 24
BATCH = 768
EXPERTS = 32
CAP = 3
N_EP = 32
N_TP = 8


def block_scale(stream_key, extent, pieces, low, top_value):
    factor_of = 1.0
    for dim, blocks in pieces:
        heights = jax.random.uniform(jax.random.fold_in(jax.random.fold_in(stream_key, 6), dim), (blocks,), jnp.float32, low / len(pieces), top_value / len(pieces))
        factor_of = factor_of * jnp.repeat(jnp.exp(heights), extent[dim] // blocks).reshape((-1,) + (1,) * (len(extent) - 1 - dim))
    return factor_of


def routed_block(own_key, own, number, rows, count, top, reach, slope):
    sequence = jax.random.permutation(own_key, count)
    crowded, usual = portions_of(count, rows * top, reach, slope, True), portions_of(count, rows * top, reach, slope, False)
    places = jnp.arange(count)

    def named(lengths, offset_by):
        used = int((lengths > 0).sum())
        fixed = max(1, used // 4)
        shifted = fixed + (places - fixed + offset_by * (used - fixed)) % max(1, count - fixed)
        return jnp.zeros((count,), jnp.int32).at[sequence[jnp.where(places < fixed, places, shifted)]].set(jnp.asarray(lengths, jnp.int32))

    lengths = jnp.where(number % 4 == 0, named(crowded, number // 4), named(usual, number - number // 4 - 1))
    mixed = jax.random.permutation(jax.random.fold_in(own, 3), count)
    giver, receiver = mixed[0:count // 2 * 2:2], mixed[1:count // 2 * 2:2]
    slack = jnp.minimum(lengths[giver] - 1, reach - lengths[receiver]) // 2
    slack = jnp.where((giver == sequence[0]) | (receiver == sequence[0]) | (lengths[receiver] == 0), 0, jnp.maximum(slack, 0))
    shifted = jax.random.randint(jax.random.fold_in(own, 4), (count // 2,), 0, 1 << 20) % (slack + 1)
    lengths = lengths.at[giver].add(-shifted).at[receiver].add(shifted)
    items = jnp.searchsorted(jnp.cumsum(lengths), jnp.arange(rows * top), side="right").astype(jnp.int32)
    table = items.reshape(top, rows).T
    table = table[jax.random.permutation(jax.random.fold_in(own, 1), rows)]
    offset_by = jax.random.randint(jax.random.fold_in(own, 2), (rows, 1), 0, top)
    return jnp.take_along_axis(table, (jnp.arange(top)[None, :] + offset_by) % top, axis=1)


def portions_of(count, total, most, lean, full):
    portions = [(1 << 20) // math.isqrt(grade ** lean) + 1 for grade in range(1, count + 1)]
    largest = most if full else min(most, max(-(-total // count), total * portions[0] // sum(portions)))
    least = 1 if total - largest >= count - 1 else 0
    holding, rest = [largest] + [least] * (count - 1), total - largest - least * (count - 1)
    while rest > 0:
        free = [i for i in range(1, count) if holding[i] < largest] or [i for i in range(1, count) if holding[i] < most]
        whole, budget = sum([portions[i] for i in free]), rest
        for i in free:
            more = min(most - holding[i], max(1, budget * portions[i] // whole), rest)
            holding[i] = holding[i] + more
            rest = rest - more
    return np.array(holding)


def bell_draw(stream_key, extent, width, most, pieces=(), held_as=jnp.bfloat16):
    drawn = width * jax.random.normal(stream_key, extent, jnp.float32)
    if pieces:
        drawn = drawn * block_scale(stream_key, extent, pieces, -0.22, 0.18)
    return jnp.clip(drawn, -most, most).astype(held_as)


def setup_inputs(seed: int = 0) -> dict:
    keys = jax.random.split(jax.random.key(seed), 23)
    tokens = bell_draw(keys[0], (BATCH, D), 1.0, 6.0, ((0, 32),))
    delta_state = bell_draw(keys[1], (BATCH, HEADS, HEAD, HEAD), 0.1, 0.625, ((0, 32), (1, 8)), jnp.float32)
    attn_gain = jnp.clip(1.0 + 0.18 * jax.random.normal(keys[2], (D,), jnp.float32), 0.1, 1.9)
    query_weight = bell_draw(keys[3], (D, HEADS * HEAD), D ** -0.5, 0.09375, ((0, 32), (1, 8)))
    key_weight = bell_draw(keys[4], (D, HEADS * HEAD), D ** -0.5, 0.09375, ((0, 32), (1, 8)))
    value_weight = bell_draw(keys[5], (D, HEADS * HEAD), D ** -0.5, 0.09375, ((0, 32), (1, 8)))
    decay_weight = bell_draw(keys[6], (D, HEADS), D ** -0.5, 0.09375)
    beta_weight = bell_draw(keys[7], (D, HEADS), D ** -0.5, 0.09375)
    decay_rate = jnp.clip(jnp.exp(math.log(3.0) - 4.0943445 * jax.random.uniform(keys[8], (HEADS,), jnp.float32) ** block_scale(keys[8], (HEADS,), ((0, 8),), -0.2, 0.2)), 0.05, 3.0)
    head_gain = jnp.clip(1.0 + 0.18 * jax.random.normal(keys[9], (HEAD,), jnp.float32), 0.1, 1.9)
    output_weight = bell_draw(keys[10], (HEADS * HEAD, D), (HEADS * HEAD) ** -0.5, 0.125, ((0, 8),))
    ffn_gain = jnp.clip(1.0 + 0.18 * jax.random.normal(keys[11], (D,), jnp.float32), 0.1, 1.9)
    expert_ids_keys = jax.random.split(jax.random.fold_in(keys[12], 1), BATCH // SEQ_DEV)
    expert_ids_turns = jax.random.permutation(jax.random.fold_in(keys[12], 3), BATCH // SEQ_DEV)
    expert_ids = jax.vmap(lambda own, number: routed_block(jax.random.fold_in(keys[12], 2), own, number, SEQ_DEV, EXPERTS, TOPK, CAP, 2))(expert_ids_keys, expert_ids_turns).reshape((BATCH, TOPK))
    group_prob = jnp.clip(0.3 + 0.7 * jax.random.uniform(keys[13], (BATCH,), jnp.float32) ** block_scale(keys[13], (BATCH,), ((0, 32),), -0.2, 0.2), 0.3, 1.0)
    expert_logit = bell_draw(keys[14], (BATCH, TOPK), 1.5, 8.0, ((0, 32),), jnp.float32)
    expert_gate = bell_draw(keys[15], (EXPERTS, D, FE), D ** -0.5, 0.09375, ((0, 32), (2, 8)))
    expert_up = bell_draw(keys[16], (EXPERTS, D, FE), D ** -0.5, 0.09375, ((0, 32), (2, 8)))
    expert_down = bell_draw(keys[17], (EXPERTS, FE, D), FE ** -0.5, 0.1875, ((0, 32), (1, 8)))
    dense_gate = bell_draw(keys[18], (D, FD), D ** -0.5, 0.09375, ((0, 8), (1, 32)))
    dense_up = bell_draw(keys[19], (D, FD), D ** -0.5, 0.09375, ((0, 8), (1, 32)))
    dense_down = bell_draw(keys[20], (FD, D), FD ** -0.5, 0.09375, ((0, 32), (1, 8)))
    dense_mix = jnp.clip(jax.random.uniform(keys[21], (D,), jnp.float32, -3.0, 3.0) * block_scale(keys[21], (D,), ((0, 8),), -0.4, 0.0), -3.0, 3.0)
    return {"tokens": tokens, "delta_state": delta_state, "attn_gain": attn_gain, "query_weight": query_weight, "key_weight": key_weight, "value_weight": value_weight, "decay_weight": decay_weight, "beta_weight": beta_weight, "decay_rate": decay_rate, "head_gain": head_gain, "output_weight": output_weight, "ffn_gain": ffn_gain, "expert_ids": expert_ids, "group_prob": group_prob, "expert_logit": expert_logit, "expert_gate": expert_gate, "expert_up": expert_up, "expert_down": expert_down, "dense_gate": dense_gate, "dense_up": dense_up, "dense_down": dense_down, "dense_mix": dense_mix}


EPS = 1e-06

def rms_scale(values, gain):
    mean_sq = lax.optimization_barrier(jnp.mean(values * values, axis=-1, keepdims=True))
    return values * lax.rsqrt(mean_sq + EPS) * gain

def unit_rows(values):
    return values * lax.rsqrt(lax.optimization_barrier(jnp.sum(values * values, axis=-1, keepdims=True)) + EPS)

def rounded_back(values):
    return lax.optimization_barrier(values.astype(jnp.bfloat16)).astype(jnp.float32)

def block_sum(left, right, blocks):
    size = left.shape[1] // blocks
    total = jnp.zeros((left.shape[0], right.shape[1]), jnp.float32)
    for index in range(blocks):
        part = jnp.dot(left[:, index * size:(index + 1) * size], right[index * size:(index + 1) * size], preferred_element_type=jnp.float32)
        total = total + rounded_back(part)
    return total

def reference(tokens, delta_state, attn_gain, query_weight, key_weight, value_weight, decay_weight, beta_weight, decay_rate, head_gain, output_weight, ffn_gain, expert_ids, group_prob, expert_logit, expert_gate, expert_up, expert_down, dense_gate, dense_up, dense_down, dense_mix):
    residual = tokens.astype(jnp.float32)
    normed = rms_scale(residual, attn_gain).astype(jnp.bfloat16)

    def heads_of(weight):
        product = jnp.dot(normed, weight, preferred_element_type=jnp.float32)
        return rounded_back(product).reshape(BATCH, HEADS, HEAD)
    query_unit = unit_rows(heads_of(query_weight)) * HEAD ** (-0.5)
    key_unit = unit_rows(heads_of(key_weight))
    value_heads = heads_of(value_weight)
    decay = jnp.exp(-decay_rate * jax.nn.softplus(jnp.dot(normed, decay_weight, preferred_element_type=jnp.float32)))
    beta_gate = jax.nn.sigmoid(jnp.dot(normed, beta_weight, preferred_element_type=jnp.float32))
    recalled = jnp.einsum('bhk,bhkv->bhv', key_unit, delta_state, precision=lax.Precision.HIGHEST)
    correction = beta_gate[..., None] * (value_heads - decay[..., None] * recalled)
    new_state = decay[..., None, None] * delta_state + key_unit[..., :, None] * correction[..., None, :]
    read_out = jnp.einsum('bhk,bhkv->bhv', query_unit, new_state, precision=lax.Precision.HIGHEST)
    head_out = rms_scale(read_out, head_gain).astype(jnp.bfloat16).reshape(BATCH, HEADS * HEAD)
    attn_sum = block_sum(head_out, output_weight, N_TP)
    middle = residual + attn_sum
    ffn_in = rms_scale(middle, ffn_gain).astype(jnp.bfloat16)
    dense_pre_gate = block_sum(ffn_in, dense_gate, N_TP)
    dense_pre_up = block_sum(ffn_in, dense_up, N_TP)
    dense_hidden = (jax.nn.silu(dense_pre_gate) * dense_pre_up).astype(jnp.bfloat16)
    dense_out = jnp.dot(dense_hidden, dense_down, preferred_element_type=jnp.float32)
    pairs = SEQ_DEV * TOPK
    block_ids = expert_ids.reshape(N_EP, pairs)
    onehot = (block_ids[:, :, None] == jnp.arange(EXPERTS, dtype=jnp.int32)[None, None, :]).astype(jnp.int32)
    ranks = lax.optimization_barrier(jnp.sum(onehot * (jnp.cumsum(onehot, axis=1) - 1), axis=2))
    sources = jnp.arange(N_EP, dtype=jnp.int32)[:, None]
    places = (block_ids * (N_EP * CAP) + sources * CAP + ranks).reshape(-1).astype(jnp.int32)
    repeated = jnp.repeat(ffn_in, TOPK, axis=0)
    slots = jnp.zeros((EXPERTS * N_EP * CAP, D), jnp.bfloat16).at[places].set(repeated)
    slots = slots.reshape(EXPERTS, N_EP * CAP, D)

    def one_expert(inputs):
        arrived, gate_w, up_w, down_w = inputs
        gate_vals = jnp.dot(arrived, gate_w, preferred_element_type=jnp.float32)
        up_vals = jnp.dot(arrived, up_w, preferred_element_type=jnp.float32)
        expert_hidden = (jax.nn.silu(gate_vals) * up_vals).astype(jnp.bfloat16)
        return block_sum(expert_hidden, down_w, N_TP).astype(jnp.bfloat16)
    expert_result = lax.map(one_expert, (slots, expert_gate, expert_up, expert_down))
    picked = jnp.take(expert_result.reshape(EXPERTS * N_EP * CAP, D), places, axis=0)
    picked = picked.astype(jnp.float32).reshape(BATCH, TOPK, D)
    logit_exp = jnp.exp(expert_logit)
    route_weight = group_prob[:, None] * logit_exp / lax.optimization_barrier(jnp.sum(logit_exp, axis=1, keepdims=True))
    expert_mix = lax.optimization_barrier(jnp.sum(route_weight[..., None] * picked, axis=1))
    mixed_out = (middle + jax.nn.sigmoid(dense_mix) * dense_out + expert_mix).astype(jnp.bfloat16)
    return (mixed_out, new_state)
```

```python
import jax
import jax.numpy as jnp
from jax import lax
from jax.sharding import Mesh, PartitionSpec as P

EPS = 1e-06
BF = jnp.bfloat16
F32 = jnp.float32
NZ, NX, NT = 8, 4, 8
CAP = 3


def exchange(tiles, axes):
    return lax.all_to_all(tiles, axes, split_axis=0, concat_axis=0, tiled=True)


def gathered(shard, axis):
    count = lax.axis_size(axis)
    return exchange(jnp.broadcast_to(shard[None], (count, *shard.shape)), axis)


def two_parts(values):
    high = lax.reduce_precision(values, 8, 7)
    return high.astype(BF), (values - high).astype(BF)


def unit_rows(values):
    return values * lax.rsqrt(jnp.sum(values * values, axis=-1, keepdims=True) + EPS)


def rms_scale(values, gain):
    mean_sq = jnp.mean(values * values, axis=-1, keepdims=True)
    return values * lax.rsqrt(mean_sq + EPS) * gain


def per_device(
    tokens,
    delta_state,
    attn_gain,
    query_weight,
    key_weight,
    value_weight,
    decay_weight,
    beta_weight,
    decay_rate,
    head_gain,
    output_weight,
    ffn_gain,
    expert_ids,
    group_prob,
    expert_logit,
    expert_gate,
    expert_up,
    expert_down,
    dense_gate,
    dense_up,
    dense_down,
    dense_mix,
):
    rows, width = tokens.shape
    heads, size = delta_state.shape[1:3]
    cols = heads * size
    block = width // NT
    zi = lax.axis_index("z")
    ti = lax.axis_index("y") * 2 + lax.axis_index("c")

    qkv_weight = gathered(jnp.concatenate((query_weight, key_weight, value_weight), axis=1), "x")
    qkv_weight = qkv_weight.reshape(block, 3 * cols)
    half = dense_gate.shape[1]
    dense_all = gathered(
        jnp.concatenate(
            (
                jnp.concatenate((dense_gate, dense_up), axis=1),
                dense_down[:, : block // 2],
                dense_down[:, block // 2 :],
            ),
            axis=0,
        ),
        "x",
    )
    gate_up = dense_all[:, :block]
    down = jnp.concatenate((dense_all[:, block : block + half], dense_all[:, block + half :]), axis=2)

    pair_ids = expert_ids.reshape(-1)
    experts = jnp.arange(NZ * NX, dtype=jnp.int32)
    onehot = (pair_ids[:, None] == experts[None, :]).astype(F32)
    count = rows * 2
    earlier = jnp.arange(count)[:, None] > jnp.arange(count)[None, :]
    before = jnp.dot(earlier.astype(F32), onehot, preferred_element_type=F32)
    ranks = jnp.sum(onehot * before, axis=1)
    places = (pair_ids.astype(F32) * CAP + ranks).reshape(rows, 2)
    logit_exp = jnp.exp(expert_logit)
    route = group_prob[:, None] * logit_exp / jnp.sum(logit_exp, axis=1, keepdims=True)
    route_high, route_low = two_parts(route)
    meta = jnp.concatenate((places.astype(BF).T, route_high.T, route_low.T, jnp.zeros((2, rows), BF)), 0)
    meta = jnp.where(jnp.arange(NZ)[None, :, None] == zi, meta[:, None, :], 0).reshape(8, NZ * rows)
    meta = jnp.pad(meta, ((0, 0), (0, block - NZ * rows)))

    residual = tokens.astype(F32)
    token_scale = lax.rsqrt(jnp.mean(residual * residual, axis=-1, keepdims=True) + EPS)
    gained = (residual * attn_gain).astype(BF)
    message = gained.reshape(rows, NZ, block).transpose(1, 0, 2)
    message = jnp.concatenate((message, jnp.broadcast_to(meta[None], (NZ, 8, block))), axis=1)
    arrived = exchange(message, "z")
    spread = arrived[:, :rows].reshape(NZ * rows, block)
    route_rows = jnp.sum(arrived[:, rows:, : NZ * rows].astype(F32), axis=0)

    part = jnp.dot(spread, qkv_weight, preferred_element_type=F32).astype(BF)
    summed = exchange(part.reshape(NZ, rows, 3 * cols), "z").astype(F32).sum(axis=0) * token_scale

    def heads_of(values):
        return values.reshape(rows, heads, size)

    query_unit = unit_rows(heads_of(summed[:, :cols])) * size ** (-0.5)
    key_unit = unit_rows(heads_of(summed[:, cols : 2 * cols]))
    value_heads = heads_of(summed[:, 2 * cols :])
    decay_cols = lax.dynamic_slice_in_dim(decay_weight, ti * heads, heads, 1)
    beta_cols = lax.dynamic_slice_in_dim(beta_weight, ti * heads, heads, 1)
    decay_pre = jnp.dot(gained, decay_cols, preferred_element_type=F32) * token_scale
    beta_pre = jnp.dot(gained, beta_cols, preferred_element_type=F32) * token_scale
    decay = jnp.exp(-decay_rate * jax.nn.softplus(decay_pre))
    beta_gate = jax.nn.sigmoid(beta_pre)
    recalled = jnp.einsum("bhk,bhkv->bhv", key_unit, delta_state)
    correction = beta_gate[..., None] * (value_heads - decay[..., None] * recalled)
    new_state = (
        decay[..., None, None] * delta_state + key_unit[..., :, None] * correction[..., None, :]
    )
    read_out = jnp.einsum("bhk,bhkv->bhv", query_unit, new_state)
    head_out = rms_scale(read_out, head_gain).astype(BF).reshape(rows, cols)
    attn_part = jnp.dot(head_out, output_weight, preferred_element_type=F32).astype(BF)
    attn_part = attn_part.reshape(rows, NT, block).transpose(1, 0, 2)
    attn_sum = exchange(attn_part, ("y", "c")).astype(F32).sum(axis=0)
    own_tokens = lax.dynamic_slice_in_dim(tokens, ti * block, block, 1)
    middle = own_tokens.astype(F32) + attn_sum

    mid = gathered(middle.astype(BF), "z").reshape(NZ * rows, block)
    own_gain = lax.dynamic_slice_in_dim(ffn_gain, ti * block, block, 0)
    mid_wide = mid.astype(F32)
    square = jnp.sum(mid_wide * mid_wide, axis=1).reshape(NT, rows)
    square_high, square_low = two_parts(square)
    scaled = (mid_wide * own_gain).astype(BF)
    dense_part = jnp.einsum("nd,xdf->xnf", scaled, gate_up, preferred_element_type=F32).astype(BF)
    dense_part = dense_part.reshape(NX, NT, rows, 2 * half)

    code = route_rows[:2].astype(jnp.int32) - zi * (NX * CAP)
    token_z = jnp.arange(NZ * rows, dtype=jnp.int32) // rows
    slot = (code // CAP) * (NZ * CAP) + token_z[None] * CAP + code % CAP
    slot = jnp.where((code >= 0) & (code < NX * CAP), slot, -1)
    slots = NX * NZ * CAP
    hits = jnp.arange(slots, dtype=jnp.int32)[None, :, None] == slot[:, None, :]
    dispatch = (hits[0] | hits[1]).astype(BF)
    chosen = jnp.dot(dispatch, mid, preferred_element_type=F32).astype(BF)
    chosen = chosen.reshape(NX, 1, NZ * CAP, 2, block // 2)
    chosen = jnp.broadcast_to(chosen, (NX, NT, NZ * CAP, 2, block // 2))
    squares = jnp.stack((square_high, square_low), axis=1)
    squares = jnp.pad(squares, ((0, 0), (0, 6), (0, 2 * half - rows)))
    squares = jnp.broadcast_to(squares[None], (NX, NT, 8, 2 * half))
    message = jnp.concatenate(
        (chosen[:, :, :, 0], chosen[:, :, :, 1], dense_part, squares), axis=2
    )
    message = message.reshape(NX * NT, *message.shape[2:])
    arrived = exchange(message, ("x", "y", "c")).reshape(NX, NT, *message.shape[1:])
    per = NZ * CAP
    routed = arrived[:, :, : 2 * per].reshape(NX, NT, 2, per, block // 2)
    routed = routed.transpose(0, 3, 1, 2, 4).reshape(NX * per, width).astype(F32)
    routed_scale = lax.rsqrt(jnp.mean(routed * routed, axis=1, keepdims=True) + EPS)
    routed = (routed * routed_scale * ffn_gain).astype(BF)
    gate_vals = jnp.dot(routed, expert_gate[0], preferred_element_type=F32)
    up_vals = jnp.dot(routed, expert_up[0], preferred_element_type=F32)
    hidden = (jax.nn.silu(gate_vals) * up_vals).astype(BF)
    result = jnp.dot(hidden, expert_down[0], preferred_element_type=F32).astype(BF)
    result = result.reshape(NX, per, NT, block).transpose(0, 2, 1, 3)

    dense_sum = arrived[:, :, 2 * per : 2 * per + rows].astype(F32).sum(axis=1)
    square_sum = arrived[:, :, 2 * per + rows : 2 * per + rows + 2, :rows].astype(F32).sum(axis=(1, 2))
    dense_scale = lax.rsqrt(square_sum / width + EPS)
    dense_sum = dense_sum * dense_scale[:, :, None]
    dense_hidden = (jax.nn.silu(dense_sum[..., :half]) * dense_sum[..., half:]).astype(BF)
    dense_hidden = jnp.broadcast_to(dense_hidden[:, None], (NX, NT, rows, half))
    message = jnp.concatenate((result, dense_hidden), axis=3).reshape(NX * NT, rows, block + half)
    arrived = exchange(message, ("x", "y", "c")).reshape(NX, NT, rows, block + half)
    expert_sum = arrived[..., :block].astype(F32).sum(axis=1).astype(BF).reshape(slots, block)
    dense_in = arrived[..., block:].reshape(NX, NT * rows, half)
    dense_out = jnp.einsum("xnf,xfd->nd", dense_in, down, preferred_element_type=F32)
    mix_high = jnp.where(hits[0], route_rows[2], jnp.where(hits[1], route_rows[3], 0)).astype(BF)
    mix_low = jnp.where(hits[0], route_rows[4], jnp.where(hits[1], route_rows[5], 0)).astype(BF)
    over_slots = (((0,), (0,)), ((), ()))
    expert_mix = lax.dot_general(mix_high, expert_sum, over_slots, preferred_element_type=F32)
    expert_mix += lax.dot_general(mix_low, expert_sum, over_slots, preferred_element_type=F32)
    mixed = (jax.nn.sigmoid(dense_mix) * dense_out + expert_mix).astype(BF)
    mixed = exchange(mixed.reshape(NZ, rows, block), "z").astype(F32).sum(axis=0)
    return ((middle + mixed).astype(BF), new_state)


def solution(mesh):
    fine = Mesh(mesh.devices.reshape(NZ, NX, 4, 2), ("z", "x", "y", "c"))
    ep, tp = ("z", "x"), ("y", "c")
    return jax.shard_map(
        per_device,
        mesh=fine,
        in_specs=(
            P(ep, None),
            P(ep, tp, None, None),
            P(),
            P(ep, tp),
            P(ep, tp),
            P(ep, tp),
            P(),
            P(),
            P(tp),
            P(),
            P(tp, None),
            P(),
            P(ep, None),
            P(ep),
            P(ep, None),
            P(ep, None, tp),
            P(ep, None, tp),
            P(ep, tp, None),
            P(tp, ep),
            P(tp, ep),
            P(ep, tp),
            P(tp),
        ),
        out_specs=(P(ep, tp), P(ep, tp, None, None)),
        check_vma=False,
    )
```

```python
import jax
import jax.numpy as jnp
from jax import lax
from jax.experimental import pallas as pl
from jax.experimental.pallas import tpu as pltpu
from jax.sharding import Mesh, PartitionSpec as P

EPS = 1e-06
BF = jnp.bfloat16
F32 = jnp.float32
NZ, NX, NT = 8, 4, 8
CAP = 3
MIB = 1 << 20


def exchange(tiles, axes):
    return lax.all_to_all(tiles, axes, split_axis=0, concat_axis=0, tiled=True)


def from_neighbours(shard, axis):
    count = lax.axis_size(axis)
    parts = [shard]
    for step in range(1, count):
        pairs = [(source, (source - step) % count) for source in range(count)]
        parts.append(lax.ppermute(shard, axis, pairs))
    return parts


def two_parts(values):
    high = lax.reduce_precision(values, 8, 7)
    return high.astype(BF), (values - high).astype(BF)


def unit_rows(values):
    return values * lax.rsqrt(jnp.sum(values * values, axis=-1, keepdims=True) + EPS)


def silu(values):
    return values / (1.0 + jnp.exp(-values))


def kernel(body, outs, index, *args, scratch=(), flops=0, limit=16):
    specs = [pl.BlockSpec(memory_space=pltpu.SMEM)]
    specs += [pl.BlockSpec(memory_space=pltpu.VMEM)] * len(args)
    return pl.pallas_call(
        body,
        out_shape=outs,
        in_specs=specs,
        out_specs=jax.tree.map(lambda _: pl.BlockSpec(memory_space=pltpu.VMEM), outs),
        scratch_shapes=list(scratch),
        cost_estimate=pl.CostEstimate(flops=flops, bytes_accessed=0, transcendentals=0),
        compiler_params=pltpu.CompilerParams(vmem_limit_bytes=limit * MIB),
    )(index, *args)


def wrapped(value, count):
    return jnp.where(value >= count, value - count, value)


def spread_body(index, tokens, gain, out):
    block = out.shape[2]
    for z in range(NZ):
        cols = slice(z * block, (z + 1) * block)
        out[z] = (tokens[:, cols].astype(F32) * gain[:, cols]).astype(BF)


def project_body(index, arrived, w0, w1, w2, w3, out):
    groups, rows, _ = arrived.shape
    total = None
    for step, weight in enumerate((w0, w1, w2, w3)):
        size = weight.shape[0]
        place = pl.multiple_of(wrapped(index[1] + step, NX) * size, size)
        left = arrived[:, :, pl.ds(place, size)].astype(F32).reshape(groups * rows, size).astype(BF)
        part = jnp.dot(left, weight[...], preferred_element_type=F32)
        total = part if total is None else total + part
    out[...] = total.reshape(groups, rows, -1).astype(BF)


def state_body(index, arrived, scale, decay, beta, state, head_gain, weight, new_state, out, read):
    rows, heads, size = state.shape[:3]
    cols = heads * size
    summed = arrived[0].astype(F32)
    for z in range(1, NZ):
        summed = summed + arrived[z].astype(F32)
    summed = summed * scale[...]
    head_rows = []
    for h in range(heads):
        query = unit_rows(summed[:, h * size : (h + 1) * size]) * size ** (-0.5)
        key = unit_rows(summed[:, cols + h * size : cols + (h + 1) * size])
        value = summed[:, 2 * cols + h * size : 2 * cols + (h + 1) * size]
        query_cols = query.T
        key_cols = key.T
        both = jnp.sum(query * key, axis=1, keepdims=True)
        for b in range(rows):
            old = state[b, h]
            key_col = key_cols[:, b : b + 1]
            query_col = query_cols[:, b : b + 1]
            fade = decay[b : b + 1, h : h + 1]
            recalled = jnp.sum(key_col * old, axis=0, keepdims=True)
            asked = jnp.sum(query_col * old, axis=0, keepdims=True)
            correction = beta[b : b + 1, h : h + 1] * (value[b : b + 1] - fade * recalled)
            new_state[b, h] = fade * old + key_col * correction
            read[b : b + 1, :] = fade * asked + both[b : b + 1] * correction
        result = read[...]
        mean_sq = jnp.mean(result * result, axis=1, keepdims=True)
        head_rows.append((result * lax.rsqrt(mean_sq + EPS) * head_gain[...]).astype(BF))
    block = out.shape[2]
    for t in range(NT):
        part = None
        for h in range(heads):
            right = weight[h * size : (h + 1) * size, t * block : (t + 1) * block]
            product = jnp.dot(head_rows[h], right, preferred_element_type=F32)
            part = product if part is None else part + product
        out[t] = part.astype(BF)


def middle_body(index, arrived, tokens, meta, middle, out):
    block = middle.shape[1]
    rows = middle.shape[0]
    summed = arrived[0].astype(F32)
    for t in range(1, NT):
        summed = summed + arrived[t].astype(F32)
    place = pl.multiple_of(index[2] * block, block)
    total = tokens[:, pl.ds(place, block)].astype(F32) + summed
    middle[...] = total
    narrow = total.astype(BF)
    for z in range(NZ):
        out[z, :rows, :] = narrow
        out[z, rows:, :] = meta[...]


def slots_of(route, zi):
    tokens = route.shape[1]
    lane = lax.broadcasted_iota(jnp.int32, (1, tokens), 1)
    source = jnp.zeros((1, tokens), jnp.int32)
    for z in range(1, NZ):
        source = source + jnp.where(lane >= z * (tokens // NZ), 1, 0)
    slots = []
    for k in range(2):
        code = route[k : k + 1, :].astype(jnp.int32) - zi * (NX * CAP)
        expert = jnp.zeros((1, tokens), jnp.int32)
        for x in range(1, NX):
            expert = expert + jnp.where(code >= x * CAP, 1, 0)
        slot = expert * (NZ * CAP) + source * CAP + (code - expert * CAP)
        slots.append(jnp.where((code >= 0) & (code < NX * CAP), slot, -1))
    return slots


def dispatch_body(index, arrived, gain, g0, g1, g2, g3, out, route):
    rows = out.shape[2] - 8
    rows = rows // 3
    tokens = NZ * rows
    block = arrived.shape[2]
    half = block // 2
    wide = arrived[:, :rows, :].astype(F32).reshape(tokens, block)
    narrow = wide.astype(BF)
    routing = arrived[0, rows:, :tokens].astype(F32)
    for z in range(1, NZ):
        routing = routing + arrived[z, rows:, :tokens].astype(F32)
    route[...] = routing
    slot0, slot1 = slots_of(routing, index[0])
    place = lax.broadcasted_iota(jnp.int32, (NX * rows, tokens), 0)
    picks = jnp.where((place == slot0) | (place == slot1), 1.0, 0.0).astype(BF)
    chosen = jnp.dot(picks, narrow, preferred_element_type=F32).astype(BF)
    square = lax.dot_general(
        jnp.ones((8, block), F32),
        wide * wide,
        (((1,), (1,)), ((), ())),
        precision=lax.Precision.HIGHEST,
        preferred_element_type=F32,
    )
    high = square.astype(BF).astype(F32)
    first = lax.broadcasted_iota(jnp.int32, square.shape, 0) == 0
    square = jnp.where(first, high, square - high).astype(BF)
    for x in range(NX):
        own = chosen[x * rows : (x + 1) * rows]
        for t in range(NT):
            out[x, t, :rows, :] = own[:, :half]
            out[x, t, rows : 2 * rows, :] = own[:, half:]
            out[x, t, 3 * rows :, :tokens] = square
            out[x, t, 3 * rows :, tokens:] = jnp.zeros((8, half - tokens), BF)
    scaled = (wide * gain[...]).astype(BF)
    for step, weight in enumerate((g0, g1, g2, g3)):
        part = jnp.dot(scaled, weight[:block, :], preferred_element_type=F32)
        x = wrapped(index[1] + step, NX)
        out[x, :, 2 * rows : 3 * rows, :] = part.reshape(NT, rows, half).astype(BF)


def expert_body(index, arrived, gain, gate, up, down, out):
    rows = out.shape[2]
    block = out.shape[3] - 128
    half = block // 2
    width = gate.shape[0]
    slots = NX * rows
    squares = jnp.zeros((slots, half), F32)
    gate_sum = jnp.zeros((slots, gate.shape[1]), F32)
    up_sum = jnp.zeros((slots, gate.shape[1]), F32)
    for t in range(NT):
        for part in range(2):
            wide = arrived[:, t, part * rows : (part + 1) * rows, :].astype(F32).reshape(slots, half)
            squares = squares + wide * wide
            place = t * block + part * half
            left = (wide * gain[:, place : place + half]).astype(BF)
            gate_sum += jnp.dot(left, gate[place : place + half, :], preferred_element_type=F32)
            up_sum += jnp.dot(left, up[place : place + half, :], preferred_element_type=F32)
    scale = lax.rsqrt(jnp.sum(squares, axis=1, keepdims=True) / width + EPS)
    hidden = (silu(gate_sum * scale) * (up_sum * scale)).astype(BF)
    for t in range(NT):
        result = jnp.dot(hidden, down[:, t * block : (t + 1) * block], preferred_element_type=F32)
        out[:, t, :, :block] = result.reshape(NX, rows, block).astype(BF)
    tokens = NZ * rows
    lane = lax.broadcasted_iota(jnp.int32, (rows, tokens), 1)
    own = lane == lax.broadcasted_iota(jnp.int32, (rows, tokens), 0) + index[2] * rows
    for x in range(NX):
        summed = arrived[x, 0, 2 * rows : 3 * rows, :].astype(F32)
        square = arrived[x, 0, 3 * rows :, :tokens].astype(F32)
        for t in range(1, NT):
            summed = summed + arrived[x, t, 2 * rows : 3 * rows, :].astype(F32)
            square = square + arrived[x, t, 3 * rows :, :tokens].astype(F32)
        square = square[0:1, :] + square[1:2, :]
        square = jnp.sum(jnp.where(own, square, 0.0), axis=1, keepdims=True)
        summed = summed * lax.rsqrt(square / width + EPS)
        result = (silu(summed[:, : half // 2]) * summed[:, half // 2 :]).astype(BF)
        for t in range(NT):
            out[x, t, :, block:] = result


def combine_body(index, arrived, route, d0, d1, d2, d3, mix, out):
    rows = arrived.shape[2]
    block = out.shape[2]
    tokens = NZ * rows
    results = []
    for x in range(NX):
        summed = arrived[x, 0, :, :block].astype(F32)
        for t in range(1, NT):
            summed = summed + arrived[x, t, :, :block].astype(F32)
        results.append(summed)
    results = jnp.concatenate(results, axis=0).astype(BF)
    routing = route[...]
    slot0, slot1 = slots_of(routing, index[0])
    place = lax.broadcasted_iota(jnp.int32, (NX * rows, tokens), 0)
    mixed = jnp.zeros((tokens, block), F32)
    for k in range(2):
        share = jnp.where(place == slot0, routing[2 + 2 * k : 3 + 2 * k, :], 0.0)
        share = jnp.where(place == slot1, routing[3 + 2 * k : 4 + 2 * k, :], share).astype(BF)
        mixed += lax.dot_general(
            share, results, (((0,), (0,)), ((), ())), preferred_element_type=F32
        )
    lower = jnp.zeros((tokens, block // 2), F32)
    upper = jnp.zeros((tokens, block // 2), F32)
    for step, weight in enumerate((d0, d1, d2, d3)):
        x = wrapped(index[1] + step, NX)
        left = arrived[x, :, :, block:].astype(F32).reshape(tokens, -1).astype(BF)
        size = left.shape[1]
        lower += jnp.dot(left, weight[block : block + size, :], preferred_element_type=F32)
        upper += jnp.dot(left, weight[block + size :, :], preferred_element_type=F32)
    gate = 1.0 / (1.0 + jnp.exp(-mix[...]))
    dense = jnp.concatenate((lower, upper), axis=1)
    out[...] = (gate * dense + mixed).reshape(NZ, rows, block).astype(BF)


def final_body(index, arrived, middle, out):
    summed = arrived[0].astype(F32)
    for z in range(1, NZ):
        summed = summed + arrived[z].astype(F32)
    out[...] = (middle[...] + summed).astype(BF)


def per_device(
    tokens,
    delta_state,
    attn_gain,
    query_weight,
    key_weight,
    value_weight,
    decay_weight,
    beta_weight,
    decay_rate,
    head_gain,
    output_weight,
    ffn_gain,
    expert_ids,
    group_prob,
    expert_logit,
    expert_gate,
    expert_up,
    expert_down,
    dense_gate,
    dense_up,
    dense_down,
    dense_mix,
):
    rows, width = tokens.shape
    heads, size = delta_state.shape[1:3]
    cols = heads * size
    block = width // NT
    half = block // 2
    zi = lax.axis_index("z")
    ti = lax.axis_index("y") * 2 + lax.axis_index("c")
    index = jnp.stack((zi, lax.axis_index("x"), ti)).astype(jnp.int32)

    def shape(*dims, dtype=BF):
        return jax.ShapeDtypeStruct(dims, dtype)

    qkv_weights = from_neighbours(
        jnp.concatenate((query_weight, key_weight, value_weight), axis=1), "x"
    )
    dense_weights = from_neighbours(
        jnp.concatenate(
            (
                jnp.concatenate((dense_gate, dense_up), axis=1),
                dense_down[:, :half],
                dense_down[:, half:],
            ),
            axis=0,
        ),
        "x",
    )

    message = kernel(spread_body, shape(NZ, rows, block), index, tokens, attn_gain[None])
    spread = exchange(message, "z")

    pair_ids = expert_ids.reshape(-1)
    experts = jnp.arange(NZ * NX, dtype=jnp.int32)
    onehot = (pair_ids[:, None] == experts[None, :]).astype(F32)
    count = rows * 2
    earlier = jnp.arange(count)[:, None] > jnp.arange(count)[None, :]
    before = jnp.dot(earlier.astype(F32), onehot, preferred_element_type=F32)
    ranks = jnp.sum(onehot * before, axis=1)
    places = (pair_ids.astype(F32) * CAP + ranks).reshape(rows, 2)
    logit_exp = jnp.exp(expert_logit)
    route = group_prob[:, None] * logit_exp / jnp.sum(logit_exp, axis=1, keepdims=True)
    route_high, route_low = two_parts(route)
    meta = jnp.concatenate((places.astype(BF).T, route_high.T, route_low.T, jnp.zeros((2, rows), BF)), 0)
    meta = jnp.where(jnp.arange(NZ)[None, :, None] == zi, meta[:, None, :], 0).reshape(8, NZ * rows)
    meta = jnp.pad(meta, ((0, 0), (0, block - NZ * rows)))

    residual = tokens.astype(F32)
    token_scale = lax.rsqrt(jnp.mean(residual * residual, axis=-1, keepdims=True) + EPS)
    gained = (residual * attn_gain).astype(BF)
    decay_cols = lax.dynamic_slice_in_dim(decay_weight, ti * heads, heads, 1)
    beta_cols = lax.dynamic_slice_in_dim(beta_weight, ti * heads, heads, 1)
    decay_pre = jnp.dot(gained, decay_cols, preferred_element_type=F32) * token_scale
    beta_pre = jnp.dot(gained, beta_cols, preferred_element_type=F32) * token_scale
    decay = jnp.exp(-decay_rate * jax.nn.softplus(decay_pre))
    beta_gate = jax.nn.sigmoid(beta_pre)

    part = kernel(
        project_body,
        shape(NZ, rows, 3 * cols),
        index,
        spread,
        *qkv_weights,
        flops=2 * NZ * rows * block * 3 * cols,
    )
    arrived = exchange(part, "z")
    new_state, attn_part = kernel(
        state_body,
        (shape(*delta_state.shape, dtype=F32), shape(NT, rows, block)),
        index,
        arrived,
        token_scale,
        decay,
        beta_gate,
        delta_state,
        head_gain[None],
        output_weight,
        scratch=(pltpu.VMEM((rows, size), F32),),
        flops=2 * rows * cols * width,
    )
    arrived = exchange(attn_part, ("y", "c"))
    middle, message = kernel(
        middle_body,
        (shape(rows, block, dtype=F32), shape(NZ, rows + 8, block)),
        index,
        arrived,
        tokens,
        meta,
    )

    arrived = exchange(message, "z")
    own_gain = lax.dynamic_slice_in_dim(ffn_gain, ti * block, block, 0)[None]
    message, route_rows = kernel(
        dispatch_body,
        (shape(NX, NT, 3 * rows + 8, half), shape(8, NZ * rows, dtype=F32)),
        index,
        arrived,
        own_gain,
        *dense_weights,
        flops=2 * NZ * rows * block * 2 * block,
    )
    sides = ("x", "y", "c")
    arrived = exchange(message.reshape(NX * NT, -1, half), sides).reshape(message.shape)
    message = kernel(
        expert_body,
        shape(NX, NT, rows, block + 128),
        index,
        arrived,
        ffn_gain[None],
        expert_gate[0],
        expert_up[0],
        expert_down[0],
        flops=6 * NX * rows * width * 128,
    )
    arrived = exchange(message.reshape(NX * NT, rows, -1), sides).reshape(message.shape)
    message = kernel(
        combine_body,
        shape(NZ, rows, block),
        index,
        arrived,
        route_rows,
        *dense_weights,
        dense_mix[None],
        flops=2 * NZ * rows * block * block,
    )
    arrived = exchange(message, "z")
    mixed_out = kernel(final_body, shape(rows, block), index, arrived, middle)
    return (mixed_out, new_state)


def solution(mesh):
    fine = Mesh(mesh.devices.reshape(NZ, NX, 4, 2), ("z", "x", "y", "c"))
    ep, tp = ("z", "x"), ("y", "c")
    return jax.shard_map(
        per_device,
        mesh=fine,
        in_specs=(
            P(ep, None),
            P(ep, tp, None, None),
            P(),
            P(ep, tp),
            P(ep, tp),
            P(ep, tp),
            P(),
            P(),
            P(tp),
            P(),
            P(tp, None),
            P(),
            P(ep, None),
            P(ep),
            P(ep, None),
            P(ep, None, tp),
            P(ep, None, tp),
            P(ep, tp, None),
            P(tp, ep),
            P(tp, ep),
            P(ep, tp),
            P(tp),
        ),
        out_specs=(P(ep, tp), P(ep, tp, None, None)),
        check_vma=False,
    )
```

```python
import jax
import jax.numpy as jnp
from jax import lax
from jax.experimental import pallas as pl
from jax.experimental.pallas import tpu as pltpu
from jax.sharding import Mesh, PartitionSpec as P

EPS = 1e-06
BF = jnp.bfloat16
F32 = jnp.float32
NZ, NX, NT = 8, 4, 8
CAP = 3
MIB = 1 << 20


def exchange(tiles, axes):
    return lax.all_to_all(tiles, axes, split_axis=0, concat_axis=0, tiled=True)


def from_neighbours(shard, axis):
    count = lax.axis_size(axis)
    parts = [shard]
    for step in range(1, count):
        pairs = [(source, (source - step) % count) for source in range(count)]
        parts.append(lax.ppermute(shard, axis, pairs))
    return parts


def unit_rows(values):
    return values * lax.rsqrt(jnp.sum(values * values, axis=-1, keepdims=True) + EPS)


def silu(values):
    return values / (1.0 + jnp.exp(-values))


class Late:
    def __init__(self, source, near, done):
        self.near = near
        self.copy = pltpu.make_async_copy(source, near, done)
        self.copy.start()
        self.waits = True

    def arrive(self):
        if self.waits:
            self.copy.wait()
            self.waits = False
        return self.near

    def __getitem__(self, where):
        return self.arrive()[where]

    @property
    def shape(self):
        return self.near.shape


def kernel(
    body, outs, *args, far=(), plain=(), parts=None, far_outs=(), scratch=(), flops=0, limit=16
):
    parts = parts or {}
    far = tuple(far)
    nears = [parts[n][0] if n in parts else args[n].shape for n in far]

    def run(*refs):
        sides = [lax.axis_index(name) for name in ("z", "x", "y", "c")]
        index = (sides[0], sides[1], sides[2] * 2 + sides[3])
        refs = list(refs)
        ins, refs = refs[: len(args)], refs[len(args) :]
        dones = refs.pop() if far else None
        buffers = refs[len(refs) - len(far) :]
        refs = refs[: len(refs) - len(far)]
        for place, number in enumerate(far):
            source = ins[number]
            if number in parts:
                source = parts[number][1](source, index)
            ins[number] = Late(source, buffers[place], dones.at[place])
        body(index, *ins, *refs)
        for number in far:
            ins[number].arrive()

    specs = [
        pl.BlockSpec(memory_space=pltpu.HBM if number in far or number in plain else pltpu.VMEM)
        for number in range(len(args))
    ]
    out_specs = [
        pl.BlockSpec(memory_space=pltpu.HBM if number in far_outs else pltpu.VMEM)
        for number in range(len(outs))
    ]
    scratches = list(scratch) + [pltpu.VMEM(near, args[n].dtype) for n, near in zip(far, nears)]
    if far:
        scratches.append(pltpu.SemaphoreType.DMA((len(far),)))
    return pl.pallas_call(
        run,
        out_shape=outs,
        in_specs=specs,
        out_specs=out_specs,
        scratch_shapes=scratches,
        cost_estimate=pl.CostEstimate(flops=flops, bytes_accessed=0, transcendentals=0),
        compiler_params=pltpu.CompilerParams(vmem_limit_bytes=limit * MIB),
    )(*args)


def wrapped(value, count):
    return jnp.where(value >= count, value - count, value)


def spread_body(index, tokens, gain, query, key, value, out, weights, packed):
    cols = query.shape[1]
    copies = []
    for place, weight in enumerate((query, key, value)):
        target = weights.at[:, place * cols : (place + 1) * cols]
        copies.append(pltpu.make_async_copy(weight, target, packed.at[place]))
        copies[-1].start()
    block = out.shape[2]
    for z in range(NZ):
        cols = slice(z * block, (z + 1) * block)
        out[z] = (tokens[:, cols].astype(F32) * gain[:, cols]).astype(BF)
    for copy in copies:
        copy.wait()


def pack_body(index, after, gate, up, down, out, packed):
    block, size = gate.shape
    half = down.shape[1] // 2
    moves = (
        (gate, out.at[:block, :size]),
        (up, out.at[:block, size:]),
        (down.at[:, :half], out.at[block : block + size, :]),
        (down.at[:, half:], out.at[block + size :, :]),
    )
    copies = [
        pltpu.make_async_copy(source, target, packed.at[place])
        for place, (source, target) in enumerate(moves)
    ]
    for copy in copies:
        copy.start()
    for copy in copies:
        copy.wait()


def turned(row, rows):
    shape = (rows, row.shape[1])
    same = lax.broadcasted_iota(jnp.int32, shape, 0) == lax.broadcasted_iota(jnp.int32, shape, 1)
    return jnp.sum(jnp.where(same, row, 0.0), axis=1, keepdims=True)


def prepare_body(
    index, tokens, gain, decay_weight, beta_weight, rate, ids, prob, logit, meta, factors
):
    rows, width = tokens.shape
    block = meta.shape[1]
    wide = tokens[...].astype(F32)
    row_scale = lax.rsqrt(jnp.sum(wide * wide, axis=1, keepdims=True) / width + EPS)
    gained = (wide * gain[...]).astype(BF)
    over_width = (((1,), (1,)), ((), ()))
    heads = rate.shape[1]
    factor_lane = lax.broadcasted_iota(jnp.int32, factors.shape, 1)
    table = jnp.where(factor_lane == 0, row_scale, 0.0)

    def own_heads(weight):
        product = lax.dot_general(gained, weight[...], over_width, preferred_element_type=F32)
        lane = lax.broadcasted_iota(jnp.int32, product.shape, 1)
        columns = []
        for h in range(heads):
            own = lane == index[2] * heads + h
            columns.append(jnp.sum(jnp.where(own, product, 0.0), axis=1, keepdims=True) * row_scale)
        return columns

    for h, column in enumerate(own_heads(decay_weight)):
        soft = jnp.maximum(column, 0.0) + jnp.log1p(jnp.exp(-jnp.abs(column)))
        table = jnp.where(factor_lane == 1 + h, jnp.exp(-rate[:, h : h + 1] * soft), table)
    for h, column in enumerate(own_heads(beta_weight)):
        table = jnp.where(factor_lane == 1 + heads + h, 1.0 / (1.0 + jnp.exp(-column)), table)
    factors[...] = table

    picks = [ids[k : k + 1, :].astype(F32) for k in range(2)]
    pick_cols = [turned(pick, rows) for pick in picks]
    shape = (rows, rows)
    earlier = lax.broadcasted_iota(jnp.int32, shape, 0) < lax.broadcasted_iota(jnp.int32, shape, 1)
    powers = [jnp.exp(logit[k : k + 1, :]) for k in range(2)]
    total = powers[0] + powers[1]
    lines = []
    for k in range(2):
        named = jnp.zeros(shape, F32)
        for column in pick_cols:
            named = named + jnp.where(earlier & (column == picks[k]), 1.0, 0.0)
        lines.append(picks[k] * CAP + jnp.sum(named, axis=0, keepdims=True))
    for k in range(2):
        route = prob[...] * powers[k] / total
        high = route.astype(BF).astype(F32)
        lines += [high, route - high]
    line = lax.broadcasted_iota(jnp.int32, (8, rows), 0)
    table = jnp.zeros((8, rows), F32)
    for number, values in enumerate(lines):
        table = jnp.where(line == number, values, table)
    shape = (rows, block)
    lane = lax.broadcasted_iota(jnp.int32, shape, 1)
    spot = lane == lax.broadcasted_iota(jnp.int32, shape, 0) + index[0] * rows
    spot = jnp.where(spot, 1.0, 0.0).astype(BF)
    meta[...] = jnp.dot(table.astype(BF), spot, preferred_element_type=F32).astype(BF)


def project_body(index, arrived, w0, w1, w2, w3, out):
    groups, rows, _ = arrived.shape
    total = None
    for step, weight in enumerate((w0, w1, w2, w3)):
        size = weight.shape[0]
        place = pl.multiple_of(wrapped(index[1] + step, NX) * size, size)
        left = arrived[:, :, pl.ds(place, size)].astype(F32).reshape(groups * rows, size).astype(BF)
        part = jnp.dot(left, weight[...], preferred_element_type=F32)
        total = part if total is None else total + part
    out[...] = total.reshape(groups, rows, -1).astype(BF)


def state_body(
    index, arrived, factors, state, head_gain, weight, new_state, out, read, fresh, stored
):
    rows, heads, size = state.shape[:3]
    cols = heads * size
    summed = arrived[0].astype(F32)
    for z in range(1, NZ):
        summed = summed + arrived[z].astype(F32)
    summed = summed * factors[:, 0:1]
    parts = []
    for h in range(heads):
        query = unit_rows(summed[:, h * size : (h + 1) * size]) * size ** (-0.5)
        key = unit_rows(summed[:, cols + h * size : cols + (h + 1) * size])
        value = summed[:, 2 * cols + h * size : 2 * cols + (h + 1) * size]
        both = jnp.sum(query * key, axis=1, keepdims=True)
        parts.append((query.T, key.T, value, both))
    batch = rows // stored.shape[0]
    stores = []
    for b in range(rows):
        for h, (query_cols, key_cols, value, both) in enumerate(parts):
            old = state[b, h]
            key_col = key_cols[:, b : b + 1]
            query_col = query_cols[:, b : b + 1]
            fade = factors[b : b + 1, 1 + h : 2 + h]
            recalled = jnp.sum(key_col * old, axis=0, keepdims=True)
            asked = jnp.sum(query_col * old, axis=0, keepdims=True)
            gate = factors[b : b + 1, 1 + heads + h : 2 + heads + h]
            correction = gate * (value[b : b + 1] - fade * recalled)
            fresh[b, h] = fade * old + key_col * correction
            read[b : b + 1, h * size : (h + 1) * size] = (
                fade * asked + both[b : b + 1] * correction
            )
        if (b + 1) % batch == 0:
            group = pl.ds(b + 1 - batch, batch)
            stores.append(
                pltpu.make_async_copy(fresh.at[group], new_state.at[group], stored.at[b // batch])
            )
            stores[-1].start()
    head_rows = []
    for h in range(heads):
        result = read[:, h * size : (h + 1) * size]
        mean_sq = jnp.mean(result * result, axis=1, keepdims=True)
        head_rows.append(result * lax.rsqrt(mean_sq + EPS) * head_gain[...])
    left = jnp.concatenate(head_rows, axis=1).astype(BF)
    block = out.shape[2]
    for t in range(NT):
        right = weight[:, t * block : (t + 1) * block]
        out[t] = jnp.dot(left, right, preferred_element_type=F32).astype(BF)
    for store in stores:
        store.wait()


def middle_body(index, arrived, tokens, meta, middle, out):
    block = middle.shape[1]
    rows = middle.shape[0]
    summed = arrived[0].astype(F32)
    for t in range(1, NT):
        summed = summed + arrived[t].astype(F32)
    total = tokens[...].astype(F32) + summed
    middle[...] = total
    narrow = total.astype(BF)
    for z in range(NZ):
        out[z, :rows, :] = narrow
        out[z, rows:, :] = meta[...]


def slots_of(route, zi):
    tokens = route.shape[1]
    lane = lax.broadcasted_iota(jnp.int32, (1, tokens), 1)
    source = jnp.zeros((1, tokens), jnp.int32)
    for z in range(1, NZ):
        source = source + jnp.where(lane >= z * (tokens // NZ), 1, 0)
    slots = []
    for k in range(2):
        code = route[k : k + 1, :].astype(jnp.int32) - zi * (NX * CAP)
        expert = jnp.zeros((1, tokens), jnp.int32)
        for x in range(1, NX):
            expert = expert + jnp.where(code >= x * CAP, 1, 0)
        slot = expert * (NZ * CAP) + source * CAP + (code - expert * CAP)
        slots.append(jnp.where((code >= 0) & (code < NX * CAP), slot, -1))
    return slots


def dispatch_body(index, arrived, gain, g0, g1, g2, g3, out, route):
    rows = out.shape[2] - 8
    rows = rows // 3
    tokens = NZ * rows
    block = arrived.shape[2]
    half = block // 2
    wide = arrived[:, :rows, :].astype(F32).reshape(tokens, block)
    narrow = wide.astype(BF)
    routing = arrived[0, rows:, :tokens].astype(F32)
    for z in range(1, NZ):
        routing = routing + arrived[z, rows:, :tokens].astype(F32)
    route[...] = routing
    slot0, slot1 = slots_of(routing, index[0])
    place = lax.broadcasted_iota(jnp.int32, (NX * rows, tokens), 0)
    picks = jnp.where((place == slot0) | (place == slot1), 1.0, 0.0).astype(BF)
    chosen = jnp.dot(picks, narrow, preferred_element_type=F32).astype(BF)
    square = lax.dot_general(
        jnp.ones((8, block), F32),
        wide * wide,
        (((1,), (1,)), ((), ())),
        precision=lax.Precision.HIGHEST,
        preferred_element_type=F32,
    )
    high = square.astype(BF).astype(F32)
    first = lax.broadcasted_iota(jnp.int32, square.shape, 0) == 0
    square = jnp.where(first, high, square - high).astype(BF)
    for x in range(NX):
        own = chosen[x * rows : (x + 1) * rows]
        for t in range(NT):
            out[x, t, :rows, :] = own[:, :half]
            out[x, t, rows : 2 * rows, :] = own[:, half:]
            out[x, t, 3 * rows :, :tokens] = square
            out[x, t, 3 * rows :, tokens:] = jnp.zeros((8, half - tokens), BF)
    scaled = (wide * gain[...]).astype(BF)
    for step, weight in enumerate((g0, g1, g2, g3)):
        part = jnp.dot(scaled, weight[...], preferred_element_type=F32)
        x = wrapped(index[1] + step, NX)
        out[x, :, 2 * rows : 3 * rows, :] = part.reshape(NT, rows, half).astype(BF)


def expert_body(index, arrived, gain, gate, up, down, out):
    rows = out.shape[2]
    block = out.shape[3] - 128
    half = block // 2
    width = gate.shape[0]
    slots = NX * rows
    squares = jnp.zeros((slots, half), F32)
    gate_sum = jnp.zeros((slots, gate.shape[1]), F32)
    up_sum = jnp.zeros((slots, gate.shape[1]), F32)
    for t in range(NT):
        for part in range(2):
            wide = arrived[:, t, part * rows : (part + 1) * rows, :].astype(F32).reshape(slots, half)
            squares = squares + wide * wide
            place = t * block + part * half
            left = (wide * gain[:, place : place + half]).astype(BF)
            gate_sum += jnp.dot(left, gate[place : place + half, :], preferred_element_type=F32)
            up_sum += jnp.dot(left, up[place : place + half, :], preferred_element_type=F32)
    scale = lax.rsqrt(jnp.sum(squares, axis=1, keepdims=True) / width + EPS)
    hidden = (silu(gate_sum * scale) * (up_sum * scale)).astype(BF)
    for t in range(NT):
        result = jnp.dot(hidden, down[:, t * block : (t + 1) * block], preferred_element_type=F32)
        out[:, t, :, :block] = result.reshape(NX, rows, block).astype(BF)
    tokens = NZ * rows
    lane = lax.broadcasted_iota(jnp.int32, (rows, tokens), 1)
    own = lane == lax.broadcasted_iota(jnp.int32, (rows, tokens), 0) + index[2] * rows
    for x in range(NX):
        summed = arrived[x, 0, 2 * rows : 3 * rows, :].astype(F32)
        square = arrived[x, 0, 3 * rows :, :tokens].astype(F32)
        for t in range(1, NT):
            summed = summed + arrived[x, t, 2 * rows : 3 * rows, :].astype(F32)
            square = square + arrived[x, t, 3 * rows :, :tokens].astype(F32)
        square = square[0:1, :] + square[1:2, :]
        square = jnp.sum(jnp.where(own, square, 0.0), axis=1, keepdims=True)
        summed = summed * lax.rsqrt(square / width + EPS)
        result = (silu(summed[:, : half // 2]) * summed[:, half // 2 :]).astype(BF)
        for t in range(NT):
            out[x, t, :, block:] = result


def combine_body(index, arrived, route, d0, d1, d2, d3, mix, out):
    rows = arrived.shape[2]
    block = out.shape[2]
    tokens = NZ * rows
    results = []
    for x in range(NX):
        summed = arrived[x, 0, :, :block].astype(F32)
        for t in range(1, NT):
            summed = summed + arrived[x, t, :, :block].astype(F32)
        results.append(summed)
    results = jnp.concatenate(results, axis=0).astype(BF)
    routing = route[...]
    slot0, slot1 = slots_of(routing, index[0])
    place = lax.broadcasted_iota(jnp.int32, (NX * rows, tokens), 0)
    mixed = jnp.zeros((tokens, block), F32)
    for k in range(2):
        share = jnp.where(place == slot0, routing[2 + k : 3 + k, :], 0.0)
        share = jnp.where(place == slot1, routing[4 + k : 5 + k, :], share).astype(BF)
        mixed += lax.dot_general(
            share, results, (((0,), (0,)), ((), ())), preferred_element_type=F32
        )
    lower = jnp.zeros((tokens, block // 2), F32)
    upper = jnp.zeros((tokens, block // 2), F32)
    for step, weight in enumerate((d0, d1, d2, d3)):
        x = wrapped(index[1] + step, NX)
        left = arrived[x, :, :, block:].astype(F32).reshape(tokens, -1).astype(BF)
        size = left.shape[1]
        lower += jnp.dot(left, weight[:size, :], preferred_element_type=F32)
        upper += jnp.dot(left, weight[size:, :], preferred_element_type=F32)
    gate = 1.0 / (1.0 + jnp.exp(-mix[...]))
    dense = jnp.concatenate((lower, upper), axis=1)
    out[...] = (gate * dense + mixed).reshape(NZ, rows, block).astype(BF)


def final_body(index, arrived, middle, out):
    summed = arrived[0].astype(F32)
    for z in range(1, NZ):
        summed = summed + arrived[z].astype(F32)
    out[...] = (middle[...] + summed).astype(BF)


def per_device(
    tokens,
    delta_state,
    attn_gain,
    query_weight,
    key_weight,
    value_weight,
    decay_weight,
    beta_weight,
    decay_rate,
    head_gain,
    output_weight,
    ffn_gain,
    expert_ids,
    group_prob,
    expert_logit,
    expert_gate,
    expert_up,
    expert_down,
    dense_gate,
    dense_up,
    dense_down,
    dense_mix,
):
    rows, width = tokens.shape
    heads, size = delta_state.shape[1:3]
    cols = heads * size
    block = width // NT
    half = block // 2

    def shape(*dims, dtype=BF):
        return jax.ShapeDtypeStruct(dims, dtype)

    def own_block(ref, index):
        place = pl.multiple_of(index[2] * block, block)
        return ref.at[:, pl.ds(place, block)]

    message, own_weights = kernel(
        spread_body,
        (shape(NZ, rows, block), shape(query_weight.shape[0], 3 * cols)),
        tokens,
        attn_gain[None],
        query_weight,
        key_weight,
        value_weight,
        far=(0, 1),
        plain=(2, 3, 4),
        far_outs=(1,),
        scratch=(pltpu.SemaphoreType.DMA((3,)),),
        limit=63,
    )
    qkv_weights = from_neighbours(own_weights, "x")
    spread = exchange(message, "z")
    meta, factors = kernel(
        prepare_body,
        (shape(8, block), shape(rows, 128, dtype=F32)),
        tokens,
        attn_gain[None],
        decay_weight.T,
        beta_weight.T,
        decay_rate[None],
        expert_ids.T,
        group_prob[None],
        expert_logit.T,
        far=range(8),
        flops=10**8,
        limit=63,
    )
    (part,) = kernel(
        project_body,
        (shape(NZ, rows, 3 * cols),),
        spread,
        *qkv_weights,
        far=range(5),
        flops=2 * NZ * rows * block * 3 * cols,
        limit=63,
    )
    (packed,) = kernel(
        pack_body,
        (shape(block + dense_gate.shape[1] * 2, half),),
        part,
        dense_gate,
        dense_up,
        dense_down,
        plain=(0, 1, 2, 3),
        far_outs=(0,),
        scratch=(pltpu.SemaphoreType.DMA((4,)),),
        limit=63,
    )
    dense_weights = from_neighbours(packed, "x")
    arrived = exchange(part, "z")
    new_state, attn_part = kernel(
        state_body,
        (shape(*delta_state.shape, dtype=F32), shape(NT, rows, block)),
        arrived,
        factors,
        delta_state,
        head_gain[None],
        output_weight,
        far=range(5),
        far_outs=(0,),
        scratch=(
            pltpu.VMEM((rows, cols), F32),
            pltpu.VMEM(delta_state.shape, F32),
            pltpu.SemaphoreType.DMA((3,)),
        ),
        flops=2 * rows * cols * width,
        limit=63,
    )
    arrived = exchange(attn_part, ("y", "c"))
    middle, message = kernel(
        middle_body,
        (shape(rows, block, dtype=F32), shape(NZ, rows + 8, block)),
        arrived,
        tokens,
        meta,
        far=(1, 2),
        parts={1: ((rows, block), own_block)},
    )

    arrived = exchange(message, "z")
    message, route_rows = kernel(
        dispatch_body,
        (shape(NX, NT, 3 * rows + 8, half), shape(8, NZ * rows, dtype=F32)),
        arrived,
        ffn_gain[None],
        *dense_weights,
        far=(1, 2, 3, 4, 5),
        parts={
            1: ((1, block), own_block),
            **{n: ((block, half), lambda ref, index: ref.at[:block]) for n in range(2, 6)},
        },
        flops=2 * NZ * rows * block * 2 * block,
    )
    sides = ("x", "y", "c")
    arrived = exchange(message.reshape(NX * NT, -1, half), sides).reshape(message.shape)
    (message,) = kernel(
        expert_body,
        (shape(NX, NT, rows, block + 128),),
        arrived,
        ffn_gain[None],
        expert_gate[0],
        expert_up[0],
        expert_down[0],
        far=(1,),
        flops=6 * NX * rows * width * 128,
    )
    arrived = exchange(message.reshape(NX * NT, rows, -1), sides).reshape(message.shape)
    (message,) = kernel(
        combine_body,
        (shape(NZ, rows, block),),
        arrived,
        route_rows,
        *dense_weights,
        dense_mix[None],
        far=(1, 2, 3, 4, 5, 6),
        parts={n: ((half, half), lambda ref, index: ref.at[block:]) for n in range(2, 6)},
        flops=2 * NZ * rows * block * block,
    )
    arrived = exchange(message, "z")
    (mixed_out,) = kernel(
        final_body, (shape(rows, block),), arrived, middle, far=(1,)
    )
    return (mixed_out, new_state)


def solution(mesh):
    fine = Mesh(mesh.devices.reshape(NZ, NX, 4, 2), ("z", "x", "y", "c"))
    ep, tp = ("z", "x"), ("y", "c")

    return jax.shard_map(
        per_device,
        mesh=fine,
        in_specs=(
            P(ep, None),
            P(ep, tp, None, None),
            P(),
            P(ep, tp),
            P(ep, tp),
            P(ep, tp),
            P(),
            P(),
            P(tp),
            P(),
            P(tp, None),
            P(),
            P(ep, None),
            P(ep),
            P(ep, None),
            P(ep, None, tp),
            P(ep, None, tp),
            P(ep, tp, None),
            P(tp, ep),
            P(tp, ep),
            P(ep, tp),
            P(tp),
        ),
        out_specs=(P(ep, tp), P(ep, tp, None, None)),
        check_vma=False,
    )
```

```python
import jax
import jax.numpy as jnp
from jax import lax
from jax.experimental import pallas as pl
from jax.experimental.pallas import tpu as pltpu
from jax.sharding import Mesh, PartitionSpec as P

EPS = 1e-06
BF = jnp.bfloat16
F32 = jnp.float32
NZ, NX, NY, NT = 8, 4, 4, 8
CAP = 3
MIB = 1 << 20


def exchange(tiles, axes):
    return lax.all_to_all(tiles, axes, split_axis=0, concat_axis=0, tiled=True)


def from_neighbours(shard, axis):
    count = lax.axis_size(axis)
    parts = [shard]
    for step in range(1, count):
        pairs = [(source, (source - step) % count) for source in range(count)]
        parts.append(lax.ppermute(shard, axis, pairs))
    return parts


def unit_rows(values):
    return values * lax.rsqrt(jnp.sum(values * values, axis=-1, keepdims=True) + EPS)


def silu(values):
    return values / (1.0 + jnp.exp(-values))


class Late:
    def __init__(self, source, near, done):
        self.near = near
        self.copy = pltpu.make_async_copy(source, near, done)
        self.copy.start()
        self.waits = True

    def arrive(self):
        if self.waits:
            self.copy.wait()
            self.waits = False
        return self.near

    def __getitem__(self, where):
        return self.arrive()[where]

    @property
    def shape(self):
        return self.near.shape


def kernel(
    body, outs, *args, far=(), plain=(), parts=None, far_outs=(), scratch=(), flops=0, limit=16
):
    parts = parts or {}
    far, plain = tuple(far), tuple(plain)
    nears = [parts[n][0] if n in parts else args[n].shape for n in far]

    def run(*refs):
        sides = [lax.axis_index(name) for name in ("z", "x", "y", "c")]
        index = (sides[0], sides[1], sides[2] * 2 + sides[3], sides[3])
        refs = list(refs)
        ins, refs = refs[: len(args)], refs[len(args) :]
        dones = refs.pop() if far else None
        buffers = refs[len(refs) - len(far) :]
        refs = refs[: len(refs) - len(far)]
        for place, number in enumerate(far):
            source = ins[number]
            if number in parts:
                source = parts[number][1](source, index)
            ins[number] = Late(source, buffers[place], dones.at[place])
        body(index, *ins, *refs)
        for number in far:
            ins[number].arrive()

    specs = [
        pl.BlockSpec(memory_space=pltpu.HBM if number in far or number in plain else pltpu.VMEM)
        for number in range(len(args))
    ]
    out_specs = [
        pl.BlockSpec(memory_space=pltpu.HBM if number in far_outs else pltpu.VMEM)
        for number in range(len(outs))
    ]
    scratches = list(scratch) + [pltpu.VMEM(near, args[n].dtype) for n, near in zip(far, nears)]
    if far:
        scratches.append(pltpu.SemaphoreType.DMA((len(far),)))
    args = [
        pltpu.with_memory_space_constraint(arg, pltpu.HBM) if n in far or n in plain else arg
        for n, arg in enumerate(args)
    ]
    return pl.pallas_call(
        run,
        out_shape=outs,
        in_specs=specs,
        out_specs=out_specs,
        scratch_shapes=scratches,
        cost_estimate=pl.CostEstimate(flops=flops, bytes_accessed=0, transcendentals=0),
        compiler_params=pltpu.CompilerParams(vmem_limit_bytes=limit * MIB),
    )(*args)


def wrapped(value, count):
    return jnp.where(value >= count, value - count, value)


def join_body(index, query, key, value, out):
    cols = query.shape[1]
    for place, weight in enumerate((query, key, value)):
        out[:, place * cols : (place + 1) * cols] = weight[...]


def spread_body(index, tokens, gain, out):
    block = out.shape[2]
    for z in range(NZ):
        cols = slice(z * block, (z + 1) * block)
        out[z] = (tokens[:, cols].astype(F32) * gain[:, cols]).astype(BF)


def pack_body(index, after, gate, up, down, out):
    block, size = gate.shape
    half = down.shape[1] // 2
    out[:block, :size] = gate[...]
    out[:block, size:] = up[...]
    out[block : block + size, :] = down[:, :half]
    out[block + size :, :] = down[:, half:]


def turned(row, rows):
    shape = (rows, row.shape[1])
    same = lax.broadcasted_iota(jnp.int32, shape, 0) == lax.broadcasted_iota(jnp.int32, shape, 1)
    return jnp.sum(jnp.where(same, row, 0.0), axis=1, keepdims=True)


def prepare_body(
    index, tokens, gain, decay_weight, beta_weight, rate, ids, prob, logit, meta, factors
):
    rows, width = tokens.shape
    block = meta.shape[1]
    wide = tokens[...].astype(F32)
    row_scale = lax.rsqrt(jnp.sum(wide * wide, axis=1, keepdims=True) / width + EPS)
    gained = (wide * gain[...]).astype(BF)
    over_width = (((1,), (1,)), ((), ()))
    heads = rate.shape[1]
    factor_lane = lax.broadcasted_iota(jnp.int32, factors.shape, 1)
    table = jnp.where(factor_lane == 0, row_scale, 0.0)

    def own_heads(weight):
        product = lax.dot_general(gained, weight[...], over_width, preferred_element_type=F32)
        lane = lax.broadcasted_iota(jnp.int32, product.shape, 1)
        columns = []
        for h in range(heads):
            own = lane == index[2] * heads + h
            columns.append(jnp.sum(jnp.where(own, product, 0.0), axis=1, keepdims=True) * row_scale)
        return columns

    for h, column in enumerate(own_heads(decay_weight)):
        soft = jnp.maximum(column, 0.0) + jnp.log1p(jnp.exp(-jnp.abs(column)))
        table = jnp.where(factor_lane == 1 + h, jnp.exp(-rate[:, h : h + 1] * soft), table)
    for h, column in enumerate(own_heads(beta_weight)):
        table = jnp.where(factor_lane == 1 + heads + h, 1.0 / (1.0 + jnp.exp(-column)), table)
    factors[...] = table

    picks = [ids[k : k + 1, :].astype(F32) for k in range(2)]
    pick_cols = [turned(pick, rows) for pick in picks]
    shape = (rows, rows)
    earlier = lax.broadcasted_iota(jnp.int32, shape, 0) < lax.broadcasted_iota(jnp.int32, shape, 1)
    powers = [jnp.exp(logit[k : k + 1, :]) for k in range(2)]
    total = powers[0] + powers[1]
    lines = []
    for k in range(2):
        named = jnp.zeros(shape, F32)
        for column in pick_cols:
            named = named + jnp.where(earlier & (column == picks[k]), 1.0, 0.0)
        lines.append(picks[k] * CAP + jnp.sum(named, axis=0, keepdims=True))
    for k in range(2):
        route = prob[...] * powers[k] / total
        high = route.astype(BF).astype(F32)
        lines += [high, route - high]
    line = lax.broadcasted_iota(jnp.int32, (8, rows), 0)
    table = jnp.zeros((8, rows), F32)
    for number, values in enumerate(lines):
        table = jnp.where(line == number, values, table)
    shape = (rows, block)
    lane = lax.broadcasted_iota(jnp.int32, shape, 1)
    spot = lane == lax.broadcasted_iota(jnp.int32, shape, 0) + index[0] * rows
    spot = jnp.where(spot, 1.0, 0.0).astype(BF)
    meta[...] = jnp.dot(table.astype(BF), spot, preferred_element_type=F32).astype(BF)


def project_body(index, arrived, w0, w1, w2, w3, after, out):
    groups, rows, _ = arrived.shape
    total = None
    for step, weight in enumerate((w0, w1, w2, w3)):
        size = weight.shape[0]
        place = pl.multiple_of(wrapped(index[1] + step, NX) * size, size)
        left = arrived[:, :, pl.ds(place, size)].astype(F32).reshape(groups * rows, size).astype(BF)
        part = jnp.dot(left, weight[...], preferred_element_type=F32)
        total = part if total is None else total + part
    out[...] = total.reshape(groups, rows, -1).astype(BF)


def state_body(
    index, arrived, factors, state, head_gain, weight, new_state, out, read, fresh, stored
):
    rows, heads, size = state.shape[:3]
    cols = heads * size
    summed = arrived[0].astype(F32)
    for z in range(1, NZ):
        summed = summed + arrived[z].astype(F32)
    summed = summed * factors[:, 0:1]
    parts = []
    for h in range(heads):
        query = unit_rows(summed[:, h * size : (h + 1) * size]) * size ** (-0.5)
        key = unit_rows(summed[:, cols + h * size : cols + (h + 1) * size])
        value = summed[:, 2 * cols + h * size : 2 * cols + (h + 1) * size]
        both = jnp.sum(query * key, axis=1, keepdims=True)
        parts.append((query.T, key.T, value, both))
    batch = rows // stored.shape[0]
    stores = []
    for b in range(rows):
        for h, (query_cols, key_cols, value, both) in enumerate(parts):
            old = state[b, h]
            key_col = key_cols[:, b : b + 1]
            query_col = query_cols[:, b : b + 1]
            fade = factors[b : b + 1, 1 + h : 2 + h]
            recalled = jnp.sum(key_col * old, axis=0, keepdims=True)
            asked = jnp.sum(query_col * old, axis=0, keepdims=True)
            gate = factors[b : b + 1, 1 + heads + h : 2 + heads + h]
            correction = gate * (value[b : b + 1] - fade * recalled)
            fresh[b, h] = fade * old + key_col * correction
            read[b : b + 1, h * size : (h + 1) * size] = (
                fade * asked + both[b : b + 1] * correction
            )
        if (b + 1) % batch == 0:
            group = pl.ds(b + 1 - batch, batch)
            stores.append(
                pltpu.make_async_copy(fresh.at[group], new_state.at[group], stored.at[b // batch])
            )
            stores[-1].start()
    head_rows = []
    for h in range(heads):
        result = read[:, h * size : (h + 1) * size]
        mean_sq = jnp.mean(result * result, axis=1, keepdims=True)
        head_rows.append(result * lax.rsqrt(mean_sq + EPS) * head_gain[...])
    left = jnp.concatenate(head_rows, axis=1).astype(BF)
    block = out.shape[2]
    for t in range(NT):
        right = weight[:, t * block : (t + 1) * block]
        out[t] = jnp.dot(left, right, preferred_element_type=F32).astype(BF)
    for store in stores:
        store.wait()


def middle_body(index, arrived, tokens, meta, middle, out):
    block = middle.shape[1]
    rows = middle.shape[0]
    summed = arrived[0].astype(F32)
    for t in range(1, NT):
        summed = summed + arrived[t].astype(F32)
    total = tokens[...].astype(F32) + summed
    middle[...] = total
    narrow = total.astype(BF)
    for z in range(NZ):
        out[z, :rows, :] = narrow
        out[z, rows:, :] = meta[...]


def slots_of(route, zi):
    tokens = route.shape[1]
    lane = lax.broadcasted_iota(jnp.int32, (1, tokens), 1)
    source = jnp.zeros((1, tokens), jnp.int32)
    for z in range(1, NZ):
        source = source + jnp.where(lane >= z * (tokens // NZ), 1, 0)
    slots = []
    for k in range(2):
        code = route[k : k + 1, :].astype(jnp.int32) - zi * (NX * CAP)
        expert = jnp.zeros((1, tokens), jnp.int32)
        for x in range(1, NX):
            expert = expert + jnp.where(code >= x * CAP, 1, 0)
        slot = expert * (NZ * CAP) + source * CAP + (code - expert * CAP)
        slots.append(jnp.where((code >= 0) & (code < NX * CAP), slot, -1))
    return slots


def half_tokens(arrived, gain, core, rows):
    blocks = [arrived[2 * y + core, :rows, :].astype(F32) for y in range(NY)]
    return (jnp.concatenate(blocks, axis=0) * gain[...]).astype(BF)


def away_body(index, arrived, gain, g0, g1, g2, g3, out):
    rows, half = out.shape[2:]
    scaled = half_tokens(arrived, gain, 1 - index[3], rows)
    for step, weight in enumerate((g0, g1, g2, g3)):
        part = jnp.dot(scaled, weight[...], preferred_element_type=F32)
        out[wrapped(index[1] + step, NX)] = part.reshape(NY, rows, half).astype(BF)


def dispatch_body(index, arrived, gain, g0, g1, g2, g3, away, out, route):
    rows = away.shape[2]
    tokens = NZ * rows
    block = arrived.shape[2]
    half = block // 2
    wide = arrived[:, :rows, :].astype(F32).reshape(tokens, block)
    narrow = wide.astype(BF)
    routing = arrived[0, rows:, :tokens].astype(F32)
    for z in range(1, NZ):
        routing = routing + arrived[z, rows:, :tokens].astype(F32)
    route[...] = routing
    slot0, slot1 = slots_of(routing, index[0])
    place = lax.broadcasted_iota(jnp.int32, (NX * rows, tokens), 0)
    picks = jnp.where((place == slot0) | (place == slot1), 1.0, 0.0).astype(BF)
    chosen = jnp.dot(picks, narrow, preferred_element_type=F32).astype(BF)
    square = lax.dot_general(
        jnp.ones((8, block), F32),
        wide * wide,
        (((1,), (1,)), ((), ())),
        precision=lax.Precision.HIGHEST,
        preferred_element_type=F32,
    )
    high = square.astype(BF).astype(F32)
    first = lax.broadcasted_iota(jnp.int32, square.shape, 0) == 0
    square = jnp.where(first, high, square - high).astype(BF)
    for x in range(NX):
        own = chosen[x * rows : (x + 1) * rows]
        for y in range(NY):
            out[x, y, :rows, :] = own[:, :half]
            out[x, y, rows : 2 * rows, :] = own[:, half:]
            out[x, y, 3 * rows :, :tokens] = square
            out[x, y, 3 * rows :, tokens:] = jnp.zeros((8, half - tokens), BF)
    scaled = half_tokens(arrived, gain, index[3], rows)
    for step, weight in enumerate((g0, g1, g2, g3)):
        part = jnp.dot(scaled, weight[...], preferred_element_type=F32).reshape(NY, rows, half)
        x = wrapped(index[1] + step, NX)
        out[x, :, 2 * rows : 3 * rows, :] = (part + away[x].astype(F32)).astype(BF)


def expert_body(index, arrived, partner, gain, gate, up, down, away, hidden, dense):
    rows, block = away.shape[2:]
    half = block // 2
    width = gate.shape[0]
    slots = NX * rows
    squares = jnp.zeros((slots, half), F32)
    gate_sum = jnp.zeros((slots, gate.shape[1]), F32)
    up_sum = jnp.zeros((slots, gate.shape[1]), F32)
    for y in range(NY):
        for source, core in ((arrived, index[3]), (partner, 1 - index[3])):
            for part in range(2):
                wide = source[:, y, part * rows : (part + 1) * rows, :].astype(F32)
                wide = wide.reshape(slots, half)
                squares = squares + wide * wide
                place = pl.multiple_of((2 * y + core) * block + part * half, half)
                left = (wide * gain[:, pl.ds(place, half)]).astype(BF)
                own = pl.ds(place, half)
                gate_sum += jnp.dot(left, gate[own, :], preferred_element_type=F32)
                up_sum += jnp.dot(left, up[own, :], preferred_element_type=F32)
    scale = lax.rsqrt(jnp.sum(squares, axis=1, keepdims=True) / width + EPS)
    result = (silu(gate_sum * scale) * (up_sum * scale)).astype(BF)
    hidden[...] = result
    for y in range(NY):
        place = pl.multiple_of((2 * y + 1 - index[3]) * block, block)
        part = jnp.dot(result, down[:, pl.ds(place, block)], preferred_element_type=F32)
        away[:, y] = part.reshape(NX, rows, block).astype(BF)
    tokens = NZ * rows
    lane = lax.broadcasted_iota(jnp.int32, (rows, tokens), 1)
    own = lane == lax.broadcasted_iota(jnp.int32, (rows, tokens), 0) + index[2] * rows
    for x in range(NX):
        summed = jnp.zeros((rows, half), F32)
        square = jnp.zeros((8, tokens), F32)
        for y in range(NY):
            summed = summed + arrived[x, y, 2 * rows : 3 * rows, :].astype(F32)
            for source in (arrived, partner):
                square = square + source[x, y, 3 * rows :, :tokens].astype(F32)
        square = square[0:1, :] + square[1:2, :]
        square = jnp.sum(jnp.where(own, square, 0.0), axis=1, keepdims=True)
        summed = summed * lax.rsqrt(square / width + EPS)
        dense[x] = (silu(summed[:, : half // 2]) * summed[:, half // 2 :]).astype(BF)


def result_body(index, hidden, dense, away, down, out):
    rows, block = away.shape[2:]
    for y in range(NY):
        place = pl.multiple_of((2 * y + index[3]) * block, block)
        part = jnp.dot(hidden[...], down[:, pl.ds(place, block)], preferred_element_type=F32)
        part = part.reshape(NX, rows, block) + away[:, y].astype(F32)
        out[:, y, :, :block] = part.astype(BF)
        out[:, y, :, block:] = dense[...]


def combine_body(index, arrived, partner, route, d0, d1, d2, d3, mix, out, mixed):
    rows = arrived.shape[2]
    block = out.shape[2]
    tokens = NZ * rows
    results = []
    for x in range(NX):
        summed = arrived[x, 0, :, :block].astype(F32)
        for y in range(1, NY):
            summed = summed + arrived[x, y, :, :block].astype(F32)
        results.append(summed)
    results = jnp.concatenate(results, axis=0).astype(BF)
    routing = route[...]
    slot0, slot1 = slots_of(routing, index[0])
    place = lax.broadcasted_iota(jnp.int32, (NX * rows, tokens), 0)
    total = jnp.zeros((tokens, block), F32)
    for k in range(2):
        share = jnp.where(place == slot0, routing[2 + k : 3 + k, :], 0.0)
        share = jnp.where(place == slot1, routing[4 + k : 5 + k, :], share).astype(BF)
        total += lax.dot_general(
            share, results, (((0,), (0,)), ((), ())), preferred_element_type=F32
        )
    mixed[...] = total.reshape(NZ, rows, block)
    gate = 1.0 / (1.0 + jnp.exp(-mix[...]))
    for source, core in ((arrived, index[3]), (partner, 1 - index[3])):
        lower = jnp.zeros((NY * rows, block // 2), F32)
        upper = jnp.zeros((NY * rows, block // 2), F32)
        for step, weight in enumerate((d0, d1, d2, d3)):
            x = wrapped(index[1] + step, NX)
            left = source[x, :, :, block:].astype(F32).reshape(NY * rows, -1).astype(BF)
            size = left.shape[1]
            lower += jnp.dot(left, weight[:size, :], preferred_element_type=F32)
            upper += jnp.dot(left, weight[size:, :], preferred_element_type=F32)
        dense = gate * jnp.concatenate((lower, upper), axis=1)
        for y in range(NY):
            z = 2 * y + core
            out[z] = (dense[y * rows : (y + 1) * rows] + mixed[z]).astype(BF)


def final_body(index, arrived, middle, out):
    summed = arrived[0].astype(F32)
    for z in range(1, NZ):
        summed = summed + arrived[z].astype(F32)
    out[...] = (middle[...] + summed).astype(BF)


def per_device(
    tokens,
    delta_state,
    attn_gain,
    query_weight,
    key_weight,
    value_weight,
    decay_weight,
    beta_weight,
    decay_rate,
    head_gain,
    output_weight,
    ffn_gain,
    expert_ids,
    group_prob,
    expert_logit,
    expert_gate,
    expert_up,
    expert_down,
    dense_gate,
    dense_up,
    dense_down,
    dense_mix,
):
    rows, width = tokens.shape
    heads, size = delta_state.shape[1:3]
    cols = heads * size
    block = width // NT
    half = block // 2

    def shape(*dims, dtype=BF):
        return jax.ShapeDtypeStruct(dims, dtype)

    def own_block(ref, index):
        place = pl.multiple_of(index[2] * block, block)
        return ref.at[:, pl.ds(place, block)]

    (own_weights,) = kernel(
        join_body,
        (shape(query_weight.shape[0], 3 * cols),),
        query_weight,
        key_weight,
        value_weight,
        far=range(3),
    )
    qkv_weights = from_neighbours(own_weights, "x")

    (message,) = kernel(
        spread_body, (pltpu.HBM((NZ, rows, block), BF),), tokens, attn_gain[None], far=range(2)
    )
    spread = exchange(message, "z")
    meta, factors = kernel(
        prepare_body,
        (shape(8, block), shape(rows, 128, dtype=F32)),
        tokens,
        attn_gain[None],
        decay_weight.T,
        beta_weight.T,
        decay_rate[None],
        expert_ids.T,
        group_prob[None],
        expert_logit.T,
        far=range(8),
        flops=10**8,
    )
    (part,) = kernel(
        project_body,
        (shape(NZ, rows, 3 * cols),),
        spread,
        *qkv_weights,
        factors,
        far=(1, 2, 3, 4),
        plain=(5,),
        flops=2 * NZ * rows * block * 3 * cols,
    )
    (packed,) = kernel(
        pack_body,
        (shape(block + dense_gate.shape[1] * 2, half),),
        part,
        dense_gate,
        dense_up,
        dense_down,
        plain=(0,),
        far=(1, 2, 3),
    )
    dense_weights = from_neighbours(packed, "x")
    arrived = exchange(part, "z")
    new_state, attn_part = kernel(
        state_body,
        (shape(*delta_state.shape, dtype=F32), shape(NT, rows, block)),
        arrived,
        factors,
        delta_state,
        head_gain[None],
        output_weight,
        far=(1, 3, 4),
        far_outs=(0,),
        scratch=(
            pltpu.VMEM((rows, cols), F32),
            pltpu.VMEM(delta_state.shape, F32),
            pltpu.SemaphoreType.DMA((3,)),
        ),
        flops=2 * rows * cols * width,
        limit=24,
    )
    arrived = exchange(attn_part, ("y", "c"))
    middle, message = kernel(
        middle_body,
        (shape(rows, block, dtype=F32), shape(NZ, rows + 8, block)),
        arrived,
        tokens,
        meta,
        far=(1, 2),
        parts={1: ((rows, block), own_block)},
    )

    swap = [(0, 1), (1, 0)]
    arrived = exchange(message, "z")
    gate_up = {
        1: ((1, block), own_block),
        **{n: ((block, half), lambda ref, index: ref.at[:block]) for n in range(2, 6)},
    }
    (away,) = kernel(
        away_body,
        (shape(NX, NY, rows, half),),
        arrived,
        ffn_gain[None],
        *dense_weights,
        far=range(1, 6),
        parts=gate_up,
        flops=NZ * rows * block * 2 * block,
    )
    message, route_rows = kernel(
        dispatch_body,
        (shape(NX, NY, 3 * rows + 8, half), shape(8, NZ * rows, dtype=F32)),
        arrived,
        ffn_gain[None],
        *dense_weights,
        lax.ppermute(away, "c", swap),
        far=range(1, 6),
        parts=gate_up,
        flops=NZ * rows * block * 2 * block,
    )
    sides = ("x", "y")
    arrived = exchange(message.reshape(NX * NY, -1, half), sides)
    partner = lax.ppermute(arrived, "c", swap).reshape(message.shape)
    away, hidden, dense = kernel(
        expert_body,
        (shape(NX, NY, rows, block), shape(NX * rows, 128), shape(NX, rows, 128)),
        arrived.reshape(message.shape),
        partner,
        ffn_gain[None],
        expert_gate[0],
        expert_up[0],
        expert_down[0],
        far=(2,),
        flops=5 * NX * rows * width * 128,
    )
    (message,) = kernel(
        result_body,
        (shape(NX, NY, rows, block + 128),),
        hidden,
        dense,
        lax.ppermute(away, "c", swap),
        expert_down[0],
        flops=NX * rows * width * 128,
    )
    arrived = exchange(message.reshape(NX * NY, rows, -1), sides)
    partner = lax.ppermute(arrived, "c", swap).reshape(message.shape)
    (message,) = kernel(
        combine_body,
        (shape(NZ, rows, block),),
        arrived.reshape(message.shape),
        partner,
        route_rows,
        *dense_weights,
        dense_mix[None],
        far=range(2, 8),
        parts={n: ((half, half), lambda ref, index: ref.at[block:]) for n in range(3, 7)},
        scratch=(pltpu.VMEM((NZ, rows, block), F32),),
        flops=2 * NZ * rows * block * block,
    )
    arrived = exchange(message, "z")
    (mixed_out,) = kernel(
        final_body, (shape(rows, block),), arrived, middle, far=(1,)
    )
    return (mixed_out, new_state)


def solution(mesh):
    fine = Mesh(mesh.devices.reshape(NZ, NX, 4, 2), ("z", "x", "y", "c"))
    ep, tp = ("z", "x"), ("y", "c")

    return jax.shard_map(
        per_device,
        mesh=fine,
        in_specs=(
            P(ep, None),
            P(ep, tp, None, None),
            P(),
            P(ep, tp),
            P(ep, tp),
            P(ep, tp),
            P(),
            P(),
            P(tp),
            P(),
            P(tp, None),
            P(),
            P(ep, None),
            P(ep),
            P(ep, None),
            P(ep, None, tp),
            P(ep, None, tp),
            P(ep, tp, None),
            P(tp, ep),
            P(tp, ep),
            P(ep, tp),
            P(tp),
        ),
        out_specs=(P(ep, tp), P(ep, tp, None, None)),
        check_vma=False,
    )
```

```python
import jax
import jax.numpy as jnp
from jax import lax
from jax.experimental import pallas as pl
from jax.experimental.pallas import tpu as pltpu
from jax.sharding import Mesh, PartitionSpec as P

EPS = 1e-06
BF = jnp.bfloat16
F32 = jnp.float32
NZ, NX, NY, NT = 8, 4, 4, 8
CAP = 3
MIB = 1 << 20


def exchange(tiles, axes):
    return lax.all_to_all(tiles, axes, split_axis=0, concat_axis=0, tiled=True)


def from_neighbours(shard, axis):
    count = lax.axis_size(axis)
    parts = [shard]
    for step in range(1, count):
        pairs = [(source, (source - step) % count) for source in range(count)]
        parts.append(lax.ppermute(shard, axis, pairs))
    return parts


def unit_rows(values):
    return values * lax.rsqrt(jnp.sum(values * values, axis=-1, keepdims=True) + EPS)


def silu(values):
    return values / (1.0 + jnp.exp(-values))


class Late:
    def __init__(self, source, near, done):
        self.near = near
        self.copy = pltpu.make_async_copy(source, near, done)
        self.copy.start()
        self.waits = True

    def arrive(self):
        if self.waits:
            self.copy.wait()
            self.waits = False
        return self.near

    def __getitem__(self, where):
        return self.arrive()[where]

    @property
    def shape(self):
        return self.near.shape


def kernel(
    body, outs, *args, far=(), plain=(), held=(), parts=None, far_outs=(), scratch=(), flops=0, limit=16
):
    parts = parts or {}
    far, plain, held = tuple(far), tuple(plain), tuple(held)
    nears = [parts[n][0] if n in parts else args[n].shape for n in far]

    def run(*refs):
        sides = [lax.axis_index(name) for name in ("z", "x", "y", "c")]
        index = (sides[0], sides[1], sides[2] * 2 + sides[3], sides[3])
        refs = list(refs)
        ins, refs = refs[: len(args)], refs[len(args) :]
        dones = refs.pop() if far else None
        buffers = refs[len(refs) - len(far) :]
        refs = refs[: len(refs) - len(far)]
        for place, number in enumerate(far):
            source = ins[number]
            if number in parts:
                source = parts[number][1](source, index)
            ins[number] = Late(source, buffers[place], dones.at[place])
        body(index, *ins, *refs)
        for number in far:
            ins[number].arrive()

    specs = [
        pl.BlockSpec(memory_space=pltpu.HBM if number in far or number in plain else pltpu.VMEM)
        for number in range(len(args))
    ]
    out_specs = [
        pl.BlockSpec(memory_space=pltpu.HBM if number in far_outs else pltpu.VMEM)
        for number in range(len(outs))
    ]
    scratches = list(scratch) + [pltpu.VMEM(near, args[n].dtype) for n, near in zip(far, nears)]
    if far:
        scratches.append(pltpu.SemaphoreType.DMA((len(far),)))
    args = [
        pltpu.with_memory_space_constraint(arg, pltpu.HBM) if n in far + plain + held else arg
        for n, arg in enumerate(args)
    ]
    return pl.pallas_call(
        run,
        out_shape=outs,
        in_specs=specs,
        out_specs=out_specs,
        scratch_shapes=scratches,
        cost_estimate=pl.CostEstimate(flops=flops, bytes_accessed=0, transcendentals=0),
        compiler_params=pltpu.CompilerParams(vmem_limit_bytes=limit * MIB),
    )(*args)


def wrapped(value, count):
    return jnp.where(value >= count, value - count, value)


def spread_body(index, tokens, gain, query, key, value, out, weights):
    cols = query.shape[1]
    for place, weight in enumerate((query, key, value)):
        weights[:, place * cols : (place + 1) * cols] = weight[...]
    block = out.shape[2]
    for z in range(NZ):
        cols = slice(z * block, (z + 1) * block)
        out[z] = (tokens[:, cols].astype(F32) * gain[:, cols]).astype(BF)


def pack_body(index, after, gate, up, down, out):
    block, size = gate.shape
    half = down.shape[1] // 2
    out[:block, :size] = gate[...]
    out[:block, size:] = up[...]
    out[block : block + size, :] = down[:, :half]
    out[block + size :, :] = down[:, half:]


def turned(row, rows):
    shape = (rows, row.shape[1])
    same = lax.broadcasted_iota(jnp.int32, shape, 0) == lax.broadcasted_iota(jnp.int32, shape, 1)
    return jnp.sum(jnp.where(same, row, 0.0), axis=1, keepdims=True)


def prepare_body(
    index, tokens, gain, decay_weight, beta_weight, rate, ids, prob, logit, meta, factors
):
    rows, width = tokens.shape
    block = meta.shape[1]
    wide = tokens[...].astype(F32)
    row_scale = lax.rsqrt(jnp.sum(wide * wide, axis=1, keepdims=True) / width + EPS)
    gained = (wide * gain[...]).astype(BF)
    over_width = (((1,), (1,)), ((), ()))
    heads = rate.shape[1]
    factor_lane = lax.broadcasted_iota(jnp.int32, factors.shape, 1)
    table = jnp.where(factor_lane == 0, row_scale, 0.0)

    def own_heads(weight):
        product = lax.dot_general(gained, weight[...], over_width, preferred_element_type=F32)
        lane = lax.broadcasted_iota(jnp.int32, product.shape, 1)
        columns = []
        for h in range(heads):
            own = lane == index[2] * heads + h
            columns.append(jnp.sum(jnp.where(own, product, 0.0), axis=1, keepdims=True) * row_scale)
        return columns

    for h, column in enumerate(own_heads(decay_weight)):
        soft = jnp.maximum(column, 0.0) + jnp.log1p(jnp.exp(-jnp.abs(column)))
        table = jnp.where(factor_lane == 1 + h, jnp.exp(-rate[:, h : h + 1] * soft), table)
    for h, column in enumerate(own_heads(beta_weight)):
        table = jnp.where(factor_lane == 1 + heads + h, 1.0 / (1.0 + jnp.exp(-column)), table)
    factors[...] = table

    picks = [ids[k : k + 1, :].astype(F32) for k in range(2)]
    pick_cols = [turned(pick, rows) for pick in picks]
    shape = (rows, rows)
    earlier = lax.broadcasted_iota(jnp.int32, shape, 0) < lax.broadcasted_iota(jnp.int32, shape, 1)
    powers = [jnp.exp(logit[k : k + 1, :]) for k in range(2)]
    total = powers[0] + powers[1]
    lines = []
    for k in range(2):
        named = jnp.zeros(shape, F32)
        for column in pick_cols:
            named = named + jnp.where(earlier & (column == picks[k]), 1.0, 0.0)
        lines.append(picks[k] * CAP + jnp.sum(named, axis=0, keepdims=True))
    for k in range(2):
        route = prob[...] * powers[k] / total
        high = route.astype(BF).astype(F32)
        lines += [high, route - high]
    line = lax.broadcasted_iota(jnp.int32, (8, rows), 0)
    table = jnp.zeros((8, rows), F32)
    for number, values in enumerate(lines):
        table = jnp.where(line == number, values, table)
    shape = (rows, block)
    lane = lax.broadcasted_iota(jnp.int32, shape, 1)
    spot = lane == lax.broadcasted_iota(jnp.int32, shape, 0) + index[0] * rows
    spot = jnp.where(spot, 1.0, 0.0).astype(BF)
    meta[...] = jnp.dot(table.astype(BF), spot, preferred_element_type=F32).astype(BF)


def project_body(index, arrived, w0, w1, w2, w3, after, out):
    groups, rows, _ = arrived.shape
    total = None
    for step, weight in enumerate((w0, w1, w2, w3)):
        size = weight.shape[0]
        place = pl.multiple_of(wrapped(index[1] + step, NX) * size, size)
        left = arrived[:, :, pl.ds(place, size)].astype(F32).reshape(groups * rows, size).astype(BF)
        part = jnp.dot(left, weight[...], preferred_element_type=F32)
        total = part if total is None else total + part
    out[...] = total.reshape(groups, rows, -1).astype(BF)


def recall_body(index, arrived, factors, state, head_gain, weight, out, keys, changes):
    rows, heads, size = state.shape[:3]
    cols = heads * size
    summed = arrived[0].astype(F32)
    for z in range(1, NZ):
        summed = summed + arrived[z].astype(F32)
    summed = summed * factors[:, 0:1]
    line = lax.broadcasted_iota(jnp.int32, (rows, size), 0)
    head_rows = []
    for h in range(heads):
        own = slice(h * size, (h + 1) * size)
        query = unit_rows(summed[:, own]) * size ** (-0.5)
        key = unit_rows(summed[:, cols + h * size : cols + (h + 1) * size])
        value = summed[:, 2 * cols + h * size : 2 * cols + (h + 1) * size]
        both = jnp.concatenate((key, query), axis=0).astype(BF)
        recalled = jnp.zeros((rows, size), F32)
        asked = jnp.zeros((rows, size), F32)
        for b in range(0, rows, 2):
            pair = jnp.concatenate((state[b, h], state[b + 1, h]), axis=1).astype(BF)
            product = jnp.dot(both, pair, preferred_element_type=F32)
            for side in range(2):
                lanes = slice(side * size, (side + 1) * size)
                recalled = jnp.where(line == b + side, product[:rows, lanes], recalled)
                asked = jnp.where(line == b + side, product[rows:, lanes], asked)
        fade = factors[:, 1 + h : 2 + h]
        gate = factors[:, 1 + heads + h : 2 + heads + h]
        change = gate * (value - fade * recalled)
        keys[:, own] = key
        changes[:, own] = change
        result = fade * asked + jnp.sum(query * key, axis=1, keepdims=True) * change
        mean_sq = jnp.mean(result * result, axis=1, keepdims=True)
        head_rows.append(result * lax.rsqrt(mean_sq + EPS) * head_gain[...])
    left = jnp.concatenate(head_rows, axis=1).astype(BF)
    block = out.shape[2]
    for t in range(NT):
        right = weight[:, t * block : (t + 1) * block]
        out[t] = jnp.dot(left, right, preferred_element_type=F32).astype(BF)


def update_body(index, keys, changes, factors, state, new_state):
    rows, heads, size = state.shape[:3]
    line = lax.broadcasted_iota(jnp.int32, (rows, size), 0)
    line = jnp.concatenate((line, line, line), axis=0)
    for h in range(heads):
        own = slice(h * size, (h + 1) * size)
        key, change = keys[:, own], changes[:, own]
        key_high = key.astype(BF).astype(F32)
        high = change.astype(BF).astype(F32)
        left = jnp.concatenate((key_high, key - key_high, key_high), axis=0).T.astype(BF)
        right = jnp.concatenate((high, high, change - high), axis=0)
        for b in range(0, rows, 2):
            pair = [jnp.where(line == b + side, right, 0.0) for side in range(2)]
            pair = jnp.concatenate(pair, axis=1).astype(BF)
            product = jnp.dot(left, pair, preferred_element_type=F32)
            for side in range(2):
                fade = factors[b + side : b + side + 1, 1 + h : 2 + h]
                grown = product[:, side * size : (side + 1) * size]
                new_state[b + side, h] = fade * state[b + side, h] + grown


def middle_body(index, arrived, tokens, meta, middle, out):
    block = middle.shape[1]
    rows = middle.shape[0]
    summed = arrived[0].astype(F32)
    for t in range(1, NT):
        summed = summed + arrived[t].astype(F32)
    place = pl.multiple_of(index[2] * block, block)
    total = tokens[:, pl.ds(place, block)].astype(F32) + summed
    middle[...] = total
    narrow = total.astype(BF)
    for z in range(NZ):
        out[z, :rows, :] = narrow
        out[z, rows:, :] = meta[...]


def slots_of(route, zi):
    tokens = route.shape[1]
    lane = lax.broadcasted_iota(jnp.int32, (1, tokens), 1)
    source = jnp.zeros((1, tokens), jnp.int32)
    for z in range(1, NZ):
        source = source + jnp.where(lane >= z * (tokens // NZ), 1, 0)
    slots = []
    for k in range(2):
        code = route[k : k + 1, :].astype(jnp.int32) - zi * (NX * CAP)
        expert = jnp.zeros((1, tokens), jnp.int32)
        for x in range(1, NX):
            expert = expert + jnp.where(code >= x * CAP, 1, 0)
        slot = expert * (NZ * CAP) + source * CAP + (code - expert * CAP)
        slots.append(jnp.where((code >= 0) & (code < NX * CAP), slot, -1))
    return slots


def half_tokens(arrived, gain, core, rows):
    blocks = [arrived[2 * y + core, :rows, :].astype(F32) for y in range(NY)]
    return (jnp.concatenate(blocks, axis=0) * gain[...]).astype(BF)


def away_body(index, arrived, gain, g0, g1, g2, g3, out):
    rows, half = out.shape[2:]
    scaled = half_tokens(arrived, gain, 1 - index[3], rows)
    for step, weight in enumerate((g0, g1, g2, g3)):
        part = jnp.dot(scaled, weight[: arrived.shape[2], :], preferred_element_type=F32)
        out[wrapped(index[1] + step, NX)] = part.reshape(NY, rows, half).astype(BF)


def dispatch_body(index, arrived, gain, g0, g1, g2, g3, away, out, route):
    rows = away.shape[2]
    tokens = NZ * rows
    block = arrived.shape[2]
    half = block // 2
    wide = arrived[:, :rows, :].astype(F32).reshape(tokens, block)
    narrow = wide.astype(BF)
    routing = arrived[0, rows:, :tokens].astype(F32)
    for z in range(1, NZ):
        routing = routing + arrived[z, rows:, :tokens].astype(F32)
    route[...] = routing
    slot0, slot1 = slots_of(routing, index[0])
    place = lax.broadcasted_iota(jnp.int32, (NX * rows, tokens), 0)
    picks = jnp.where((place == slot0) | (place == slot1), 1.0, 0.0).astype(BF)
    chosen = jnp.dot(picks, narrow, preferred_element_type=F32).astype(BF)
    square = lax.dot_general(
        jnp.ones((8, block), F32),
        wide * wide,
        (((1,), (1,)), ((), ())),
        precision=lax.Precision.HIGHEST,
        preferred_element_type=F32,
    )
    high = square.astype(BF).astype(F32)
    first = lax.broadcasted_iota(jnp.int32, square.shape, 0) == 0
    square = jnp.where(first, high, square - high).astype(BF)
    for x in range(NX):
        own = chosen[x * rows : (x + 1) * rows]
        for y in range(NY):
            out[x, y, :rows, :] = own[:, :half]
            out[x, y, rows : 2 * rows, :] = own[:, half:]
            out[x, y, 3 * rows :, :tokens] = square
            out[x, y, 3 * rows :, tokens:] = jnp.zeros((8, half - tokens), BF)
    scaled = half_tokens(arrived, gain, index[3], rows)
    for step, weight in enumerate((g0, g1, g2, g3)):
        part = jnp.dot(scaled, weight[: arrived.shape[2], :], preferred_element_type=F32).reshape(NY, rows, half)
        x = wrapped(index[1] + step, NX)
        out[x, :, 2 * rows : 3 * rows, :] = (part + away[x].astype(F32)).astype(BF)


def expert_body(index, arrived, partner, gain, gate, up, down, away, hidden, dense):
    rows, block = away.shape[2:]
    half = block // 2
    width = gate.shape[0]
    slots = NX * rows
    squares = jnp.zeros((slots, half), F32)
    gate_sum = jnp.zeros((slots, gate.shape[1]), F32)
    up_sum = jnp.zeros((slots, gate.shape[1]), F32)
    for y in range(NY):
        for source, core in ((arrived, index[3]), (partner, 1 - index[3])):
            for part in range(2):
                wide = source[:, y, part * rows : (part + 1) * rows, :].astype(F32)
                wide = wide.reshape(slots, half)
                squares = squares + wide * wide
                place = pl.multiple_of((2 * y + core) * block + part * half, half)
                left = (wide * gain[:, pl.ds(place, half)]).astype(BF)
                own = pl.ds(place, half)
                gate_sum += jnp.dot(left, gate[own, :], preferred_element_type=F32)
                up_sum += jnp.dot(left, up[own, :], preferred_element_type=F32)
    scale = lax.rsqrt(jnp.sum(squares, axis=1, keepdims=True) / width + EPS)
    result = (silu(gate_sum * scale) * (up_sum * scale)).astype(BF)
    hidden[...] = result
    for y in range(NY):
        place = pl.multiple_of((2 * y + 1 - index[3]) * block, block)
        part = jnp.dot(result, down[:, pl.ds(place, block)], preferred_element_type=F32)
        away[:, y] = part.reshape(NX, rows, block).astype(BF)
    tokens = NZ * rows
    lane = lax.broadcasted_iota(jnp.int32, (rows, tokens), 1)
    own = lane == lax.broadcasted_iota(jnp.int32, (rows, tokens), 0) + index[2] * rows
    for x in range(NX):
        summed = jnp.zeros((rows, half), F32)
        square = jnp.zeros((8, tokens), F32)
        for y in range(NY):
            summed = summed + arrived[x, y, 2 * rows : 3 * rows, :].astype(F32)
            for source in (arrived, partner):
                square = square + source[x, y, 3 * rows :, :tokens].astype(F32)
        square = square[0:1, :] + square[1:2, :]
        square = jnp.sum(jnp.where(own, square, 0.0), axis=1, keepdims=True)
        summed = summed * lax.rsqrt(square / width + EPS)
        dense[x] = (silu(summed[:, : half // 2]) * summed[:, half // 2 :]).astype(BF)


def result_body(index, hidden, dense, away, down, out):
    rows, block = away.shape[2:]
    for y in range(NY):
        place = pl.multiple_of((2 * y + index[3]) * block, block)
        part = jnp.dot(hidden[...], down[:, pl.ds(place, block)], preferred_element_type=F32)
        part = part.reshape(NX, rows, block) + away[:, y].astype(F32)
        out[:, y, :, :block] = part.astype(BF)
        out[:, y, :, block:] = dense[...]


def combine_body(index, arrived, partner, route, d0, d1, d2, d3, mix, out, mixed):
    rows = arrived.shape[2]
    block = out.shape[2]
    tokens = NZ * rows
    results = []
    for x in range(NX):
        summed = arrived[x, 0, :, :block].astype(F32)
        for y in range(1, NY):
            summed = summed + arrived[x, y, :, :block].astype(F32)
        results.append(summed)
    results = jnp.concatenate(results, axis=0).astype(BF)
    routing = route[...]
    slot0, slot1 = slots_of(routing, index[0])
    place = lax.broadcasted_iota(jnp.int32, (NX * rows, tokens), 0)
    total = jnp.zeros((tokens, block), F32)
    for k in range(2):
        share = jnp.where(place == slot0, routing[2 + k : 3 + k, :], 0.0)
        share = jnp.where(place == slot1, routing[4 + k : 5 + k, :], share).astype(BF)
        total += lax.dot_general(
            share, results, (((0,), (0,)), ((), ())), preferred_element_type=F32
        )
    mixed[...] = total.reshape(NZ, rows, block)
    gate = 1.0 / (1.0 + jnp.exp(-mix[...]))
    for source, core in ((arrived, index[3]), (partner, 1 - index[3])):
        lower = jnp.zeros((NY * rows, block // 2), F32)
        upper = jnp.zeros((NY * rows, block // 2), F32)
        for step, weight in enumerate((d0, d1, d2, d3)):
            x = wrapped(index[1] + step, NX)
            left = source[x, :, :, block:].astype(F32).reshape(NY * rows, -1).astype(BF)
            size = left.shape[1]
            lower += jnp.dot(left, weight[block : block + size, :], preferred_element_type=F32)
            upper += jnp.dot(left, weight[block + size :, :], preferred_element_type=F32)
        dense = gate * jnp.concatenate((lower, upper), axis=1)
        for y in range(NY):
            z = 2 * y + core
            out[z] = (dense[y * rows : (y + 1) * rows] + mixed[z]).astype(BF)


def final_body(index, arrived, middle, out):
    summed = arrived[0].astype(F32)
    for z in range(1, NZ):
        summed = summed + arrived[z].astype(F32)
    out[...] = (middle[...] + summed).astype(BF)


def per_device(
    tokens,
    delta_state,
    attn_gain,
    query_weight,
    key_weight,
    value_weight,
    decay_weight,
    beta_weight,
    decay_rate,
    head_gain,
    output_weight,
    ffn_gain,
    expert_ids,
    group_prob,
    expert_logit,
    expert_gate,
    expert_up,
    expert_down,
    dense_gate,
    dense_up,
    dense_down,
    dense_mix,
):
    rows, width = tokens.shape
    heads, size = delta_state.shape[1:3]
    cols = heads * size
    block = width // NT
    half = block // 2

    def shape(*dims, dtype=BF):
        return jax.ShapeDtypeStruct(dims, dtype)

    def own_block(ref, index):
        place = pl.multiple_of(index[2] * block, block)
        return ref.at[:, pl.ds(place, block)]

    message, own_weights = kernel(
        spread_body,
        (pltpu.HBM((NZ, rows, block), BF), shape(query_weight.shape[0], 3 * cols)),
        tokens,
        attn_gain[None],
        query_weight,
        key_weight,
        value_weight,
        far=range(5),
    )
    qkv_weights = from_neighbours(own_weights, "x")
    spread = exchange(message, "z")
    meta, factors = kernel(
        prepare_body,
        (shape(8, block), shape(rows, 128, dtype=F32)),
        tokens,
        attn_gain[None],
        decay_weight.T,
        beta_weight.T,
        decay_rate[None],
        expert_ids.T,
        group_prob[None],
        expert_logit.T,
        far=range(8),
        flops=10**8,
    )
    (part,) = kernel(
        project_body,
        (shape(NZ, rows, 3 * cols),),
        spread,
        *qkv_weights,
        factors,
        held=(1, 2, 3, 4),
        plain=(5,),
        flops=2 * NZ * rows * block * 3 * cols,
    )
    (packed,) = kernel(
        pack_body,
        (shape(block + dense_gate.shape[1] * 2, half),),
        part,
        dense_gate,
        dense_up,
        dense_down,
        plain=(0,),
        far=(1, 2, 3),
    )
    dense_weights = from_neighbours(packed, "x")
    arrived = exchange(part, "z")
    attn_part, keys, changes = kernel(
        recall_body,
        (
            shape(NT, rows, block),
            shape(rows, cols, dtype=F32),
            shape(rows, cols, dtype=F32),
        ),
        arrived,
        factors,
        delta_state,
        head_gain[None],
        output_weight,
        far=(1, 3, 4),
        flops=2 * rows * cols * width,
    )
    (new_state,) = kernel(
        update_body,
        (shape(*delta_state.shape, dtype=F32),),
        keys,
        changes,
        factors,
        delta_state,
        far=range(4),
        flops=10**8,
        limit=24,
    )
    arrived = exchange(attn_part, ("y", "c"))
    middle, message = kernel(
        middle_body,
        (shape(rows, block, dtype=F32), shape(NZ, rows + 8, block)),
        arrived,
        tokens,
        meta,
    )

    swap = [(0, 1), (1, 0)]
    arrived = exchange(message, "z")
    gain_part = {1: ((1, block), own_block)}
    (away,) = kernel(
        away_body,
        (shape(NX, NY, rows, half),),
        arrived,
        ffn_gain[None],
        *dense_weights,
        far=(1,),
        parts=gain_part,
        flops=NZ * rows * block * 2 * block,
    )
    message, route_rows = kernel(
        dispatch_body,
        (shape(NX, NY, 3 * rows + 8, half), shape(8, NZ * rows, dtype=F32)),
        arrived,
        ffn_gain[None],
        *dense_weights,
        lax.ppermute(away, "c", swap),
        far=(1,),
        parts=gain_part,
        flops=NZ * rows * block * 2 * block,
    )
    sides = ("x", "y")
    arrived = exchange(message.reshape(NX * NY, -1, half), sides)
    partner = lax.ppermute(arrived, "c", swap).reshape(message.shape)
    away, hidden, dense = kernel(
        expert_body,
        (shape(NX, NY, rows, block), shape(NX * rows, 128), shape(NX, rows, 128)),
        arrived.reshape(message.shape),
        partner,
        ffn_gain[None],
        expert_gate[0],
        expert_up[0],
        expert_down[0],
        far=(2,),
        flops=5 * NX * rows * width * 128,
    )
    (message,) = kernel(
        result_body,
        (shape(NX, NY, rows, block + 128),),
        hidden,
        dense,
        lax.ppermute(away, "c", swap),
        expert_down[0],
        flops=NX * rows * width * 128,
    )
    arrived = exchange(message.reshape(NX * NY, rows, -1), sides)
    partner = lax.ppermute(arrived, "c", swap).reshape(message.shape)
    (message,) = kernel(
        combine_body,
        (shape(NZ, rows, block),),
        arrived.reshape(message.shape),
        partner,
        route_rows,
        *dense_weights,
        dense_mix[None],
        scratch=(pltpu.VMEM((NZ, rows, block), F32),),
        flops=2 * NZ * rows * block * block,
    )
    arrived = exchange(message, "z")
    (mixed_out,) = kernel(final_body, (shape(rows, block),), arrived, middle)
    return (mixed_out, new_state)


def solution(mesh):
    fine = Mesh(mesh.devices.reshape(NZ, NX, 4, 2), ("z", "x", "y", "c"))
    ep, tp = ("z", "x"), ("y", "c")

    return jax.shard_map(
        per_device,
        mesh=fine,
        in_specs=(
            P(ep, None),
            P(ep, tp, None, None),
            P(),
            P(ep, tp),
            P(ep, tp),
            P(ep, tp),
            P(),
            P(),
            P(tp),
            P(),
            P(tp, None),
            P(),
            P(ep, None),
            P(ep),
            P(ep, None),
            P(ep, None, tp),
            P(ep, None, tp),
            P(ep, tp, None),
            P(tp, ep),
            P(tp, ep),
            P(ep, tp),
            P(tp),
        ),
        out_specs=(P(ep, tp), P(ep, tp, None, None)),
        check_vma=False,
    )
```

```python
import jax
import jax.numpy as jnp
from jax import lax
from jax.experimental import pallas as pl
from jax.experimental.pallas import tpu as pltpu
from jax.sharding import Mesh, PartitionSpec as P

EPS = 1e-06
BF = jnp.bfloat16
F32 = jnp.float32
NZ, NX, NY, NT = 8, 4, 4, 8
CAP = 3
MIB = 1 << 20


def exchange(tiles, axes):
    return lax.all_to_all(tiles, axes, split_axis=0, concat_axis=0, tiled=True)


def from_neighbours(shard, axis):
    count = lax.axis_size(axis)
    parts = [shard]
    for step in range(1, count):
        pairs = [(source, (source - step) % count) for source in range(count)]
        parts.append(lax.ppermute(shard, axis, pairs))
    return parts


def unit_rows(values):
    return values * lax.rsqrt(jnp.sum(values * values, axis=-1, keepdims=True) + EPS)


def silu(values):
    return values / (1.0 + jnp.exp(-values))


class Late:
    def __init__(self, source, near, done):
        self.near = near
        self.copy = pltpu.make_async_copy(source, near, done)
        self.copy.start()
        self.waits = True

    def arrive(self):
        if self.waits:
            self.copy.wait()
            self.waits = False
        return self.near

    def __getitem__(self, where):
        return self.arrive()[where]

    @property
    def shape(self):
        return self.near.shape


def kernel(
    body, outs, *args, far=(), plain=(), held=(), parts=None, far_outs=(), scratch=(), flops=0, limit=16
):
    parts = parts or {}
    far, plain, held = tuple(far), tuple(plain), tuple(held)
    nears = [parts[n][0] if n in parts else args[n].shape for n in far]

    def run(*refs):
        sides = [lax.axis_index(name) for name in ("z", "x", "y", "c")]
        index = (sides[0], sides[1], sides[2] * 2 + sides[3], sides[3])
        refs = list(refs)
        ins, refs = refs[: len(args)], refs[len(args) :]
        dones = refs.pop() if far else None
        buffers = refs[len(refs) - len(far) :]
        refs = refs[: len(refs) - len(far)]
        for place, number in enumerate(far):
            source = ins[number]
            if number in parts:
                source = parts[number][1](source, index)
            ins[number] = Late(source, buffers[place], dones.at[place])
        body(index, *ins, *refs)
        for number in far:
            ins[number].arrive()

    specs = [
        pl.BlockSpec(memory_space=pltpu.HBM if number in far or number in plain else pltpu.VMEM)
        for number in range(len(args))
    ]
    out_specs = [
        pl.BlockSpec(memory_space=pltpu.HBM if number in far_outs else pltpu.VMEM)
        for number in range(len(outs))
    ]
    scratches = list(scratch) + [pltpu.VMEM(near, args[n].dtype) for n, near in zip(far, nears)]
    if far:
        scratches.append(pltpu.SemaphoreType.DMA((len(far),)))
    args = [
        pltpu.with_memory_space_constraint(arg, pltpu.HBM) if n in far + plain + held else arg
        for n, arg in enumerate(args)
    ]
    return pl.pallas_call(
        run,
        out_shape=outs,
        in_specs=specs,
        out_specs=out_specs,
        scratch_shapes=scratches,
        cost_estimate=pl.CostEstimate(flops=flops, bytes_accessed=0, transcendentals=0),
        compiler_params=pltpu.CompilerParams(vmem_limit_bytes=limit * MIB),
    )(*args)


def wrapped(value, count):
    return jnp.where(value >= count, value - count, value)


def spread_body(index, tokens, gain, query, key, value, out, weights):
    cols = query.shape[1]
    for place, weight in enumerate((query, key, value)):
        weights[:, place * cols : (place + 1) * cols] = weight[...]
    block = out.shape[2]
    for z in range(NZ):
        cols = slice(z * block, (z + 1) * block)
        out[z] = (tokens[:, cols].astype(F32) * gain[:, cols]).astype(BF)


def pack_body(index, after, gate, up, down, out):
    block, size = gate.shape
    half = down.shape[1] // 2
    out[:block, :size] = gate[...]
    out[:block, size:] = up[...]
    out[block : block + size, :] = down[:, :half]
    out[block + size :, :] = down[:, half:]


def turned(row, rows):
    shape = (rows, row.shape[1])
    same = lax.broadcasted_iota(jnp.int32, shape, 0) == lax.broadcasted_iota(jnp.int32, shape, 1)
    return jnp.sum(jnp.where(same, row, 0.0), axis=1, keepdims=True)


def prepare_body(
    index, tokens, gain, decay_weight, beta_weight, rate, ids, prob, logit, meta, factors
):
    rows, width = tokens.shape
    block = meta.shape[1]
    wide = tokens[...].astype(F32)
    row_scale = lax.rsqrt(jnp.sum(wide * wide, axis=1, keepdims=True) / width + EPS)
    gained = (wide * gain[...]).astype(BF)
    over_width = (((1,), (1,)), ((), ()))
    heads = rate.shape[1]
    factor_lane = lax.broadcasted_iota(jnp.int32, factors.shape, 1)
    table = jnp.where(factor_lane == 0, row_scale, 0.0)

    def own_heads(weight):
        product = lax.dot_general(gained, weight[...], over_width, preferred_element_type=F32)
        lane = lax.broadcasted_iota(jnp.int32, product.shape, 1)
        columns = []
        for h in range(heads):
            own = lane == index[2] * heads + h
            columns.append(jnp.sum(jnp.where(own, product, 0.0), axis=1, keepdims=True) * row_scale)
        return columns

    for h, column in enumerate(own_heads(decay_weight)):
        soft = jnp.maximum(column, 0.0) + jnp.log1p(jnp.exp(-jnp.abs(column)))
        table = jnp.where(factor_lane == 1 + h, jnp.exp(-rate[:, h : h + 1] * soft), table)
    for h, column in enumerate(own_heads(beta_weight)):
        table = jnp.where(factor_lane == 1 + heads + h, 1.0 / (1.0 + jnp.exp(-column)), table)
    factors[...] = table

    picks = [ids[k : k + 1, :].astype(F32) for k in range(2)]
    pick_cols = [turned(pick, rows) for pick in picks]
    shape = (rows, rows)
    earlier = lax.broadcasted_iota(jnp.int32, shape, 0) < lax.broadcasted_iota(jnp.int32, shape, 1)
    powers = [jnp.exp(logit[k : k + 1, :]) for k in range(2)]
    total = powers[0] + powers[1]
    lines = []
    for k in range(2):
        named = jnp.zeros(shape, F32)
        for column in pick_cols:
            named = named + jnp.where(earlier & (column == picks[k]), 1.0, 0.0)
        lines.append(picks[k] * CAP + jnp.sum(named, axis=0, keepdims=True))
    for k in range(2):
        route = prob[...] * powers[k] / total
        high = route.astype(BF).astype(F32)
        lines += [high, route - high]
    line = lax.broadcasted_iota(jnp.int32, (8, rows), 0)
    table = jnp.zeros((8, rows), F32)
    for number, values in enumerate(lines):
        table = jnp.where(line == number, values, table)
    shape = (rows, block)
    lane = lax.broadcasted_iota(jnp.int32, shape, 1)
    spot = lane == lax.broadcasted_iota(jnp.int32, shape, 0) + index[0] * rows
    spot = jnp.where(spot, 1.0, 0.0).astype(BF)
    meta[...] = jnp.dot(table.astype(BF), spot, preferred_element_type=F32).astype(BF)


def project_body(index, arrived, w0, w1, w2, w3, after, out):
    groups, rows, _ = arrived.shape
    total = None
    for step, weight in enumerate((w0, w1, w2, w3)):
        size = weight.shape[0]
        place = pl.multiple_of(wrapped(index[1] + step, NX) * size, size)
        left = arrived[:, :, pl.ds(place, size)].astype(F32).reshape(groups * rows, size).astype(BF)
        part = jnp.dot(left, weight[...], preferred_element_type=F32)
        total = part if total is None else total + part
    out[...] = total.reshape(groups, rows, -1).astype(BF)


def recall_body(index, arrived, factors, state, head_gain, weight, out, keys, changes):
    rows, heads, size = state.shape[:3]
    cols = heads * size
    summed = arrived[0].astype(F32)
    for z in range(1, NZ):
        summed = summed + arrived[z].astype(F32)
    summed = summed * factors[:, 0:1]
    line = lax.broadcasted_iota(jnp.int32, (rows, size), 0)
    head_rows = []
    for h in range(heads):
        own = slice(h * size, (h + 1) * size)
        query = unit_rows(summed[:, own]) * size ** (-0.5)
        key = unit_rows(summed[:, cols + h * size : cols + (h + 1) * size])
        value = summed[:, 2 * cols + h * size : 2 * cols + (h + 1) * size]
        both = jnp.concatenate((key, query), axis=0).astype(BF)
        recalled = jnp.zeros((rows, size), F32)
        asked = jnp.zeros((rows, size), F32)
        for b in range(0, rows, 2):
            pair = jnp.concatenate((state[b, h], state[b + 1, h]), axis=1).astype(BF)
            product = jnp.dot(both, pair, preferred_element_type=F32)
            for side in range(2):
                lanes = slice(side * size, (side + 1) * size)
                recalled = jnp.where(line == b + side, product[:rows, lanes], recalled)
                asked = jnp.where(line == b + side, product[rows:, lanes], asked)
        fade = factors[:, 1 + h : 2 + h]
        gate = factors[:, 1 + heads + h : 2 + heads + h]
        change = gate * (value - fade * recalled)
        keys[:, own] = key
        changes[:, own] = change
        result = fade * asked + jnp.sum(query * key, axis=1, keepdims=True) * change
        mean_sq = jnp.mean(result * result, axis=1, keepdims=True)
        head_rows.append(result * lax.rsqrt(mean_sq + EPS) * head_gain[...])
    left = jnp.concatenate(head_rows, axis=1).astype(BF)
    block = out.shape[2]
    for t in range(NT):
        right = weight[:, t * block : (t + 1) * block]
        out[t] = jnp.dot(left, right, preferred_element_type=F32).astype(BF)


def update_body(index, keys, changes, factors, state, new_state):
    rows, heads, size = state.shape[:3]
    line = lax.broadcasted_iota(jnp.int32, (rows, size), 0)
    line = jnp.concatenate((line, line, line), axis=0)
    for h in range(heads):
        own = slice(h * size, (h + 1) * size)
        key, change = keys[:, own], changes[:, own]
        key_high = key.astype(BF).astype(F32)
        high = change.astype(BF).astype(F32)
        left = jnp.concatenate((key_high, key - key_high, key_high), axis=0).T.astype(BF)
        right = jnp.concatenate((high, high, change - high), axis=0)
        for b in range(0, rows, 2):
            pair = [jnp.where(line == b + side, right, 0.0) for side in range(2)]
            pair = jnp.concatenate(pair, axis=1).astype(BF)
            product = jnp.dot(left, pair, preferred_element_type=F32)
            for side in range(2):
                fade = factors[b + side : b + side + 1, 1 + h : 2 + h]
                grown = product[:, side * size : (side + 1) * size]
                new_state[b + side, h] = fade * state[b + side, h] + grown


def middle_body(index, arrived, tokens, meta, middle, out):
    block = middle.shape[1]
    rows = middle.shape[0]
    summed = arrived[0].astype(F32)
    for t in range(1, NT):
        summed = summed + arrived[t].astype(F32)
    place = pl.multiple_of(index[2] * block, block)
    total = tokens[:, pl.ds(place, block)].astype(F32) + summed
    middle[...] = total
    narrow = total.astype(BF)
    for z in range(NZ):
        out[z, :rows, :] = narrow
        out[z, rows:, :] = meta[...]


def slots_of(route, zi):
    tokens = route.shape[1]
    lane = lax.broadcasted_iota(jnp.int32, (1, tokens), 1)
    source = jnp.zeros((1, tokens), jnp.int32)
    for z in range(1, NZ):
        source = source + jnp.where(lane >= z * (tokens // NZ), 1, 0)
    slots = []
    for k in range(2):
        code = route[k : k + 1, :].astype(jnp.int32) - zi * (NX * CAP)
        expert = jnp.zeros((1, tokens), jnp.int32)
        for x in range(1, NX):
            expert = expert + jnp.where(code >= x * CAP, 1, 0)
        slot = expert * (NZ * CAP) + source * CAP + (code - expert * CAP)
        slots.append(jnp.where((code >= 0) & (code < NX * CAP), slot, -1))
    return slots


def dispatch_body(index, arrived, gain, g0, g1, g2, g3, after, out, route):
    rows = arrived.shape[1] - 8
    tokens = NZ * rows
    block = arrived.shape[2]
    half = block // 2
    wide = arrived[:, :rows, :].astype(F32).reshape(tokens, block)
    narrow = wide.astype(BF)
    routing = arrived[0, rows:, :tokens].astype(F32)
    for z in range(1, NZ):
        routing = routing + arrived[z, rows:, :tokens].astype(F32)
    route[...] = routing
    slot0, slot1 = slots_of(routing, index[0])
    place = lax.broadcasted_iota(jnp.int32, (NX * rows, tokens), 0)
    picks = jnp.where((place == slot0) | (place == slot1), 1.0, 0.0).astype(BF)
    chosen = jnp.dot(picks, narrow, preferred_element_type=F32).astype(BF)
    square = lax.dot_general(
        jnp.ones((8, block), F32),
        wide * wide,
        (((1,), (1,)), ((), ())),
        precision=lax.Precision.HIGHEST,
        preferred_element_type=F32,
    )
    high = square.astype(BF).astype(F32)
    first = lax.broadcasted_iota(jnp.int32, square.shape, 0) == 0
    square = jnp.where(first, high, square - high).astype(BF)
    for x in range(NX):
        own = chosen[x * rows : (x + 1) * rows]
        for y in range(NY):
            out[x, y, :rows, :] = own[:, :half]
            out[x, y, rows : 2 * rows, :] = own[:, half:]
            out[x, y, 4 * rows :, :tokens] = square
            out[x, y, 4 * rows :, tokens:] = jnp.zeros((8, half - tokens), BF)
    scaled = (wide * gain[...]).astype(BF)
    for step, weight in enumerate((g0, g1, g2, g3)):
        part = jnp.dot(scaled, weight[...], preferred_element_type=F32)
        x = wrapped(index[1] + step, NX)
        out[x, :, 2 * rows : 4 * rows, :] = part.reshape(NY, 2 * rows, half).astype(BF)


def expert_body(index, arrived, partner, gain, gate, up, down, away, hidden, dense):
    rows, block = away.shape[2:]
    size = gate.shape[1]
    half = block // 2
    width = gate.shape[0]
    slots = NX * rows
    squares = jnp.zeros((slots, half), F32)
    gate_sum = jnp.zeros((slots, gate.shape[1]), F32)
    up_sum = jnp.zeros((slots, gate.shape[1]), F32)
    for y in range(NY):
        for source, core in ((arrived, index[3]), (partner, 1 - index[3])):
            for part in range(2):
                wide = source[:, y, part * rows : (part + 1) * rows, :].astype(F32)
                wide = wide.reshape(slots, half)
                squares = squares + wide * wide
                place = pl.multiple_of((2 * y + core) * block + part * half, half)
                left = (wide * gain[:, pl.ds(place, half)]).astype(BF)
                own = pl.ds(place, half)
                gate_sum += jnp.dot(left, gate[own, :], preferred_element_type=F32)
                up_sum += jnp.dot(left, up[own, :], preferred_element_type=F32)
    scale = lax.rsqrt(jnp.sum(squares, axis=1, keepdims=True) / width + EPS)
    result = (silu(gate_sum * scale) * (up_sum * scale)).astype(BF)
    hidden[...] = result
    for y in range(NY):
        place = pl.multiple_of((2 * y + 1 - index[3]) * block, block)
        part = jnp.dot(result, down[:, pl.ds(place, block)], preferred_element_type=F32)
        away[:, y] = part.reshape(NX, rows, block).astype(BF)
    tokens = NZ * rows
    lane = lax.broadcasted_iota(jnp.int32, (rows, tokens), 1)
    own = lane == lax.broadcasted_iota(jnp.int32, (rows, tokens), 0) + index[2] * rows
    for x in range(NX):
        summed = jnp.zeros((rows, half), F32)
        square = jnp.zeros((8, tokens), F32)
        for y in range(NY):
            for source in (arrived, partner):
                both = source[x, y, 2 * rows : 4 * rows, :].astype(F32)
                summed = summed + jnp.where(index[3] == 0, both[:rows], both[rows:])
                square = square + source[x, y, 4 * rows :, :tokens].astype(F32)
        square = square[0:1, :] + square[1:2, :]
        square = jnp.sum(jnp.where(own, square, 0.0), axis=1, keepdims=True)
        summed = summed * lax.rsqrt(square / width + EPS)
        result = (silu(summed[:, : half // 2]) * summed[:, half // 2 :]).astype(BF)
        dense[x] = result
        away[x, NY, :, :size] = result
        away[x, NY, :, size:] = jnp.zeros((rows, block - size), BF)


def result_body(index, hidden, dense, away, down, out):
    rows, block = away.shape[2:]
    size = dense.shape[2]
    own_place = pl.multiple_of(block + index[3] * size, size)
    far_place = pl.multiple_of(block + (1 - index[3]) * size, size)
    for y in range(NY):
        place = pl.multiple_of((2 * y + index[3]) * block, block)
        part = jnp.dot(hidden[...], down[:, pl.ds(place, block)], preferred_element_type=F32)
        part = part.reshape(NX, rows, block) + away[:, y].astype(F32)
        out[:, y, :, :block] = part.astype(BF)
        out[:, y, :, pl.ds(own_place, size)] = dense[...]
        out[:, y, :, pl.ds(far_place, size)] = away[:, NY, :, :size]


def combine_body(index, arrived, route, d0, d1, d2, d3, mix, out):
    rows = arrived.shape[2]
    block = out.shape[2]
    tokens = NZ * rows
    results = []
    for x in range(NX):
        summed = arrived[x, 0, :, :block].astype(F32)
        for y in range(1, NY):
            summed = summed + arrived[x, y, :, :block].astype(F32)
        results.append(summed)
    results = jnp.concatenate(results, axis=0).astype(BF)
    routing = route[...]
    slot0, slot1 = slots_of(routing, index[0])
    place = lax.broadcasted_iota(jnp.int32, (NX * rows, tokens), 0)
    total = jnp.zeros((tokens, block), F32)
    for k in range(2):
        share = jnp.where(place == slot0, routing[2 + k : 3 + k, :], 0.0)
        share = jnp.where(place == slot1, routing[4 + k : 5 + k, :], share).astype(BF)
        total += lax.dot_general(
            share, results, (((0,), (0,)), ((), ())), preferred_element_type=F32
        )
    gate = 1.0 / (1.0 + jnp.exp(-mix[...]))
    total = total.reshape(NY, 2, rows, block)
    size = (arrived.shape[3] - block) // 2
    for core in range(2):
        lower = jnp.zeros((NY * rows, block // 2), F32)
        upper = jnp.zeros((NY * rows, block // 2), F32)
        lanes = slice(block + core * size, block + (core + 1) * size)
        for step, weight in enumerate((d0, d1, d2, d3)):
            x = wrapped(index[1] + step, NX)
            left = arrived[x, :, :, lanes].astype(F32).reshape(NY * rows, size).astype(BF)
            lower += jnp.dot(left, weight[:size, :], preferred_element_type=F32)
            upper += jnp.dot(left, weight[size:, :], preferred_element_type=F32)
        dense = gate * jnp.concatenate((lower, upper), axis=1)
        for y in range(NY):
            own = dense[y * rows : (y + 1) * rows] + total[y, core]
            out[2 * y + core] = own.astype(BF)


def final_body(index, arrived, middle, out):
    summed = arrived[0].astype(F32)
    for z in range(1, NZ):
        summed = summed + arrived[z].astype(F32)
    out[...] = (middle[...] + summed).astype(BF)


def per_device(
    tokens,
    delta_state,
    attn_gain,
    query_weight,
    key_weight,
    value_weight,
    decay_weight,
    beta_weight,
    decay_rate,
    head_gain,
    output_weight,
    ffn_gain,
    expert_ids,
    group_prob,
    expert_logit,
    expert_gate,
    expert_up,
    expert_down,
    dense_gate,
    dense_up,
    dense_down,
    dense_mix,
):
    rows, width = tokens.shape
    heads, size = delta_state.shape[1:3]
    cols = heads * size
    block = width // NT
    half = block // 2

    def shape(*dims, dtype=BF):
        return jax.ShapeDtypeStruct(dims, dtype)

    def own_block(ref, index):
        place = pl.multiple_of(index[2] * block, block)
        return ref.at[:, pl.ds(place, block)]

    message, own_weights = kernel(
        spread_body,
        (pltpu.HBM((NZ, rows, block), BF), shape(query_weight.shape[0], 3 * cols)),
        tokens,
        attn_gain[None],
        query_weight,
        key_weight,
        value_weight,
        far=range(5),
    )
    qkv_weights = from_neighbours(own_weights, "x")
    spread = exchange(message, "z")
    meta, factors = kernel(
        prepare_body,
        (shape(8, block), shape(rows, 128, dtype=F32)),
        tokens,
        attn_gain[None],
        decay_weight.T,
        beta_weight.T,
        decay_rate[None],
        expert_ids.T,
        group_prob[None],
        expert_logit.T,
        far=range(8),
        flops=10**8,
    )
    (part,) = kernel(
        project_body,
        (shape(NZ, rows, 3 * cols),),
        spread,
        *qkv_weights,
        factors,
        held=(1, 2, 3, 4),
        plain=(5,),
        flops=2 * NZ * rows * block * 3 * cols,
    )
    (packed,) = kernel(
        pack_body,
        (shape(block + dense_gate.shape[1] * 2, half),),
        part,
        dense_gate,
        dense_up,
        dense_down,
        plain=(0,),
        far=(1, 2, 3),
    )
    dense_weights = from_neighbours(packed, "x")
    arrived = exchange(part, "z")
    attn_part, keys, changes = kernel(
        recall_body,
        (
            shape(NT, rows, block),
            shape(rows, cols, dtype=F32),
            shape(rows, cols, dtype=F32),
        ),
        arrived,
        factors,
        delta_state,
        head_gain[None],
        output_weight,
        far=(1, 3, 4),
        flops=2 * rows * cols * width,
    )
    (new_state,) = kernel(
        update_body,
        (shape(*delta_state.shape, dtype=F32),),
        keys,
        changes,
        factors,
        delta_state,
        far=range(4),
        flops=10**8,
        limit=24,
    )
    arrived = exchange(attn_part, ("y", "c"))
    middle, message = kernel(
        middle_body,
        (shape(rows, block, dtype=F32), shape(NZ, rows + 8, block)),
        arrived,
        tokens,
        meta,
    )

    swap = [(0, 1), (1, 0)]
    arrived = exchange(message, "z")
    message, route_rows = kernel(
        dispatch_body,
        (shape(NX, NY, 4 * rows + 8, half), shape(8, NZ * rows, dtype=F32)),
        arrived,
        ffn_gain[None],
        *dense_weights,
        new_state,
        far=range(1, 6),
        plain=(6,),
        parts={
            1: ((1, block), own_block),
            **{n: ((block, half), lambda ref, index: ref.at[:block]) for n in range(2, 6)},
        },
        flops=2 * NZ * rows * block * 2 * block,
    )
    sides = ("x", "y")
    arrived = exchange(message.reshape(NX * NY, -1, half), sides)
    partner = lax.ppermute(arrived, "c", swap).reshape(message.shape)
    away, hidden, dense = kernel(
        expert_body,
        (shape(NX, NY + 1, rows, block), shape(NX * rows, 128), shape(NX, rows, 128)),
        arrived.reshape(message.shape),
        partner,
        ffn_gain[None],
        expert_gate[0],
        expert_up[0],
        expert_down[0],
        far=(2,),
        flops=5 * NX * rows * width * 128,
    )
    (message,) = kernel(
        result_body,
        (shape(NX, NY, rows, block + 2 * 128),),
        hidden,
        dense,
        lax.ppermute(away, "c", swap),
        expert_down[0],
        flops=NX * rows * width * 128,
    )
    arrived = exchange(message.reshape(NX * NY, rows, -1), sides)
    (message,) = kernel(
        combine_body,
        (shape(NZ, rows, block),),
        arrived.reshape(message.shape),
        route_rows,
        *dense_weights,
        dense_mix[None],
        far=range(1, 7),
        parts={n: ((half, half), lambda ref, index: ref.at[block:]) for n in range(2, 6)},
        flops=2 * NZ * rows * block * block,
    )
    arrived = exchange(message, "z")
    (mixed_out,) = kernel(final_body, (shape(rows, block),), arrived, middle)
    return (mixed_out, new_state)


def solution(mesh):
    fine = Mesh(mesh.devices.reshape(NZ, NX, 4, 2), ("z", "x", "y", "c"))
    ep, tp = ("z", "x"), ("y", "c")

    return jax.shard_map(
        per_device,
        mesh=fine,
        in_specs=(
            P(ep, None),
            P(ep, tp, None, None),
            P(),
            P(ep, tp),
            P(ep, tp),
            P(ep, tp),
            P(),
            P(),
            P(tp),
            P(),
            P(tp, None),
            P(),
            P(ep, None),
            P(ep),
            P(ep, None),
            P(ep, None, tp),
            P(ep, None, tp),
            P(ep, tp, None),
            P(tp, ep),
            P(tp, ep),
            P(ep, tp),
            P(tp),
        ),
        out_specs=(P(ep, tp), P(ep, tp, None, None)),
        check_vma=False,
    )
```

```python
import jax
import jax.numpy as jnp
from jax import lax
from jax.experimental import pallas as pl
from jax.experimental.pallas import tpu as pltpu
from jax.sharding import Mesh, PartitionSpec as P

EPS = 1e-06
BF = jnp.bfloat16
F32 = jnp.float32
NZ, NX, NY, NT = 8, 4, 4, 8
CAP = 3
MIB = 1 << 20


def exchange(tiles, axes):
    return lax.all_to_all(tiles, axes, split_axis=0, concat_axis=0, tiled=True)


def from_neighbours(shard, axis):
    count = lax.axis_size(axis)
    parts = [shard]
    for step in range(1, count):
        pairs = [(source, (source - step) % count) for source in range(count)]
        parts.append(lax.ppermute(shard, axis, pairs))
    return parts


def unit_rows(values):
    return values * lax.rsqrt(jnp.sum(values * values, axis=-1, keepdims=True) + EPS)


def silu(values):
    return values / (1.0 + jnp.exp(-values))


class Late:
    def __init__(self, source, near, done):
        self.near = near
        self.copy = pltpu.make_async_copy(source, near, done)
        self.copy.start()
        self.waits = True

    def arrive(self):
        if self.waits:
            self.copy.wait()
            self.waits = False
        return self.near

    def __getitem__(self, where):
        return self.arrive()[where]

    @property
    def shape(self):
        return self.near.shape


def kernel(
    body, outs, *args, far=(), plain=(), held=(), parts=None, far_outs=(), scratch=(), flops=0, limit=16
):
    parts = parts or {}
    far, plain, held = tuple(far), tuple(plain), tuple(held)
    nears = [parts[n][0] if n in parts else args[n].shape for n in far]

    def run(*refs):
        sides = [lax.axis_index(name) for name in ("z", "x", "y", "c")]
        index = (sides[0], sides[1], sides[2] * 2 + sides[3], sides[3])
        refs = list(refs)
        ins, refs = refs[: len(args)], refs[len(args) :]
        dones = refs.pop() if far else None
        buffers = refs[len(refs) - len(far) :]
        refs = refs[: len(refs) - len(far)]
        for place, number in enumerate(far):
            source = ins[number]
            if number in parts:
                source = parts[number][1](source, index)
            ins[number] = Late(source, buffers[place], dones.at[place])
        body(index, *ins, *refs)
        for number in far:
            ins[number].arrive()

    specs = [
        pl.BlockSpec(memory_space=pltpu.HBM if number in far or number in plain else pltpu.VMEM)
        for number in range(len(args))
    ]
    out_specs = [
        pl.BlockSpec(memory_space=pltpu.HBM if number in far_outs else pltpu.VMEM)
        for number in range(len(outs))
    ]
    scratches = list(scratch) + [pltpu.VMEM(near, args[n].dtype) for n, near in zip(far, nears)]
    if far:
        scratches.append(pltpu.SemaphoreType.DMA((len(far),)))
    args = [
        pltpu.with_memory_space_constraint(arg, pltpu.HBM) if n in far + plain + held else arg
        for n, arg in enumerate(args)
    ]
    return pl.pallas_call(
        run,
        out_shape=outs,
        in_specs=specs,
        out_specs=out_specs,
        scratch_shapes=scratches,
        cost_estimate=pl.CostEstimate(flops=flops, bytes_accessed=0, transcendentals=0),
        compiler_params=pltpu.CompilerParams(vmem_limit_bytes=limit * MIB),
    )(*args)


def wrapped(value, count):
    return jnp.where(value >= count, value - count, value)


def weights_and_tokens(tokens, gain, query, key, value, out, weights):
    cols = query.shape[1]
    for place, weight in enumerate((query, key, value)):
        weights[:, place * cols : (place + 1) * cols] = weight[...]
    block = out.shape[2]
    for z in range(NZ):
        cols = slice(z * block, (z + 1) * block)
        out[z] = (tokens[:, cols].astype(F32) * gain[:, cols]).astype(BF)


def pack_body(index, after, gate, up, down, out):
    block, size = gate.shape
    half = down.shape[1] // 2
    out[:block, :size] = gate[...]
    out[:block, size:] = up[...]
    out[block : block + size, :] = down[:, :half]
    out[block + size :, :] = down[:, half:]


def turned(row, rows):
    shape = (rows, row.shape[1])
    same = lax.broadcasted_iota(jnp.int32, shape, 0) == lax.broadcasted_iota(jnp.int32, shape, 1)
    return jnp.sum(jnp.where(same, row, 0.0), axis=1, keepdims=True)


def spread_body(
    index, tokens, gain, query, key, value, decay_weight, beta_weight, rate, ids, prob, logit,
    out, weights, meta, factors,
):
    weights_and_tokens(tokens, gain, query, key, value, out, weights)
    rows, width = tokens.shape
    block = meta.shape[1]
    wide = tokens[...].astype(F32)
    row_scale = lax.rsqrt(jnp.sum(wide * wide, axis=1, keepdims=True) / width + EPS)
    gained = (wide * gain[...]).astype(BF)
    over_width = (((1,), (1,)), ((), ()))
    heads = rate.shape[1]
    factor_lane = lax.broadcasted_iota(jnp.int32, factors.shape, 1)
    table = jnp.where(factor_lane == 0, row_scale, 0.0)

    def own_heads(weight):
        product = lax.dot_general(gained, weight[...], over_width, preferred_element_type=F32)
        lane = lax.broadcasted_iota(jnp.int32, product.shape, 1)
        columns = []
        for h in range(heads):
            own = lane == index[2] * heads + h
            columns.append(jnp.sum(jnp.where(own, product, 0.0), axis=1, keepdims=True) * row_scale)
        return columns

    for h, column in enumerate(own_heads(decay_weight)):
        soft = jnp.maximum(column, 0.0) + jnp.log1p(jnp.exp(-jnp.abs(column)))
        table = jnp.where(factor_lane == 1 + h, jnp.exp(-rate[:, h : h + 1] * soft), table)
    for h, column in enumerate(own_heads(beta_weight)):
        table = jnp.where(factor_lane == 1 + heads + h, 1.0 / (1.0 + jnp.exp(-column)), table)
    factors[...] = table

    picks = [ids[k : k + 1, :].astype(F32) for k in range(2)]
    pick_cols = [turned(pick, rows) for pick in picks]
    shape = (rows, rows)
    earlier = lax.broadcasted_iota(jnp.int32, shape, 0) < lax.broadcasted_iota(jnp.int32, shape, 1)
    powers = [jnp.exp(logit[k : k + 1, :]) for k in range(2)]
    total = powers[0] + powers[1]
    lines = []
    for k in range(2):
        named = jnp.zeros(shape, F32)
        for column in pick_cols:
            named = named + jnp.where(earlier & (column == picks[k]), 1.0, 0.0)
        lines.append(picks[k] * CAP + jnp.sum(named, axis=0, keepdims=True))
    for k in range(2):
        route = prob[...] * powers[k] / total
        high = route.astype(BF).astype(F32)
        lines += [high, route - high]
    line = lax.broadcasted_iota(jnp.int32, (8, rows), 0)
    table = jnp.zeros((8, rows), F32)
    for number, values in enumerate(lines):
        table = jnp.where(line == number, values, table)
    shape = (rows, block)
    lane = lax.broadcasted_iota(jnp.int32, shape, 1)
    spot = lane == lax.broadcasted_iota(jnp.int32, shape, 0) + index[0] * rows
    spot = jnp.where(spot, 1.0, 0.0).astype(BF)
    meta[...] = jnp.dot(table.astype(BF), spot, preferred_element_type=F32).astype(BF)


def project_body(index, arrived, w0, w1, w2, w3, out):
    groups, rows, _ = arrived.shape
    total = None
    for step, weight in enumerate((w0, w1, w2, w3)):
        size = weight.shape[0]
        place = pl.multiple_of(wrapped(index[1] + step, NX) * size, size)
        left = arrived[:, :, pl.ds(place, size)].astype(F32).reshape(groups * rows, size).astype(BF)
        part = jnp.dot(left, weight[...], preferred_element_type=F32)
        total = part if total is None else total + part
    out[...] = total.reshape(groups, rows, -1).astype(BF)


def recall_body(index, arrived, factors, state, head_gain, weight, out, keys, changes):
    rows, heads, size = state.shape[:3]
    cols = heads * size
    summed = arrived[0].astype(F32)
    for z in range(1, NZ):
        summed = summed + arrived[z].astype(F32)
    summed = summed * factors[:, 0:1]
    line = lax.broadcasted_iota(jnp.int32, (rows, size), 0)
    head_rows = []
    for h in range(heads):
        own = slice(h * size, (h + 1) * size)
        query = unit_rows(summed[:, own]) * size ** (-0.5)
        key = unit_rows(summed[:, cols + h * size : cols + (h + 1) * size])
        value = summed[:, 2 * cols + h * size : 2 * cols + (h + 1) * size]
        both = jnp.concatenate((key, query), axis=0).astype(BF)
        recalled = jnp.zeros((rows, size), F32)
        asked = jnp.zeros((rows, size), F32)
        for b in range(0, rows, 2):
            pair = jnp.concatenate((state[b, h], state[b + 1, h]), axis=1).astype(BF)
            product = jnp.dot(both, pair, preferred_element_type=F32)
            for side in range(2):
                lanes = slice(side * size, (side + 1) * size)
                recalled = jnp.where(line == b + side, product[:rows, lanes], recalled)
                asked = jnp.where(line == b + side, product[rows:, lanes], asked)
        fade = factors[:, 1 + h : 2 + h]
        gate = factors[:, 1 + heads + h : 2 + heads + h]
        change = gate * (value - fade * recalled)
        keys[:, own] = key
        changes[:, own] = change
        result = fade * asked + jnp.sum(query * key, axis=1, keepdims=True) * change
        mean_sq = jnp.mean(result * result, axis=1, keepdims=True)
        head_rows.append(result * lax.rsqrt(mean_sq + EPS) * head_gain[...])
    left = jnp.concatenate(head_rows, axis=1).astype(BF)
    block = out.shape[2]
    for t in range(NT):
        right = weight[:, t * block : (t + 1) * block]
        out[t] = jnp.dot(left, right, preferred_element_type=F32).astype(BF)


def update_body(keys, changes, factors, state, new_state):
    rows, heads, size = state.shape[:3]
    line = lax.broadcasted_iota(jnp.int32, (rows, size), 0)
    line = jnp.concatenate((line, line, line), axis=0)
    for h in range(heads):
        own = slice(h * size, (h + 1) * size)
        key, change = keys[:, own], changes[:, own]
        key_high = key.astype(BF).astype(F32)
        high = change.astype(BF).astype(F32)
        left = jnp.concatenate((key_high, key - key_high, key_high), axis=0).T.astype(BF)
        right = jnp.concatenate((high, high, change - high), axis=0)
        for b in range(0, rows, 2):
            pair = [jnp.where(line == b + side, right, 0.0) for side in range(2)]
            pair = jnp.concatenate(pair, axis=1).astype(BF)
            product = jnp.dot(left, pair, preferred_element_type=F32)
            for side in range(2):
                fade = factors[b + side : b + side + 1, 1 + h : 2 + h]
                grown = product[:, side * size : (side + 1) * size]
                new_state[b + side, h] = fade * state[b + side, h] + grown


def updated(keys, changes, factors, state):
    rows, heads, size = state.shape[:3]
    step = 8
    flat = lambda i: (i, 0)
    deep = lambda i: (i, 0, 0, 0)
    args = [
        pltpu.with_memory_space_constraint(arg, pltpu.HBM)
        for arg in (keys, changes, factors, state)
    ]
    return pl.pallas_call(
        update_body,
        name="update_body",
        out_shape=jax.ShapeDtypeStruct(state.shape, F32),
        grid=(rows // step,),
        in_specs=[
            pl.BlockSpec((step, heads * size), flat),
            pl.BlockSpec((step, heads * size), flat),
            pl.BlockSpec((step, factors.shape[1]), flat),
            pl.BlockSpec((step, heads, size, size), deep),
        ],
        out_specs=pl.BlockSpec((step, heads, size, size), deep),
        cost_estimate=pl.CostEstimate(flops=10**8, bytes_accessed=0, transcendentals=0),
        compiler_params=pltpu.CompilerParams(vmem_limit_bytes=16 * MIB),
    )(*args)


def middle_body(index, arrived, tokens, meta, middle, out):
    block = middle.shape[1]
    rows = middle.shape[0]
    summed = arrived[0].astype(F32)
    for t in range(1, NT):
        summed = summed + arrived[t].astype(F32)
    place = pl.multiple_of(index[2] * block, block)
    total = tokens[:, pl.ds(place, block)].astype(F32) + summed
    middle[...] = total
    narrow = total.astype(BF)
    for z in range(NZ):
        out[z, :rows, :] = narrow
        out[z, rows:, :] = meta[...]


def slots_of(route, zi):
    tokens = route.shape[1]
    lane = lax.broadcasted_iota(jnp.int32, (1, tokens), 1)
    source = jnp.zeros((1, tokens), jnp.int32)
    for z in range(1, NZ):
        source = source + jnp.where(lane >= z * (tokens // NZ), 1, 0)
    slots = []
    for k in range(2):
        code = route[k : k + 1, :].astype(jnp.int32) - zi * (NX * CAP)
        expert = jnp.zeros((1, tokens), jnp.int32)
        for x in range(1, NX):
            expert = expert + jnp.where(code >= x * CAP, 1, 0)
        slot = expert * (NZ * CAP) + source * CAP + (code - expert * CAP)
        slots.append(jnp.where((code >= 0) & (code < NX * CAP), slot, -1))
    return slots


def dispatch_body(index, arrived, gain, g0, g1, g2, g3, out, route):
    rows = arrived.shape[1] - 8
    tokens = NZ * rows
    block = arrived.shape[2]
    half = block // 2
    wide = arrived[:, :rows, :].astype(F32).reshape(tokens, block)
    narrow = wide.astype(BF)
    routing = arrived[0, rows:, :tokens].astype(F32)
    for z in range(1, NZ):
        routing = routing + arrived[z, rows:, :tokens].astype(F32)
    route[...] = routing
    slot0, slot1 = slots_of(routing, index[0])
    place = lax.broadcasted_iota(jnp.int32, (NX * rows, tokens), 0)
    picks = jnp.where((place == slot0) | (place == slot1), 1.0, 0.0).astype(BF)
    chosen = jnp.dot(picks, narrow, preferred_element_type=F32).astype(BF)
    square = lax.dot_general(
        jnp.ones((8, block), F32),
        wide * wide,
        (((1,), (1,)), ((), ())),
        precision=lax.Precision.HIGHEST,
        preferred_element_type=F32,
    )
    high = square.astype(BF).astype(F32)
    first = lax.broadcasted_iota(jnp.int32, square.shape, 0) == 0
    square = jnp.where(first, high, square - high).astype(BF)
    for x in range(NX):
        own = chosen[x * rows : (x + 1) * rows]
        for y in range(NY):
            out[x, y, :rows, :] = own[:, :half]
            out[x, y, rows : 2 * rows, :] = own[:, half:]
            out[x, y, 4 * rows :, :tokens] = square
            out[x, y, 4 * rows :, tokens:] = jnp.zeros((8, half - tokens), BF)
    scaled = (wide * gain[...]).astype(BF)
    for step, weight in enumerate((g0, g1, g2, g3)):
        part = jnp.dot(scaled, weight[...], preferred_element_type=F32)
        x = wrapped(index[1] + step, NX)
        out[x, :, 2 * rows : 4 * rows, :] = part.reshape(NY, 2 * rows, half).astype(BF)


def expert_body(index, arrived, partner, gain, gate, up, down, away, hidden, dense):
    rows, block = away.shape[2:]
    size = gate.shape[1]
    half = block // 2
    width = gate.shape[0]
    slots = NX * rows
    squares = jnp.zeros((slots, half), F32)
    gate_sum = jnp.zeros((slots, gate.shape[1]), F32)
    up_sum = jnp.zeros((slots, gate.shape[1]), F32)
    for y in range(NY):
        for source, core in ((arrived, index[3]), (partner, 1 - index[3])):
            for part in range(2):
                wide = source[:, y, part * rows : (part + 1) * rows, :].astype(F32)
                wide = wide.reshape(slots, half)
                squares = squares + wide * wide
                place = pl.multiple_of((2 * y + core) * block + part * half, half)
                left = (wide * gain[:, pl.ds(place, half)]).astype(BF)
                own = pl.ds(place, half)
                gate_sum += jnp.dot(left, gate[own, :], preferred_element_type=F32)
                up_sum += jnp.dot(left, up[own, :], preferred_element_type=F32)
    scale = lax.rsqrt(jnp.sum(squares, axis=1, keepdims=True) / width + EPS)
    result = (silu(gate_sum * scale) * (up_sum * scale)).astype(BF)
    hidden[...] = result
    for y in range(NY):
        place = pl.multiple_of((2 * y + 1 - index[3]) * block, block)
        part = jnp.dot(result, down[:, pl.ds(place, block)], preferred_element_type=F32)
        away[:, y] = part.reshape(NX, rows, block).astype(BF)
    tokens = NZ * rows
    lane = lax.broadcasted_iota(jnp.int32, (rows, tokens), 1)
    own = lane == lax.broadcasted_iota(jnp.int32, (rows, tokens), 0) + index[2] * rows
    for x in range(NX):
        summed = jnp.zeros((rows, half), F32)
        square = jnp.zeros((8, tokens), F32)
        for y in range(NY):
            for source in (arrived, partner):
                both = source[x, y, 2 * rows : 4 * rows, :].astype(F32)
                summed = summed + jnp.where(index[3] == 0, both[:rows], both[rows:])
                square = square + source[x, y, 4 * rows :, :tokens].astype(F32)
        square = square[0:1, :] + square[1:2, :]
        square = jnp.sum(jnp.where(own, square, 0.0), axis=1, keepdims=True)
        summed = summed * lax.rsqrt(square / width + EPS)
        result = (silu(summed[:, : half // 2]) * summed[:, half // 2 :]).astype(BF)
        dense[x] = result
        away[x, NY, :, :size] = result
        away[x, NY, :, size:] = jnp.zeros((rows, block - size), BF)


def result_body(index, hidden, dense, away, down, out):
    rows, block = away.shape[2:]
    size = dense.shape[2]
    own_place = pl.multiple_of(block + index[3] * size, size)
    far_place = pl.multiple_of(block + (1 - index[3]) * size, size)
    for y in range(NY):
        place = pl.multiple_of((2 * y + index[3]) * block, block)
        part = jnp.dot(hidden[...], down[:, pl.ds(place, block)], preferred_element_type=F32)
        part = part.reshape(NX, rows, block) + away[:, y].astype(F32)
        out[:, y, :, :block] = part.astype(BF)
        out[:, y, :, pl.ds(own_place, size)] = dense[...]
        out[:, y, :, pl.ds(far_place, size)] = away[:, NY, :, :size]


def combine_body(index, arrived, route, d0, d1, d2, d3, mix, out):
    rows = arrived.shape[2]
    block = out.shape[2]
    tokens = NZ * rows
    results = []
    for x in range(NX):
        summed = arrived[x, 0, :, :block].astype(F32)
        for y in range(1, NY):
            summed = summed + arrived[x, y, :, :block].astype(F32)
        results.append(summed)
    results = jnp.concatenate(results, axis=0).astype(BF)
    routing = route[...]
    slot0, slot1 = slots_of(routing, index[0])
    place = lax.broadcasted_iota(jnp.int32, (NX * rows, tokens), 0)
    total = jnp.zeros((tokens, block), F32)
    for k in range(2):
        share = jnp.where(place == slot0, routing[2 + k : 3 + k, :], 0.0)
        share = jnp.where(place == slot1, routing[4 + k : 5 + k, :], share).astype(BF)
        total += lax.dot_general(
            share, results, (((0,), (0,)), ((), ())), preferred_element_type=F32
        )
    gate = 1.0 / (1.0 + jnp.exp(-mix[...]))
    total = total.reshape(NY, 2, rows, block)
    size = (arrived.shape[3] - block) // 2
    for core in range(2):
        lower = jnp.zeros((NY * rows, block // 2), F32)
        upper = jnp.zeros((NY * rows, block // 2), F32)
        lanes = slice(block + core * size, block + (core + 1) * size)
        for step, weight in enumerate((d0, d1, d2, d3)):
            x = wrapped(index[1] + step, NX)
            left = arrived[x, :, :, lanes].astype(F32).reshape(NY * rows, size).astype(BF)
            lower += jnp.dot(left, weight[:size, :], preferred_element_type=F32)
            upper += jnp.dot(left, weight[size:, :], preferred_element_type=F32)
        dense = gate * jnp.concatenate((lower, upper), axis=1)
        for y in range(NY):
            own = dense[y * rows : (y + 1) * rows] + total[y, core]
            out[2 * y + core] = own.astype(BF)


def final_body(index, arrived, middle, out):
    summed = arrived[0].astype(F32)
    for z in range(1, NZ):
        summed = summed + arrived[z].astype(F32)
    out[...] = (middle[...] + summed).astype(BF)


def per_device(
    tokens,
    delta_state,
    attn_gain,
    query_weight,
    key_weight,
    value_weight,
    decay_weight,
    beta_weight,
    decay_rate,
    head_gain,
    output_weight,
    ffn_gain,
    expert_ids,
    group_prob,
    expert_logit,
    expert_gate,
    expert_up,
    expert_down,
    dense_gate,
    dense_up,
    dense_down,
    dense_mix,
):
    rows, width = tokens.shape
    heads, size = delta_state.shape[1:3]
    cols = heads * size
    block = width // NT
    half = block // 2

    def shape(*dims, dtype=BF):
        return jax.ShapeDtypeStruct(dims, dtype)

    def own_block(ref, index):
        place = pl.multiple_of(index[2] * block, block)
        return ref.at[:, pl.ds(place, block)]

    message, own_weights, meta, factors = kernel(
        spread_body,
        (
            pltpu.HBM((NZ, rows, block), BF),
            shape(query_weight.shape[0], 3 * cols),
            shape(8, block),
            shape(rows, 128, dtype=F32),
        ),
        tokens,
        attn_gain[None],
        query_weight,
        key_weight,
        value_weight,
        decay_weight.T,
        beta_weight.T,
        decay_rate[None],
        expert_ids.T,
        group_prob[None],
        expert_logit.T,
        far=range(11),
    )
    qkv_weights = from_neighbours(own_weights, "x")
    spread = exchange(message, "z")
    (packed,) = kernel(
        pack_body,
        (shape(block + dense_gate.shape[1] * 2, half),),
        message,
        dense_gate,
        dense_up,
        dense_down,
        plain=(0,),
        far=(1, 2, 3),
    )
    dense_weights = from_neighbours(packed, "x")
    (part,) = kernel(
        project_body,
        (shape(NZ, rows, 3 * cols),),
        spread,
        *qkv_weights,
        held=(1, 2, 3, 4),
        flops=2 * NZ * rows * block * 3 * cols,
    )
    arrived = exchange(part, "z")
    attn_part, keys, changes = kernel(
        recall_body,
        (
            shape(NT, rows, block),
            shape(rows, cols, dtype=F32),
            shape(rows, cols, dtype=F32),
        ),
        arrived,
        factors,
        delta_state,
        head_gain[None],
        output_weight,
        far=(1, 3, 4),
        flops=2 * rows * cols * width,
    )
    new_state = updated(keys, changes, factors, delta_state)
    arrived = exchange(attn_part, ("y", "c"))
    middle, message = kernel(
        middle_body,
        (shape(rows, block, dtype=F32), shape(NZ, rows + 8, block)),
        arrived,
        tokens,
        meta,
    )

    swap = [(0, 1), (1, 0)]
    arrived = exchange(message, "z")
    message, route_rows = kernel(
        dispatch_body,
        (shape(NX, NY, 4 * rows + 8, half), shape(8, NZ * rows, dtype=F32)),
        arrived,
        ffn_gain[None],
        *dense_weights,
        far=range(1, 6),
        parts={
            1: ((1, block), own_block),
            **{n: ((block, half), lambda ref, index: ref.at[:block]) for n in range(2, 6)},
        },
        flops=2 * NZ * rows * block * 2 * block,
    )
    sides = ("x", "y")
    arrived = exchange(message.reshape(NX * NY, -1, half), sides)
    partner = lax.ppermute(arrived, "c", swap).reshape(message.shape)
    away, hidden, dense = kernel(
        expert_body,
        (shape(NX, NY + 1, rows, block), shape(NX * rows, 128), shape(NX, rows, 128)),
        arrived.reshape(message.shape),
        partner,
        ffn_gain[None],
        expert_gate[0],
        expert_up[0],
        expert_down[0],
        far=(2,),
        flops=5 * NX * rows * width * 128,
    )
    (message,) = kernel(
        result_body,
        (shape(NX, NY, rows, block + 2 * 128),),
        hidden,
        dense,
        lax.ppermute(away, "c", swap),
        expert_down[0],
        flops=NX * rows * width * 128,
    )
    arrived = exchange(message.reshape(NX * NY, rows, -1), sides)
    (message,) = kernel(
        combine_body,
        (shape(NZ, rows, block),),
        arrived.reshape(message.shape),
        route_rows,
        *dense_weights,
        dense_mix[None],
        far=range(1, 7),
        parts={n: ((half, half), lambda ref, index: ref.at[block:]) for n in range(2, 6)},
        flops=2 * NZ * rows * block * block,
    )
    arrived = exchange(message, "z")
    (mixed_out,) = kernel(final_body, (shape(rows, block),), arrived, middle)
    return (mixed_out, new_state)


def solution(mesh):
    fine = Mesh(mesh.devices.reshape(NZ, NX, 4, 2), ("z", "x", "y", "c"))
    ep, tp = ("z", "x"), ("y", "c")

    return jax.shard_map(
        per_device,
        mesh=fine,
        in_specs=(
            P(ep, None),
            P(ep, tp, None, None),
            P(),
            P(ep, tp),
            P(ep, tp),
            P(ep, tp),
            P(),
            P(),
            P(tp),
            P(),
            P(tp, None),
            P(),
            P(ep, None),
            P(ep),
            P(ep, None),
            P(ep, None, tp),
            P(ep, None, tp),
            P(ep, tp, None),
            P(tp, ep),
            P(tp, ep),
            P(ep, tp),
            P(tp),
        ),
        out_specs=(P(ep, tp), P(ep, tp, None, None)),
        check_vma=False,
    )
```

```python
import jax
import jax.numpy as jnp
from jax import lax
from jax.experimental import pallas as pl
from jax.experimental.pallas import tpu as pltpu
from jax.sharding import Mesh, PartitionSpec as P

EPS = 1e-06
BF = jnp.bfloat16
F32 = jnp.float32
NZ, NX, NY, NT = 8, 4, 4, 8
CAP = 3
MIB = 1 << 20


def exchange(tiles, axes):
    return lax.all_to_all(tiles, axes, split_axis=0, concat_axis=0, tiled=True)


def from_neighbours(shard, axis):
    count = lax.axis_size(axis)
    parts = [shard]
    for step in range(1, count):
        pairs = [(source, (source - step) % count) for source in range(count)]
        parts.append(lax.ppermute(shard, axis, pairs))
    return parts


def unit_rows(values):
    return values * lax.rsqrt(jnp.sum(values * values, axis=-1, keepdims=True) + EPS)


def silu(values):
    return values / (1.0 + jnp.exp(-values))


class Late:
    def __init__(self, source, near, done):
        self.near = near
        self.copy = pltpu.make_async_copy(source, near, done)
        self.copy.start()
        self.waits = True

    def arrive(self):
        if self.waits:
            self.copy.wait()
            self.waits = False
        return self.near

    def __getitem__(self, where):
        return self.arrive()[where]

    @property
    def shape(self):
        return self.near.shape


def kernel(
    body, outs, *args, far=(), plain=(), held=(), parts=None, far_outs=(), scratch=(), flops=0, limit=16
):
    parts = parts or {}
    far, plain, held = tuple(far), tuple(plain), tuple(held)
    nears = [parts[n][0] if n in parts else args[n].shape for n in far]

    def run(*refs):
        sides = [lax.axis_index(name) for name in ("z", "x", "y", "c")]
        index = (sides[0], sides[1], sides[2] * 2 + sides[3], sides[3])
        refs = list(refs)
        ins, refs = refs[: len(args)], refs[len(args) :]
        dones = refs.pop() if far else None
        buffers = refs[len(refs) - len(far) :]
        refs = refs[: len(refs) - len(far)]
        for place, number in enumerate(far):
            source = ins[number]
            if number in parts:
                source = parts[number][1](source, index)
            ins[number] = Late(source, buffers[place], dones.at[place])
        body(index, *ins, *refs)
        for number in far:
            ins[number].arrive()

    specs = [
        pl.BlockSpec(memory_space=pltpu.HBM if number in far or number in plain else pltpu.VMEM)
        for number in range(len(args))
    ]
    out_specs = [
        pl.BlockSpec(memory_space=pltpu.HBM if number in far_outs else pltpu.VMEM)
        for number in range(len(outs))
    ]
    scratches = list(scratch) + [pltpu.VMEM(near, args[n].dtype) for n, near in zip(far, nears)]
    if far:
        scratches.append(pltpu.SemaphoreType.DMA((len(far),)))
    args = [
        pltpu.with_memory_space_constraint(arg, pltpu.HBM) if n in far + plain + held else arg
        for n, arg in enumerate(args)
    ]
    return pl.pallas_call(
        run,
        out_shape=outs,
        in_specs=specs,
        out_specs=out_specs,
        scratch_shapes=scratches,
        cost_estimate=pl.CostEstimate(flops=flops, bytes_accessed=0, transcendentals=0),
        compiler_params=pltpu.CompilerParams(vmem_limit_bytes=limit * MIB),
    )(*args)


def wrapped(value, count):
    return jnp.where(value >= count, value - count, value)


def weights_and_tokens(tokens, gain, query, key, value, out, weights):
    cols = query.shape[1]
    for place, weight in enumerate((query, key, value)):
        weights[:, place * cols : (place + 1) * cols] = weight[...]
    block = out.shape[2]
    for z in range(NZ):
        cols = slice(z * block, (z + 1) * block)
        out[z] = (tokens[:, cols].astype(F32) * gain[:, cols]).astype(BF)


def pack_body(index, after, gate, up, down, out):
    block, size = gate.shape
    half = down.shape[1] // 2
    out[:block, :size] = gate[...]
    out[:block, size:] = up[...]
    out[block : block + size, :] = down[:, :half]
    out[block + size :, :] = down[:, half:]


def turned(row, rows):
    shape = (rows, row.shape[1])
    same = lax.broadcasted_iota(jnp.int32, shape, 0) == lax.broadcasted_iota(jnp.int32, shape, 1)
    return jnp.sum(jnp.where(same, row, 0.0), axis=1, keepdims=True)


def spread_body(
    index, tokens, gain, query, key, value, decay_weight, beta_weight, rate, ids, prob, logit,
    far_out, far_weights, far_meta, far_factors, out, weights, meta, factors, stored,
):
    stores = [
        pltpu.make_async_copy(near, far, stored.at[place])
        for place, (near, far) in enumerate(
            ((out, far_out), (weights, far_weights), (meta, far_meta), (factors, far_factors))
        )
    ]
    weights_and_tokens(tokens, gain, query, key, value, out, weights)
    stores[0].start()
    stores[1].start()
    rows, width = tokens.shape
    block = meta.shape[1]
    wide = tokens[...].astype(F32)
    row_scale = lax.rsqrt(jnp.sum(wide * wide, axis=1, keepdims=True) / width + EPS)
    gained = (wide * gain[...]).astype(BF)
    over_width = (((1,), (1,)), ((), ()))
    heads = rate.shape[1]
    factor_lane = lax.broadcasted_iota(jnp.int32, factors.shape, 1)
    table = jnp.where(factor_lane == 0, row_scale, 0.0)

    def own_heads(weight):
        product = lax.dot_general(gained, weight[...], over_width, preferred_element_type=F32)
        lane = lax.broadcasted_iota(jnp.int32, product.shape, 1)
        columns = []
        for h in range(heads):
            own = lane == index[2] * heads + h
            columns.append(jnp.sum(jnp.where(own, product, 0.0), axis=1, keepdims=True) * row_scale)
        return columns

    for h, column in enumerate(own_heads(decay_weight)):
        soft = jnp.maximum(column, 0.0) + jnp.log1p(jnp.exp(-jnp.abs(column)))
        table = jnp.where(factor_lane == 1 + h, jnp.exp(-rate[:, h : h + 1] * soft), table)
    for h, column in enumerate(own_heads(beta_weight)):
        table = jnp.where(factor_lane == 1 + heads + h, 1.0 / (1.0 + jnp.exp(-column)), table)
    factors[...] = table

    picks = [ids[k : k + 1, :].astype(F32) for k in range(2)]
    pick_cols = [turned(pick, rows) for pick in picks]
    shape = (rows, rows)
    earlier = lax.broadcasted_iota(jnp.int32, shape, 0) < lax.broadcasted_iota(jnp.int32, shape, 1)
    powers = [jnp.exp(logit[k : k + 1, :]) for k in range(2)]
    total = powers[0] + powers[1]
    lines = []
    for k in range(2):
        named = jnp.zeros(shape, F32)
        for column in pick_cols:
            named = named + jnp.where(earlier & (column == picks[k]), 1.0, 0.0)
        lines.append(picks[k] * CAP + jnp.sum(named, axis=0, keepdims=True))
    for k in range(2):
        route = prob[...] * powers[k] / total
        high = route.astype(BF).astype(F32)
        lines += [high, route - high]
    line = lax.broadcasted_iota(jnp.int32, (8, rows), 0)
    table = jnp.zeros((8, rows), F32)
    for number, values in enumerate(lines):
        table = jnp.where(line == number, values, table)
    shape = (rows, block)
    lane = lax.broadcasted_iota(jnp.int32, shape, 1)
    spot = lane == lax.broadcasted_iota(jnp.int32, shape, 0) + index[0] * rows
    spot = jnp.where(spot, 1.0, 0.0).astype(BF)
    meta[...] = jnp.dot(table.astype(BF), spot, preferred_element_type=F32).astype(BF)
    stores[2].start()
    stores[3].start()
    for store in stores:
        store.wait()


def project_body(index, arrived, w0, w1, w2, w3, out):
    groups, rows, _ = arrived.shape
    total = None
    for step, weight in enumerate((w0, w1, w2, w3)):
        size = weight.shape[0]
        place = pl.multiple_of(wrapped(index[1] + step, NX) * size, size)
        left = arrived[:, :, pl.ds(place, size)].astype(F32).reshape(groups * rows, size).astype(BF)
        part = jnp.dot(left, weight[...], preferred_element_type=F32)
        total = part if total is None else total + part
    out[...] = total.reshape(groups, rows, -1).astype(BF)


def recall_body(index, arrived, factors, state, head_gain, weight, out, keys, changes):
    rows, heads, size = state.shape[:3]
    cols = heads * size
    summed = arrived[0].astype(F32)
    for z in range(1, NZ):
        summed = summed + arrived[z].astype(F32)
    summed = summed * factors[:, 0:1]
    line = lax.broadcasted_iota(jnp.int32, (rows, size), 0)
    head_rows = []
    for h in range(heads):
        own = slice(h * size, (h + 1) * size)
        query = unit_rows(summed[:, own]) * size ** (-0.5)
        key = unit_rows(summed[:, cols + h * size : cols + (h + 1) * size])
        value = summed[:, 2 * cols + h * size : 2 * cols + (h + 1) * size]
        both = jnp.concatenate((key, query), axis=0).astype(BF)
        recalled = jnp.zeros((rows, size), F32)
        asked = jnp.zeros((rows, size), F32)
        for b in range(0, rows, 2):
            pair = jnp.concatenate((state[b, h], state[b + 1, h]), axis=1).astype(BF)
            product = jnp.dot(both, pair, preferred_element_type=F32)
            for side in range(2):
                lanes = slice(side * size, (side + 1) * size)
                recalled = jnp.where(line == b + side, product[:rows, lanes], recalled)
                asked = jnp.where(line == b + side, product[rows:, lanes], asked)
        fade = factors[:, 1 + h : 2 + h]
        gate = factors[:, 1 + heads + h : 2 + heads + h]
        change = gate * (value - fade * recalled)
        keys[:, own] = key
        changes[:, own] = change
        result = fade * asked + jnp.sum(query * key, axis=1, keepdims=True) * change
        mean_sq = jnp.mean(result * result, axis=1, keepdims=True)
        head_rows.append(result * lax.rsqrt(mean_sq + EPS) * head_gain[...])
    left = jnp.concatenate(head_rows, axis=1).astype(BF)
    block = out.shape[2]
    for t in range(NT):
        right = weight[:, t * block : (t + 1) * block]
        out[t] = jnp.dot(left, right, preferred_element_type=F32).astype(BF)


def update_body(index, keys, changes, factors, state, new_state):
    rows, heads, size = state.shape[:3]
    line = lax.broadcasted_iota(jnp.int32, (rows, size), 0)
    line = jnp.concatenate((line, line, line), axis=0)
    for h in range(heads):
        own = slice(h * size, (h + 1) * size)
        key, change = keys[:, own], changes[:, own]
        key_high = key.astype(BF).astype(F32)
        high = change.astype(BF).astype(F32)
        left = jnp.concatenate((key_high, key - key_high, key_high), axis=0).T.astype(BF)
        right = jnp.concatenate((high, high, change - high), axis=0)
        for b in range(0, rows, 2):
            pair = [jnp.where(line == b + side, right, 0.0) for side in range(2)]
            pair = jnp.concatenate(pair, axis=1).astype(BF)
            product = jnp.dot(left, pair, preferred_element_type=F32)
            for side in range(2):
                fade = factors[b + side : b + side + 1, 1 + h : 2 + h]
                grown = product[:, side * size : (side + 1) * size]
                new_state[b + side, h] = fade * state[b + side, h] + grown


def middle_body(index, arrived, tokens, meta, middle, out):
    block = middle.shape[1]
    rows = middle.shape[0]
    summed = arrived[0].astype(F32)
    for t in range(1, NT):
        summed = summed + arrived[t].astype(F32)
    place = pl.multiple_of(index[2] * block, block)
    total = tokens[:, pl.ds(place, block)].astype(F32) + summed
    middle[...] = total
    narrow = total.astype(BF)
    for z in range(NZ):
        out[z, :rows, :] = narrow
        out[z, rows:, :] = meta[...]


def slots_of(route, zi):
    tokens = route.shape[1]
    lane = lax.broadcasted_iota(jnp.int32, (1, tokens), 1)
    source = jnp.zeros((1, tokens), jnp.int32)
    for z in range(1, NZ):
        source = source + jnp.where(lane >= z * (tokens // NZ), 1, 0)
    slots = []
    for k in range(2):
        code = route[k : k + 1, :].astype(jnp.int32) - zi * (NX * CAP)
        expert = jnp.zeros((1, tokens), jnp.int32)
        for x in range(1, NX):
            expert = expert + jnp.where(code >= x * CAP, 1, 0)
        slot = expert * (NZ * CAP) + source * CAP + (code - expert * CAP)
        slots.append(jnp.where((code >= 0) & (code < NX * CAP), slot, -1))
    return slots


def dispatch_body(index, arrived, gain, g0, g1, g2, g3, after, out, route):
    rows = arrived.shape[1] - 8
    tokens = NZ * rows
    block = arrived.shape[2]
    half = block // 2
    wide = arrived[:, :rows, :].astype(F32).reshape(tokens, block)
    narrow = wide.astype(BF)
    routing = arrived[0, rows:, :tokens].astype(F32)
    for z in range(1, NZ):
        routing = routing + arrived[z, rows:, :tokens].astype(F32)
    route[...] = routing
    slot0, slot1 = slots_of(routing, index[0])
    place = lax.broadcasted_iota(jnp.int32, (NX * rows, tokens), 0)
    picks = jnp.where((place == slot0) | (place == slot1), 1.0, 0.0).astype(BF)
    chosen = jnp.dot(picks, narrow, preferred_element_type=F32).astype(BF)
    square = lax.dot_general(
        jnp.ones((8, block), F32),
        wide * wide,
        (((1,), (1,)), ((), ())),
        precision=lax.Precision.HIGHEST,
        preferred_element_type=F32,
    )
    high = square.astype(BF).astype(F32)
    first = lax.broadcasted_iota(jnp.int32, square.shape, 0) == 0
    square = jnp.where(first, high, square - high).astype(BF)
    for x in range(NX):
        own = chosen[x * rows : (x + 1) * rows]
        for y in range(NY):
            out[x, y, :rows, :] = own[:, :half]
            out[x, y, rows : 2 * rows, :] = own[:, half:]
            out[x, y, 4 * rows :, :tokens] = square
            out[x, y, 4 * rows :, tokens:] = jnp.zeros((8, half - tokens), BF)
    scaled = (wide * gain[...]).astype(BF)
    for step, weight in enumerate((g0, g1, g2, g3)):
        part = jnp.dot(scaled, weight[...], preferred_element_type=F32)
        x = wrapped(index[1] + step, NX)
        out[x, :, 2 * rows : 4 * rows, :] = part.reshape(NY, 2 * rows, half).astype(BF)


def expert_body(index, arrived, partner, gain, gate, up, down, away, hidden, dense):
    rows, block = away.shape[2:]
    size = gate.shape[1]
    half = block // 2
    width = gate.shape[0]
    slots = NX * rows
    squares = jnp.zeros((slots, half), F32)
    gate_sum = jnp.zeros((slots, gate.shape[1]), F32)
    up_sum = jnp.zeros((slots, gate.shape[1]), F32)
    for y in range(NY):
        for source, core in ((arrived, index[3]), (partner, 1 - index[3])):
            for part in range(2):
                wide = source[:, y, part * rows : (part + 1) * rows, :].astype(F32)
                wide = wide.reshape(slots, half)
                squares = squares + wide * wide
                place = pl.multiple_of((2 * y + core) * block + part * half, half)
                left = (wide * gain[:, pl.ds(place, half)]).astype(BF)
                own = pl.ds(place, half)
                gate_sum += jnp.dot(left, gate[own, :], preferred_element_type=F32)
                up_sum += jnp.dot(left, up[own, :], preferred_element_type=F32)
    scale = lax.rsqrt(jnp.sum(squares, axis=1, keepdims=True) / width + EPS)
    result = (silu(gate_sum * scale) * (up_sum * scale)).astype(BF)
    hidden[...] = result
    for y in range(NY):
        place = pl.multiple_of((2 * y + 1 - index[3]) * block, block)
        part = jnp.dot(result, down[:, pl.ds(place, block)], preferred_element_type=F32)
        away[:, y] = part.reshape(NX, rows, block).astype(BF)
    tokens = NZ * rows
    lane = lax.broadcasted_iota(jnp.int32, (rows, tokens), 1)
    own = lane == lax.broadcasted_iota(jnp.int32, (rows, tokens), 0) + index[2] * rows
    for x in range(NX):
        summed = jnp.zeros((rows, half), F32)
        square = jnp.zeros((8, tokens), F32)
        for y in range(NY):
            for source in (arrived, partner):
                both = source[x, y, 2 * rows : 4 * rows, :].astype(F32)
                summed = summed + jnp.where(index[3] == 0, both[:rows], both[rows:])
                square = square + source[x, y, 4 * rows :, :tokens].astype(F32)
        square = square[0:1, :] + square[1:2, :]
        square = jnp.sum(jnp.where(own, square, 0.0), axis=1, keepdims=True)
        summed = summed * lax.rsqrt(square / width + EPS)
        result = (silu(summed[:, : half // 2]) * summed[:, half // 2 :]).astype(BF)
        dense[x] = result
        away[x, NY, :, :size] = result
        away[x, NY, :, size:] = jnp.zeros((rows, block - size), BF)


def result_body(index, hidden, dense, away, down, out):
    rows, block = away.shape[2:]
    size = dense.shape[2]
    own_place = pl.multiple_of(block + index[3] * size, size)
    far_place = pl.multiple_of(block + (1 - index[3]) * size, size)
    for y in range(NY):
        place = pl.multiple_of((2 * y + index[3]) * block, block)
        part = jnp.dot(hidden[...], down[:, pl.ds(place, block)], preferred_element_type=F32)
        part = part.reshape(NX, rows, block) + away[:, y].astype(F32)
        out[:, y, :, :block] = part.astype(BF)
        out[:, y, :, pl.ds(own_place, size)] = dense[...]
        out[:, y, :, pl.ds(far_place, size)] = away[:, NY, :, :size]


def combine_body(index, arrived, route, d0, d1, d2, d3, mix, out):
    rows = arrived.shape[2]
    block = out.shape[2]
    tokens = NZ * rows
    results = []
    for x in range(NX):
        summed = arrived[x, 0, :, :block].astype(F32)
        for y in range(1, NY):
            summed = summed + arrived[x, y, :, :block].astype(F32)
        results.append(summed)
    results = jnp.concatenate(results, axis=0).astype(BF)
    routing = route[...]
    slot0, slot1 = slots_of(routing, index[0])
    place = lax.broadcasted_iota(jnp.int32, (NX * rows, tokens), 0)
    total = jnp.zeros((tokens, block), F32)
    for k in range(2):
        share = jnp.where(place == slot0, routing[2 + k : 3 + k, :], 0.0)
        share = jnp.where(place == slot1, routing[4 + k : 5 + k, :], share).astype(BF)
        total += lax.dot_general(
            share, results, (((0,), (0,)), ((), ())), preferred_element_type=F32
        )
    gate = 1.0 / (1.0 + jnp.exp(-mix[...]))
    total = total.reshape(NY, 2, rows, block)
    size = (arrived.shape[3] - block) // 2
    for core in range(2):
        lower = jnp.zeros((NY * rows, block // 2), F32)
        upper = jnp.zeros((NY * rows, block // 2), F32)
        lanes = slice(block + core * size, block + (core + 1) * size)
        for step, weight in enumerate((d0, d1, d2, d3)):
            x = wrapped(index[1] + step, NX)
            left = arrived[x, :, :, lanes].astype(F32).reshape(NY * rows, size).astype(BF)
            lower += jnp.dot(left, weight[:size, :], preferred_element_type=F32)
            upper += jnp.dot(left, weight[size:, :], preferred_element_type=F32)
        dense = gate * jnp.concatenate((lower, upper), axis=1)
        for y in range(NY):
            own = dense[y * rows : (y + 1) * rows] + total[y, core]
            out[2 * y + core] = own.astype(BF)


def final_body(index, arrived, middle, out):
    summed = arrived[0].astype(F32)
    for z in range(1, NZ):
        summed = summed + arrived[z].astype(F32)
    out[...] = (middle[...] + summed).astype(BF)


def per_device(
    tokens,
    delta_state,
    attn_gain,
    query_weight,
    key_weight,
    value_weight,
    decay_weight,
    beta_weight,
    decay_rate,
    head_gain,
    output_weight,
    ffn_gain,
    expert_ids,
    group_prob,
    expert_logit,
    expert_gate,
    expert_up,
    expert_down,
    dense_gate,
    dense_up,
    dense_down,
    dense_mix,
):
    rows, width = tokens.shape
    heads, size = delta_state.shape[1:3]
    cols = heads * size
    block = width // NT
    half = block // 2

    def shape(*dims, dtype=BF):
        return jax.ShapeDtypeStruct(dims, dtype)

    def own_block(ref, index):
        place = pl.multiple_of(index[2] * block, block)
        return ref.at[:, pl.ds(place, block)]

    first = (
        shape(NZ, rows, block),
        shape(query_weight.shape[0], 3 * cols),
        shape(8, block),
        shape(rows, 128, dtype=F32),
    )
    message, own_weights, meta, factors = kernel(
        spread_body,
        tuple(pltpu.HBM(made.shape, made.dtype) for made in first),
        tokens,
        attn_gain[None],
        query_weight,
        key_weight,
        value_weight,
        decay_weight.T,
        beta_weight.T,
        decay_rate[None],
        expert_ids.T,
        group_prob[None],
        expert_logit.T,
        far=range(11),
        far_outs=range(4),
        scratch=[pltpu.VMEM(made.shape, made.dtype) for made in first]
        + [pltpu.SemaphoreType.DMA((4,))],
    )
    qkv_weights = from_neighbours(own_weights, "x")
    spread = exchange(message, "z")
    (packed,) = kernel(
        pack_body,
        (shape(block + dense_gate.shape[1] * 2, half),),
        message,
        dense_gate,
        dense_up,
        dense_down,
        plain=(0,),
        far=(1, 2, 3),
    )
    dense_weights = from_neighbours(packed, "x")
    (part,) = kernel(
        project_body,
        (shape(NZ, rows, 3 * cols),),
        spread,
        *qkv_weights,
        held=(1, 2, 3, 4),
        flops=2 * NZ * rows * block * 3 * cols,
    )
    arrived = exchange(part, "z")
    attn_part, keys, changes = kernel(
        recall_body,
        (
            shape(NT, rows, block),
            pltpu.HBM((rows, cols), F32),
            pltpu.HBM((rows, cols), F32),
        ),
        arrived,
        factors,
        delta_state,
        head_gain[None],
        output_weight,
        far=(1, 3, 4),
        flops=2 * rows * cols * width,
    )
    (new_state,) = kernel(
        update_body,
        (shape(*delta_state.shape, dtype=F32),),
        keys,
        changes,
        factors,
        delta_state,
        far=range(4),
        flops=10**8,
        limit=24,
    )
    arrived = exchange(attn_part, ("y", "c"))
    middle, message = kernel(
        middle_body,
        (shape(rows, block, dtype=F32), shape(NZ, rows + 8, block)),
        arrived,
        tokens,
        meta,
    )

    swap = [(0, 1), (1, 0)]
    arrived = exchange(message, "z")
    message, route_rows = kernel(
        dispatch_body,
        (shape(NX, NY, 4 * rows + 8, half), shape(8, NZ * rows, dtype=F32)),
        arrived,
        ffn_gain[None],
        *dense_weights,
        new_state,
        plain=(6,),
        far=range(1, 6),
        parts={
            1: ((1, block), own_block),
            **{n: ((block, half), lambda ref, index: ref.at[:block]) for n in range(2, 6)},
        },
        flops=2 * NZ * rows * block * 2 * block,
    )
    sides = ("x", "y")
    arrived = exchange(message.reshape(NX * NY, -1, half), sides)
    partner = lax.ppermute(arrived, "c", swap).reshape(message.shape)
    away, hidden, dense = kernel(
        expert_body,
        (shape(NX, NY + 1, rows, block), shape(NX * rows, 128), shape(NX, rows, 128)),
        arrived.reshape(message.shape),
        partner,
        ffn_gain[None],
        expert_gate[0],
        expert_up[0],
        expert_down[0],
        far=(2,),
        flops=5 * NX * rows * width * 128,
    )
    (message,) = kernel(
        result_body,
        (shape(NX, NY, rows, block + 2 * 128),),
        hidden,
        dense,
        lax.ppermute(away, "c", swap),
        expert_down[0],
        flops=NX * rows * width * 128,
    )
    arrived = exchange(message.reshape(NX * NY, rows, -1), sides)
    (message,) = kernel(
        combine_body,
        (shape(NZ, rows, block),),
        arrived.reshape(message.shape),
        route_rows,
        *dense_weights,
        dense_mix[None],
        far=range(1, 7),
        parts={n: ((half, half), lambda ref, index: ref.at[block:]) for n in range(2, 6)},
        flops=2 * NZ * rows * block * block,
    )
    arrived = exchange(message, "z")
    (mixed_out,) = kernel(final_body, (shape(rows, block),), arrived, middle)
    return (mixed_out, new_state)


def solution(mesh):
    fine = Mesh(mesh.devices.reshape(NZ, NX, 4, 2), ("z", "x", "y", "c"))
    ep, tp = ("z", "x"), ("y", "c")

    return jax.shard_map(
        per_device,
        mesh=fine,
        in_specs=(
            P(ep, None),
            P(ep, tp, None, None),
            P(),
            P(ep, tp),
            P(ep, tp),
            P(ep, tp),
            P(),
            P(),
            P(tp),
            P(),
            P(tp, None),
            P(),
            P(ep, None),
            P(ep),
            P(ep, None),
            P(ep, None, tp),
            P(ep, None, tp),
            P(ep, tp, None),
            P(tp, ep),
            P(tp, ep),
            P(ep, tp),
            P(tp),
        ),
        out_specs=(P(ep, tp), P(ep, tp, None, None)),
        check_vma=False,
    )
```

```python
import jax
import jax.numpy as jnp
from jax import lax
from jax.experimental import pallas as pl
from jax.experimental.pallas import tpu as pltpu
from jax.sharding import Mesh, PartitionSpec as P

EPS = 1e-06
BF = jnp.bfloat16
F32 = jnp.float32
NZ, NX, NY, NT = 8, 4, 4, 8
CAP = 3
MIB = 1 << 20


def exchange(tiles, axes):
    return lax.all_to_all(tiles, axes, split_axis=0, concat_axis=0, tiled=True)


def from_neighbours(shard, axis):
    count = lax.axis_size(axis)
    parts = [shard]
    for step in range(1, count):
        pairs = [(source, (source - step) % count) for source in range(count)]
        parts.append(lax.ppermute(shard, axis, pairs))
    return parts


def unit_rows(values):
    return values * lax.rsqrt(jnp.sum(values * values, axis=-1, keepdims=True) + EPS)


def silu(values):
    return values / (1.0 + jnp.exp(-values))


class Late:
    def __init__(self, source, near, done):
        self.near = near
        self.copy = pltpu.make_async_copy(source, near, done)
        self.copy.start()
        self.waits = True

    def arrive(self):
        if self.waits:
            self.copy.wait()
            self.waits = False
        return self.near

    def __getitem__(self, where):
        return self.arrive()[where]

    @property
    def shape(self):
        return self.near.shape


def kernel(
    body, outs, *args, far=(), plain=(), held=(), parts=None, far_outs=(), scratch=(), flops=0, limit=16
):
    parts = parts or {}
    far, plain, held = tuple(far), tuple(plain), tuple(held)
    nears = [parts[n][0] if n in parts else args[n].shape for n in far]

    def run(*refs):
        sides = [lax.axis_index(name) for name in ("z", "x", "y", "c")]
        index = (sides[0], sides[1], sides[2] * 2 + sides[3], sides[3])
        refs = list(refs)
        ins, refs = refs[: len(args)], refs[len(args) :]
        dones = refs.pop() if far else None
        buffers = refs[len(refs) - len(far) :]
        refs = refs[: len(refs) - len(far)]
        for place, number in enumerate(far):
            source = ins[number]
            if number in parts:
                source = parts[number][1](source, index)
            ins[number] = Late(source, buffers[place], dones.at[place])
        body(index, *ins, *refs)
        for number in far:
            ins[number].arrive()

    specs = [
        pl.BlockSpec(memory_space=pltpu.HBM if number in far or number in plain else pltpu.VMEM)
        for number in range(len(args))
    ]
    out_specs = [
        pl.BlockSpec(memory_space=pltpu.HBM if number in far_outs else pltpu.VMEM)
        for number in range(len(outs))
    ]
    scratches = list(scratch) + [pltpu.VMEM(near, args[n].dtype) for n, near in zip(far, nears)]
    if far:
        scratches.append(pltpu.SemaphoreType.DMA((len(far),)))
    args = [
        pltpu.with_memory_space_constraint(arg, pltpu.HBM) if n in far + plain + held else arg
        for n, arg in enumerate(args)
    ]
    return pl.pallas_call(
        run,
        out_shape=outs,
        in_specs=specs,
        out_specs=out_specs,
        scratch_shapes=scratches,
        cost_estimate=pl.CostEstimate(flops=flops, bytes_accessed=0, transcendentals=0),
        compiler_params=pltpu.CompilerParams(vmem_limit_bytes=limit * MIB),
    )(*args)


def wrapped(value, count):
    return jnp.where(value >= count, value - count, value)


def weights_and_tokens(tokens, gain, query, key, value, out, weights):
    rows = tokens.shape[0]
    cols = query.shape[1]
    for place, weight in enumerate((query, key, value)):
        weights[:, place * cols : (place + 1) * cols] = weight[...]
    block = out.shape[2]
    for z in range(NZ):
        cols = slice(z * block, (z + 1) * block)
        out[z, :rows, :] = (tokens[:, cols].astype(F32) * gain[:, cols]).astype(BF)


def pack_body(index, after, gate, up, down, out):
    block, size = gate.shape
    half = down.shape[1] // 2
    out[:block, :size] = gate[...]
    out[:block, size:] = up[...]
    out[block : block + size, :] = down[:, :half]
    out[block + size :, :] = down[:, half:]


def turned(row, rows):
    shape = (rows, row.shape[1])
    same = lax.broadcasted_iota(jnp.int32, shape, 0) == lax.broadcasted_iota(jnp.int32, shape, 1)
    return jnp.sum(jnp.where(same, row, 0.0), axis=1, keepdims=True)


def spread_body(
    index, tokens, gain, query, key, value, decay_weight, beta_weight, rate, ids, prob, logit,
    far_out, far_weights, far_factors, out, weights, factors, stored,
):
    stores = [
        pltpu.make_async_copy(near, far, stored.at[place])
        for place, (near, far) in enumerate(
            ((weights, far_weights), (out, far_out), (factors, far_factors))
        )
    ]
    weights_and_tokens(tokens, gain, query, key, value, out, weights)
    stores[0].start()
    rows, width = tokens.shape
    block = out.shape[2]
    wide = tokens[...].astype(F32)
    row_scale = lax.rsqrt(jnp.sum(wide * wide, axis=1, keepdims=True) / width + EPS)
    gained = (wide * gain[...]).astype(BF)
    over_width = (((1,), (1,)), ((), ()))
    heads = rate.shape[1]
    factor_lane = lax.broadcasted_iota(jnp.int32, factors.shape, 1)
    table = jnp.where(factor_lane == 0, row_scale, 0.0)

    def own_heads(weight):
        product = lax.dot_general(gained, weight[...], over_width, preferred_element_type=F32)
        lane = lax.broadcasted_iota(jnp.int32, product.shape, 1)
        columns = []
        for h in range(heads):
            own = lane == index[2] * heads + h
            columns.append(jnp.sum(jnp.where(own, product, 0.0), axis=1, keepdims=True) * row_scale)
        return columns

    for h, column in enumerate(own_heads(decay_weight)):
        soft = jnp.maximum(column, 0.0) + jnp.log1p(jnp.exp(-jnp.abs(column)))
        table = jnp.where(factor_lane == 1 + h, jnp.exp(-rate[:, h : h + 1] * soft), table)
    for h, column in enumerate(own_heads(beta_weight)):
        table = jnp.where(factor_lane == 1 + heads + h, 1.0 / (1.0 + jnp.exp(-column)), table)
    factors[...] = table

    picks = [ids[k : k + 1, :].astype(F32) for k in range(2)]
    pick_cols = [turned(pick, rows) for pick in picks]
    shape = (rows, rows)
    earlier = lax.broadcasted_iota(jnp.int32, shape, 0) < lax.broadcasted_iota(jnp.int32, shape, 1)
    powers = [jnp.exp(logit[k : k + 1, :]) for k in range(2)]
    total = powers[0] + powers[1]
    lines = []
    for k in range(2):
        named = jnp.zeros(shape, F32)
        for column in pick_cols:
            named = named + jnp.where(earlier & (column == picks[k]), 1.0, 0.0)
        lines.append(picks[k] * CAP + jnp.sum(named, axis=0, keepdims=True))
    for k in range(2):
        route = prob[...] * powers[k] / total
        high = route.astype(BF).astype(F32)
        lines += [high, route - high]
    line = lax.broadcasted_iota(jnp.int32, (8, rows), 0)
    table = jnp.zeros((8, rows), F32)
    for number, values in enumerate(lines):
        table = jnp.where(line == number, values, table)
    shape = (rows, block)
    lane = lax.broadcasted_iota(jnp.int32, shape, 1)
    spot = lane == lax.broadcasted_iota(jnp.int32, shape, 0) + index[0] * rows
    spot = jnp.where(spot, 1.0, 0.0).astype(BF)
    meta = jnp.dot(table.astype(BF), spot, preferred_element_type=F32).astype(BF)
    for z in range(NZ):
        out[z, rows:, :] = meta
    stores[1].start()
    stores[2].start()
    for store in stores:
        store.wait()


def project_body(index, arrived, w0, w1, w2, w3, out, route):
    groups, rows, _ = out.shape
    tokens = groups * rows
    routing = arrived[0, rows:, :tokens].astype(F32)
    for z in range(1, groups):
        routing = routing + arrived[z, rows:, :tokens].astype(F32)
    route[...] = routing
    total = None
    for step, weight in enumerate((w0, w1, w2, w3)):
        size = weight.shape[0]
        place = pl.multiple_of(wrapped(index[1] + step, NX) * size, size)
        left = arrived[:, :rows, pl.ds(place, size)].astype(F32).reshape(tokens, size).astype(BF)
        part = jnp.dot(left, weight[...], preferred_element_type=F32)
        total = part if total is None else total + part
    out[...] = total.reshape(groups, rows, -1).astype(BF)


def recall_body(index, arrived, factors, state, head_gain, weight, out, keys, changes):
    rows, heads, size = state.shape[:3]
    cols = heads * size
    summed = arrived[0].astype(F32)
    for z in range(1, NZ):
        summed = summed + arrived[z].astype(F32)
    summed = summed * factors[:, 0:1]
    line = lax.broadcasted_iota(jnp.int32, (rows, size), 0)
    head_rows = []
    for h in range(heads):
        own = slice(h * size, (h + 1) * size)
        query = unit_rows(summed[:, own]) * size ** (-0.5)
        key = unit_rows(summed[:, cols + h * size : cols + (h + 1) * size])
        value = summed[:, 2 * cols + h * size : 2 * cols + (h + 1) * size]
        both = jnp.concatenate((key, query), axis=0).astype(BF)
        recalled = jnp.zeros((rows, size), F32)
        asked = jnp.zeros((rows, size), F32)
        for b in range(0, rows, 2):
            pair = jnp.concatenate((state[b, h], state[b + 1, h]), axis=1).astype(BF)
            product = jnp.dot(both, pair, preferred_element_type=F32)
            for side in range(2):
                lanes = slice(side * size, (side + 1) * size)
                recalled = jnp.where(line == b + side, product[:rows, lanes], recalled)
                asked = jnp.where(line == b + side, product[rows:, lanes], asked)
        fade = factors[:, 1 + h : 2 + h]
        gate = factors[:, 1 + heads + h : 2 + heads + h]
        change = gate * (value - fade * recalled)
        keys[:, own] = key
        changes[:, own] = change
        result = fade * asked + jnp.sum(query * key, axis=1, keepdims=True) * change
        mean_sq = jnp.mean(result * result, axis=1, keepdims=True)
        head_rows.append(result * lax.rsqrt(mean_sq + EPS) * head_gain[...])
    left = jnp.concatenate(head_rows, axis=1).astype(BF)
    block = out.shape[2]
    for t in range(NT):
        right = weight[:, t * block : (t + 1) * block]
        out[t] = jnp.dot(left, right, preferred_element_type=F32).astype(BF)


def update_body(index, keys, changes, factors, state, new_state):
    rows, heads, size = state.shape[:3]
    line = lax.broadcasted_iota(jnp.int32, (rows, size), 0)
    line = jnp.concatenate((line, line, line), axis=0)
    for h in range(heads):
        own = slice(h * size, (h + 1) * size)
        key, change = keys[:, own], changes[:, own]
        key_high = key.astype(BF).astype(F32)
        high = change.astype(BF).astype(F32)
        left = jnp.concatenate((key_high, key - key_high, key_high), axis=0).T.astype(BF)
        right = jnp.concatenate((high, high, change - high), axis=0)
        for b in range(0, rows, 2):
            pair = [jnp.where(line == b + side, right, 0.0) for side in range(2)]
            pair = jnp.concatenate(pair, axis=1).astype(BF)
            product = jnp.dot(left, pair, preferred_element_type=F32)
            for side in range(2):
                fade = factors[b + side : b + side + 1, 1 + h : 2 + h]
                grown = product[:, side * size : (side + 1) * size]
                new_state[b + side, h] = fade * state[b + side, h] + grown


def middle_body(index, arrived, tokens, middle, out):
    block = middle.shape[1]
    summed = arrived[0].astype(F32)
    for t in range(1, NT):
        summed = summed + arrived[t].astype(F32)
    place = pl.multiple_of(index[2] * block, block)
    total = tokens[:, pl.ds(place, block)].astype(F32) + summed
    middle[...] = total
    narrow = total.astype(BF)
    for z in range(NZ):
        out[z] = narrow


def slots_of(route, zi):
    tokens = route.shape[1]
    lane = lax.broadcasted_iota(jnp.int32, (1, tokens), 1)
    source = jnp.zeros((1, tokens), jnp.int32)
    for z in range(1, NZ):
        source = source + jnp.where(lane >= z * (tokens // NZ), 1, 0)
    slots = []
    for k in range(2):
        code = route[k : k + 1, :].astype(jnp.int32) - zi * (NX * CAP)
        expert = jnp.zeros((1, tokens), jnp.int32)
        for x in range(1, NX):
            expert = expert + jnp.where(code >= x * CAP, 1, 0)
        slot = expert * (NZ * CAP) + source * CAP + (code - expert * CAP)
        slots.append(jnp.where((code >= 0) & (code < NX * CAP), slot, -1))
    return slots


def dispatch_body(index, arrived, gain, g0, g1, g2, g3, route, after, out):
    rows = arrived.shape[1]
    tokens = NZ * rows
    block = arrived.shape[2]
    half = block // 2
    wide = arrived[...].astype(F32).reshape(tokens, block)
    narrow = wide.astype(BF)
    routing = route[...]
    slot0, slot1 = slots_of(routing, index[0])
    place = lax.broadcasted_iota(jnp.int32, (NX * rows, tokens), 0)
    picks = jnp.where((place == slot0) | (place == slot1), 1.0, 0.0).astype(BF)
    chosen = jnp.dot(picks, narrow, preferred_element_type=F32).astype(BF)
    square = wide * wide
    high = square.astype(BF)
    ones = jnp.ones((8, block), BF)
    over_block = (((1,), (1,)), ((), ()))
    square = sum(
        lax.dot_general(ones, part, over_block, preferred_element_type=F32)
        for part in (high, (square - high.astype(F32)).astype(BF))
    )
    high = square.astype(BF).astype(F32)
    first = lax.broadcasted_iota(jnp.int32, square.shape, 0) == 0
    square = jnp.where(first, high, square - high).astype(BF)
    for x in range(NX):
        own = chosen[x * rows : (x + 1) * rows]
        for y in range(NY):
            out[x, y, :rows, :] = own[:, :half]
            out[x, y, rows : 2 * rows, :] = own[:, half:]
            out[x, y, 4 * rows :, :tokens] = square
            out[x, y, 4 * rows :, tokens:] = jnp.zeros((8, half - tokens), BF)
    scaled = (wide * gain[...]).astype(BF)
    for step, weight in enumerate((g0, g1, g2, g3)):
        part = jnp.dot(scaled, weight[...], preferred_element_type=F32)
        x = wrapped(index[1] + step, NX)
        out[x, :, 2 * rows : 4 * rows, :] = part.reshape(NY, 2 * rows, half).astype(BF)


def expert_body(index, arrived, partner, gain, gate, up, down, away, hidden, dense):
    rows, block = away.shape[2:]
    size = gate.shape[1]
    half = block // 2
    width = gate.shape[0]
    slots = NX * rows
    squares = jnp.zeros((slots, half), F32)
    gate_sum = jnp.zeros((slots, gate.shape[1]), F32)
    up_sum = jnp.zeros((slots, gate.shape[1]), F32)
    for y in range(NY):
        for source, core in ((arrived, index[3]), (partner, 1 - index[3])):
            for part in range(2):
                wide = source[:, y, part * rows : (part + 1) * rows, :].astype(F32)
                wide = wide.reshape(slots, half)
                squares = squares + wide * wide
                place = pl.multiple_of((2 * y + core) * block + part * half, half)
                left = (wide * gain[:, pl.ds(place, half)]).astype(BF)
                own = pl.ds(place, half)
                gate_sum += jnp.dot(left, gate[own, :], preferred_element_type=F32)
                up_sum += jnp.dot(left, up[own, :], preferred_element_type=F32)
    scale = lax.rsqrt(jnp.sum(squares, axis=1, keepdims=True) / width + EPS)
    result = (silu(gate_sum * scale) * (up_sum * scale)).astype(BF)
    hidden[...] = result
    for y in range(NY):
        place = pl.multiple_of((2 * y + 1 - index[3]) * block, block)
        part = jnp.dot(result, down[:, pl.ds(place, block)], preferred_element_type=F32)
        away[:, y] = part.reshape(NX, rows, block).astype(BF)
    tokens = NZ * rows
    lane = lax.broadcasted_iota(jnp.int32, (rows, tokens), 1)
    own = lane == lax.broadcasted_iota(jnp.int32, (rows, tokens), 0) + index[2] * rows
    for x in range(NX):
        summed = jnp.zeros((rows, half), F32)
        square = jnp.zeros((8, tokens), F32)
        for y in range(NY):
            for source in (arrived, partner):
                both = source[x, y, 2 * rows : 4 * rows, :].astype(F32)
                summed = summed + jnp.where(index[3] == 0, both[:rows], both[rows:])
                square = square + source[x, y, 4 * rows :, :tokens].astype(F32)
        square = square[0:1, :] + square[1:2, :]
        square = jnp.sum(jnp.where(own, square, 0.0), axis=1, keepdims=True)
        summed = summed * lax.rsqrt(square / width + EPS)
        result = (silu(summed[:, : half // 2]) * summed[:, half // 2 :]).astype(BF)
        dense[x] = result
        away[x, NY, :, :size] = result
        away[x, NY, :, size:] = jnp.zeros((rows, block - size), BF)


def result_body(index, hidden, dense, away, down, out):
    rows, block = away.shape[2:]
    size = dense.shape[2]
    own_place = pl.multiple_of(block + index[3] * size, size)
    far_place = pl.multiple_of(block + (1 - index[3]) * size, size)
    for y in range(NY):
        place = pl.multiple_of((2 * y + index[3]) * block, block)
        part = jnp.dot(hidden[...], down[:, pl.ds(place, block)], preferred_element_type=F32)
        part = part.reshape(NX, rows, block) + away[:, y].astype(F32)
        out[:, y, :, :block] = part.astype(BF)
        out[:, y, :, pl.ds(own_place, size)] = dense[...]
        out[:, y, :, pl.ds(far_place, size)] = away[:, NY, :, :size]


def combine_body(index, arrived, route, d0, d1, d2, d3, mix, out):
    rows = arrived.shape[2]
    block = out.shape[2]
    tokens = NZ * rows
    results = []
    for x in range(NX):
        summed = arrived[x, 0, :, :block].astype(F32)
        for y in range(1, NY):
            summed = summed + arrived[x, y, :, :block].astype(F32)
        results.append(summed)
    results = jnp.concatenate(results, axis=0).astype(BF)
    routing = route[...]
    slot0, slot1 = slots_of(routing, index[0])
    place = lax.broadcasted_iota(jnp.int32, (NX * rows, tokens), 0)
    total = jnp.zeros((tokens, block), F32)
    for k in range(2):
        share = jnp.where(place == slot0, routing[2 + k : 3 + k, :], 0.0)
        share = jnp.where(place == slot1, routing[4 + k : 5 + k, :], share).astype(BF)
        total += lax.dot_general(
            share, results, (((0,), (0,)), ((), ())), preferred_element_type=F32
        )
    gate = 1.0 / (1.0 + jnp.exp(-mix[...]))
    total = total.reshape(NY, 2, rows, block)
    size = (arrived.shape[3] - block) // 2
    for core in range(2):
        lower = jnp.zeros((NY * rows, block // 2), F32)
        upper = jnp.zeros((NY * rows, block // 2), F32)
        lanes = slice(block + core * size, block + (core + 1) * size)
        for step, weight in enumerate((d0, d1, d2, d3)):
            x = wrapped(index[1] + step, NX)
            left = arrived[x, :, :, lanes].astype(F32).reshape(NY * rows, size).astype(BF)
            lower += jnp.dot(left, weight[:size, :], preferred_element_type=F32)
            upper += jnp.dot(left, weight[size:, :], preferred_element_type=F32)
        dense = gate * jnp.concatenate((lower, upper), axis=1)
        for y in range(NY):
            own = dense[y * rows : (y + 1) * rows] + total[y, core]
            out[2 * y + core] = own.astype(BF)


def final_body(index, arrived, middle, out):
    summed = arrived[0].astype(F32)
    for z in range(1, NZ):
        summed = summed + arrived[z].astype(F32)
    out[...] = (middle[...] + summed).astype(BF)


def per_device(
    tokens,
    delta_state,
    attn_gain,
    query_weight,
    key_weight,
    value_weight,
    decay_weight,
    beta_weight,
    decay_rate,
    head_gain,
    output_weight,
    ffn_gain,
    expert_ids,
    group_prob,
    expert_logit,
    expert_gate,
    expert_up,
    expert_down,
    dense_gate,
    dense_up,
    dense_down,
    dense_mix,
):
    rows, width = tokens.shape
    heads, size = delta_state.shape[1:3]
    cols = heads * size
    block = width // NT
    half = block // 2

    def shape(*dims, dtype=BF):
        return jax.ShapeDtypeStruct(dims, dtype)

    def own_block(ref, index):
        place = pl.multiple_of(index[2] * block, block)
        return ref.at[:, pl.ds(place, block)]

    first = (
        shape(NZ, rows + 8, block),
        shape(query_weight.shape[0], 3 * cols),
        shape(rows, 128, dtype=F32),
    )
    message, own_weights, factors = kernel(
        spread_body,
        tuple(pltpu.HBM(made.shape, made.dtype) for made in first),
        tokens,
        attn_gain[None],
        query_weight,
        key_weight,
        value_weight,
        decay_weight.T,
        beta_weight.T,
        decay_rate[None],
        expert_ids.T,
        group_prob[None],
        expert_logit.T,
        far=range(11),
        far_outs=range(3),
        scratch=[pltpu.VMEM(made.shape, made.dtype) for made in first]
        + [pltpu.SemaphoreType.DMA((3,))],
    )
    qkv_weights = from_neighbours(own_weights, "x")
    spread = exchange(message, "z")
    (packed,) = kernel(
        pack_body,
        (shape(block + dense_gate.shape[1] * 2, half),),
        message,
        dense_gate,
        dense_up,
        dense_down,
        plain=(0,),
        far=(1, 2, 3),
    )
    dense_weights = from_neighbours(packed, "x")
    part, route_rows = kernel(
        project_body,
        (shape(NZ, rows, 3 * cols), pltpu.HBM((8, NZ * rows), F32)),
        spread,
        *qkv_weights,
        held=(1, 2, 3, 4),
        flops=2 * NZ * rows * block * 3 * cols,
    )
    arrived = exchange(part, "z")
    attn_part, keys, changes = kernel(
        recall_body,
        (
            shape(NT, rows, block),
            pltpu.HBM((rows, cols), F32),
            pltpu.HBM((rows, cols), F32),
        ),
        arrived,
        factors,
        delta_state,
        head_gain[None],
        output_weight,
        far=(1, 3, 4),
        flops=2 * rows * cols * width,
    )
    (new_state,) = kernel(
        update_body,
        (shape(*delta_state.shape, dtype=F32),),
        keys,
        changes,
        factors,
        delta_state,
        far=range(4),
        flops=10**8,
        limit=24,
    )
    arrived = exchange(attn_part, ("y", "c"))
    middle, message = kernel(
        middle_body,
        (shape(rows, block, dtype=F32), shape(NZ, rows, block)),
        arrived,
        tokens,
    )

    swap = [(0, 1), (1, 0)]
    arrived = exchange(message, "z")
    (message,) = kernel(
        dispatch_body,
        (shape(NX, NY, 4 * rows + 8, half),),
        arrived,
        ffn_gain[None],
        *dense_weights,
        route_rows,
        new_state,
        plain=(7,),
        far=range(1, 7),
        parts={
            1: ((1, block), own_block),
            **{n: ((block, half), lambda ref, index: ref.at[:block]) for n in range(2, 6)},
        },
        flops=2 * NZ * rows * block * 2 * block,
    )
    sides = ("x", "y")
    arrived = exchange(message.reshape(NX * NY, -1, half), sides)
    partner = lax.ppermute(arrived, "c", swap).reshape(message.shape)
    away, hidden, dense = kernel(
        expert_body,
        (shape(NX, NY + 1, rows, block), shape(NX * rows, 128), shape(NX, rows, 128)),
        arrived.reshape(message.shape),
        partner,
        ffn_gain[None],
        expert_gate[0],
        expert_up[0],
        expert_down[0],
        far=(2,),
        flops=5 * NX * rows * width * 128,
    )
    (message,) = kernel(
        result_body,
        (shape(NX, NY, rows, block + 2 * 128),),
        hidden,
        dense,
        lax.ppermute(away, "c", swap),
        expert_down[0],
        flops=NX * rows * width * 128,
    )
    arrived = exchange(message.reshape(NX * NY, rows, -1), sides)
    (message,) = kernel(
        combine_body,
        (shape(NZ, rows, block),),
        arrived.reshape(message.shape),
        route_rows,
        *dense_weights,
        dense_mix[None],
        far=range(1, 7),
        parts={n: ((half, half), lambda ref, index: ref.at[block:]) for n in range(2, 6)},
        flops=2 * NZ * rows * block * block,
    )
    arrived = exchange(message, "z")
    (mixed_out,) = kernel(final_body, (shape(rows, block),), arrived, middle)
    return (mixed_out, new_state)


def solution(mesh):
    fine = Mesh(mesh.devices.reshape(NZ, NX, 4, 2), ("z", "x", "y", "c"))
    ep, tp = ("z", "x"), ("y", "c")

    return jax.shard_map(
        per_device,
        mesh=fine,
        in_specs=(
            P(ep, None),
            P(ep, tp, None, None),
            P(),
            P(ep, tp),
            P(ep, tp),
            P(ep, tp),
            P(),
            P(),
            P(tp),
            P(),
            P(tp, None),
            P(),
            P(ep, None),
            P(ep),
            P(ep, None),
            P(ep, None, tp),
            P(ep, None, tp),
            P(ep, tp, None),
            P(tp, ep),
            P(tp, ep),
            P(ep, tp),
            P(tp),
        ),
        out_specs=(P(ep, tp), P(ep, tp, None, None)),
        check_vma=False,
    )
```

```python
import jax
import jax.numpy as jnp
from jax import lax
from jax.experimental import pallas as pl
from jax.experimental.pallas import tpu as pltpu
from jax.sharding import Mesh, PartitionSpec as P

EPS = 1e-06
BF = jnp.bfloat16
F32 = jnp.float32
NZ, NX, NY, NT = 8, 4, 4, 8
CAP = 3
MIB = 1 << 20


def exchange(tiles, axes):
    return lax.all_to_all(tiles, axes, split_axis=0, concat_axis=0, tiled=True)


def from_neighbours(shard, axis):
    count = lax.axis_size(axis)
    parts = [shard]
    for step in range(1, count):
        pairs = [(source, (source - step) % count) for source in range(count)]
        parts.append(lax.ppermute(shard, axis, pairs))
    return parts


def unit_rows(values):
    return values * lax.rsqrt(jnp.sum(values * values, axis=-1, keepdims=True) + EPS)


def silu(values):
    return values / (1.0 + jnp.exp(-values))


class Late:
    def __init__(self, source, near, done):
        self.near = near
        self.copy = pltpu.make_async_copy(source, near, done)
        self.copy.start()
        self.waits = True

    def arrive(self):
        if self.waits:
            self.copy.wait()
            self.waits = False
        return self.near

    def __getitem__(self, where):
        return self.arrive()[where]

    @property
    def shape(self):
        return self.near.shape


def kernel(
    body, outs, *args, far=(), plain=(), held=(), parts=None, far_outs=(), scratch=(), flops=0, limit=16
):
    parts = parts or {}
    far, plain, held = tuple(far), tuple(plain), tuple(held)
    nears = [parts[n][0] if n in parts else args[n].shape for n in far]

    def run(*refs):
        sides = [lax.axis_index(name) for name in ("z", "x", "y", "c")]
        index = (sides[0], sides[1], sides[2] * 2 + sides[3], sides[3])
        refs = list(refs)
        ins, refs = refs[: len(args)], refs[len(args) :]
        dones = refs.pop() if far else None
        buffers = refs[len(refs) - len(far) :]
        refs = refs[: len(refs) - len(far)]
        for place, number in enumerate(far):
            source = ins[number]
            if number in parts:
                source = parts[number][1](source, index)
            ins[number] = Late(source, buffers[place], dones.at[place])
        body(index, *ins, *refs)
        for number in far:
            ins[number].arrive()

    specs = [
        pl.BlockSpec(memory_space=pltpu.HBM if number in far or number in plain else pltpu.VMEM)
        for number in range(len(args))
    ]
    out_specs = [
        pl.BlockSpec(memory_space=pltpu.HBM if number in far_outs else pltpu.VMEM)
        for number in range(len(outs))
    ]
    scratches = list(scratch) + [pltpu.VMEM(near, args[n].dtype) for n, near in zip(far, nears)]
    if far:
        scratches.append(pltpu.SemaphoreType.DMA((len(far),)))
    args = [
        pltpu.with_memory_space_constraint(arg, pltpu.HBM) if n in far + plain + held else arg
        for n, arg in enumerate(args)
    ]
    return pl.pallas_call(
        run,
        out_shape=outs,
        in_specs=specs,
        out_specs=out_specs,
        scratch_shapes=scratches,
        cost_estimate=pl.CostEstimate(flops=flops, bytes_accessed=0, transcendentals=0),
        compiler_params=pltpu.CompilerParams(vmem_limit_bytes=limit * MIB),
    )(*args)


def wrapped(value, count):
    return jnp.where(value >= count, value - count, value)


def weights_and_tokens(tokens, gain, query, key, value, out, weights):
    rows = tokens.shape[0]
    cols = query.shape[1]
    for place, weight in enumerate((query, key, value)):
        weights[:, place * cols : (place + 1) * cols] = weight[...]
    block = out.shape[2]
    for z in range(NZ):
        cols = slice(z * block, (z + 1) * block)
        out[z, :rows, :] = (tokens[:, cols].astype(F32) * gain[:, cols]).astype(BF)


def pack_body(index, after, gate, up, down, out):
    block, size = gate.shape
    half = down.shape[1] // 2
    out[:block, :size] = gate[...]
    out[:block, size:] = up[...]
    out[block : block + size, :] = down[:, :half]
    out[block + size :, :] = down[:, half:]


def turned(row, rows):
    shape = (rows, row.shape[1])
    same = lax.broadcasted_iota(jnp.int32, shape, 0) == lax.broadcasted_iota(jnp.int32, shape, 1)
    return jnp.sum(jnp.where(same, row, 0.0), axis=1, keepdims=True)


def spread_body(
    index, tokens, gain, query, key, value, decay_weight, beta_weight, rate, ids, prob, logit,
    far_out, far_weights, far_factors, out, weights, factors, stored,
):
    stores = [
        pltpu.make_async_copy(near, far, stored.at[place])
        for place, (near, far) in enumerate(
            ((weights, far_weights), (out, far_out), (factors, far_factors))
        )
    ]
    weights_and_tokens(tokens, gain, query, key, value, out, weights)
    stores[0].start()
    rows, width = tokens.shape
    block = out.shape[2]
    wide = tokens[...].astype(F32)
    row_scale = lax.rsqrt(jnp.sum(wide * wide, axis=1, keepdims=True) / width + EPS)
    gained = (wide * gain[...]).astype(BF)
    over_width = (((1,), (1,)), ((), ()))
    heads = rate.shape[1]
    factor_lane = lax.broadcasted_iota(jnp.int32, factors.shape, 1)
    table = jnp.where(factor_lane == 0, row_scale, 0.0)

    both = jnp.concatenate((decay_weight[...], beta_weight[...]), axis=0)
    product = lax.dot_general(gained, both, over_width, preferred_element_type=F32)
    product_lane = lax.broadcasted_iota(jnp.int32, product.shape, 1)

    def own_head(place):
        own = jnp.where(product_lane == place, product, 0.0)
        return jnp.sum(own, axis=1, keepdims=True) * row_scale

    for h in range(heads):
        place = index[2] * heads + h
        column = own_head(place)
        soft = jnp.maximum(column, 0.0) + jnp.log1p(jnp.exp(-jnp.abs(column)))
        table = jnp.where(factor_lane == 1 + h, jnp.exp(-rate[:, h : h + 1] * soft), table)
        column = own_head(decay_weight.shape[0] + place)
        table = jnp.where(factor_lane == 1 + heads + h, 1.0 / (1.0 + jnp.exp(-column)), table)
    factors[...] = table

    picks = [ids[k : k + 1, :].astype(F32) for k in range(2)]
    pick_cols = [turned(pick, rows) for pick in picks]
    shape = (rows, rows)
    earlier = lax.broadcasted_iota(jnp.int32, shape, 0) < lax.broadcasted_iota(jnp.int32, shape, 1)
    powers = [jnp.exp(logit[k : k + 1, :]) for k in range(2)]
    total = powers[0] + powers[1]
    lines = []
    for k in range(2):
        named = jnp.zeros(shape, F32)
        for column in pick_cols:
            named = named + jnp.where(earlier & (column == picks[k]), 1.0, 0.0)
        lines.append(picks[k] * CAP + jnp.sum(named, axis=0, keepdims=True))
    for k in range(2):
        route = prob[...] * powers[k] / total
        high = route.astype(BF).astype(F32)
        lines += [high, route - high]
    line = lax.broadcasted_iota(jnp.int32, (8, rows), 0)
    table = jnp.zeros((8, rows), F32)
    for number, values in enumerate(lines):
        table = jnp.where(line == number, values, table)
    shape = (rows, block)
    lane = lax.broadcasted_iota(jnp.int32, shape, 1)
    spot = lane == lax.broadcasted_iota(jnp.int32, shape, 0) + index[0] * rows
    spot = jnp.where(spot, 1.0, 0.0).astype(BF)
    meta = jnp.dot(table.astype(BF), spot, preferred_element_type=F32).astype(BF)
    for z in range(NZ):
        out[z, rows:, :] = meta
    stores[1].start()
    stores[2].start()
    for store in stores:
        store.wait()


def project_body(index, arrived, w0, w1, w2, w3, out):
    groups, rows, _ = out.shape
    tokens = groups * rows
    total = None
    for step, weight in enumerate((w0, w1, w2, w3)):
        size = weight.shape[0]
        place = pl.multiple_of(wrapped(index[1] + step, NX) * size, size)
        left = arrived[:, :rows, pl.ds(place, size)].astype(F32).reshape(tokens, size).astype(BF)
        part = jnp.dot(left, weight[...], preferred_element_type=F32)
        total = part if total is None else total + part
    out[...] = total.reshape(groups, rows, -1).astype(BF)


def recall_body(index, arrived, factors, state, head_gain, weight, out, keys, changes):
    rows, heads, size = state.shape[:3]
    cols = heads * size
    summed = arrived[0].astype(F32)
    for z in range(1, NZ):
        summed = summed + arrived[z].astype(F32)
    summed = summed * factors[:, 0:1]
    line = lax.broadcasted_iota(jnp.int32, (rows, size), 0)
    head_rows = []
    for h in range(heads):
        own = slice(h * size, (h + 1) * size)
        query = unit_rows(summed[:, own]) * size ** (-0.5)
        key = unit_rows(summed[:, cols + h * size : cols + (h + 1) * size])
        value = summed[:, 2 * cols + h * size : 2 * cols + (h + 1) * size]
        both = jnp.concatenate((key, query), axis=0).astype(BF)
        recalled = jnp.zeros((rows, size), F32)
        asked = jnp.zeros((rows, size), F32)
        for b in range(0, rows, 2):
            pair = jnp.concatenate((state[b, h], state[b + 1, h]), axis=1).astype(BF)
            product = jnp.dot(both, pair, preferred_element_type=F32)
            for side in range(2):
                lanes = slice(side * size, (side + 1) * size)
                recalled = jnp.where(line == b + side, product[:rows, lanes], recalled)
                asked = jnp.where(line == b + side, product[rows:, lanes], asked)
        fade = factors[:, 1 + h : 2 + h]
        gate = factors[:, 1 + heads + h : 2 + heads + h]
        change = gate * (value - fade * recalled)
        keys[:, own] = key
        changes[:, own] = change
        result = fade * asked + jnp.sum(query * key, axis=1, keepdims=True) * change
        mean_sq = jnp.mean(result * result, axis=1, keepdims=True)
        head_rows.append(result * lax.rsqrt(mean_sq + EPS) * head_gain[...])
    left = jnp.concatenate(head_rows, axis=1).astype(BF)
    block = out.shape[2]
    for t in range(NT):
        right = weight[:, t * block : (t + 1) * block]
        out[t] = jnp.dot(left, right, preferred_element_type=F32).astype(BF)


def update_body(index, keys, changes, factors, state, spread, new_state, route):
    rows, heads, size = state.shape[:3]
    tokens = route.shape[1]
    routing = spread[0, :, :tokens].astype(F32)
    for z in range(1, NZ):
        routing = routing + spread[z, :, :tokens].astype(F32)
    route[...] = routing
    line = lax.broadcasted_iota(jnp.int32, (rows, size), 0)
    line = jnp.concatenate((line, line, line), axis=0)
    for h in range(heads):
        own = slice(h * size, (h + 1) * size)
        key, change = keys[:, own], changes[:, own]
        key_high = key.astype(BF).astype(F32)
        high = change.astype(BF).astype(F32)
        left = jnp.concatenate((key_high, key - key_high, key_high), axis=0).T.astype(BF)
        right = jnp.concatenate((high, high, change - high), axis=0)
        for b in range(0, rows, 2):
            pair = [jnp.where(line == b + side, right, 0.0) for side in range(2)]
            pair = jnp.concatenate(pair, axis=1).astype(BF)
            product = jnp.dot(left, pair, preferred_element_type=F32)
            for side in range(2):
                fade = factors[b + side : b + side + 1, 1 + h : 2 + h]
                grown = product[:, side * size : (side + 1) * size]
                new_state[b + side, h] = fade * state[b + side, h] + grown


def middle_body(index, arrived, tokens, middle, out):
    block = middle.shape[1]
    summed = arrived[0].astype(F32)
    for t in range(1, NT):
        summed = summed + arrived[t].astype(F32)
    place = pl.multiple_of(index[2] * block, block)
    total = tokens[:, pl.ds(place, block)].astype(F32) + summed
    middle[...] = total
    narrow = total.astype(BF)
    for z in range(NZ):
        out[z] = narrow


def slots_of(route, zi):
    tokens = route.shape[1]
    lane = lax.broadcasted_iota(jnp.int32, (1, tokens), 1)
    source = jnp.zeros((1, tokens), jnp.int32)
    for z in range(1, NZ):
        source = source + jnp.where(lane >= z * (tokens // NZ), 1, 0)
    slots = []
    for k in range(2):
        code = route[k : k + 1, :].astype(jnp.int32) - zi * (NX * CAP)
        expert = jnp.zeros((1, tokens), jnp.int32)
        for x in range(1, NX):
            expert = expert + jnp.where(code >= x * CAP, 1, 0)
        slot = expert * (NZ * CAP) + source * CAP + (code - expert * CAP)
        slots.append(jnp.where((code >= 0) & (code < NX * CAP), slot, -1))
    return slots


def dispatch_body(index, arrived, gain, g0, g1, g2, g3, route, out):
    rows = arrived.shape[1]
    tokens = NZ * rows
    block = arrived.shape[2]
    half = block // 2
    wide = arrived[...].astype(F32).reshape(tokens, block)
    narrow = wide.astype(BF)
    routing = route[...]
    slot0, slot1 = slots_of(routing, index[0])
    place = lax.broadcasted_iota(jnp.int32, (NX * rows, tokens), 0)
    picks = jnp.where((place == slot0) | (place == slot1), 1.0, 0.0).astype(BF)
    chosen = jnp.dot(picks, narrow, preferred_element_type=F32).astype(BF)
    square = wide * wide
    high = square.astype(BF)
    ones = jnp.ones((8, block), BF)
    over_block = (((1,), (1,)), ((), ()))
    square = sum(
        lax.dot_general(ones, part, over_block, preferred_element_type=F32)
        for part in (high, (square - high.astype(F32)).astype(BF))
    )
    high = square.astype(BF).astype(F32)
    first = lax.broadcasted_iota(jnp.int32, square.shape, 0) == 0
    square = jnp.where(first, high, square - high).astype(BF)
    for x in range(NX):
        own = chosen[x * rows : (x + 1) * rows]
        for y in range(NY):
            out[x, y, :rows, :] = own[:, :half]
            out[x, y, rows : 2 * rows, :] = own[:, half:]
            out[x, y, 4 * rows :, :tokens] = square
            out[x, y, 4 * rows :, tokens:] = jnp.zeros((8, half - tokens), BF)
    scaled = (wide * gain[...]).astype(BF)
    for step, weight in enumerate((g0, g1, g2, g3)):
        part = jnp.dot(scaled, weight[...], preferred_element_type=F32)
        x = wrapped(index[1] + step, NX)
        out[x, :, 2 * rows : 4 * rows, :] = part.reshape(NY, 2 * rows, half).astype(BF)


def expert_body(index, arrived, partner, gain, gate, up, down, away, hidden, dense):
    rows, block = away.shape[2:]
    size = gate.shape[1]
    half = block // 2
    width = gate.shape[0]
    slots = NX * rows
    squares = jnp.zeros((slots, half), F32)
    gate_sum = jnp.zeros((slots, gate.shape[1]), F32)
    up_sum = jnp.zeros((slots, gate.shape[1]), F32)
    for y in range(NY):
        for source, core in ((arrived, index[3]), (partner, 1 - index[3])):
            for part in range(2):
                wide = source[:, y, part * rows : (part + 1) * rows, :].astype(F32)
                wide = wide.reshape(slots, half)
                squares = squares + wide * wide
                place = pl.multiple_of((2 * y + core) * block + part * half, half)
                left = (wide * gain[:, pl.ds(place, half)]).astype(BF)
                own = pl.ds(place, half)
                gate_sum += jnp.dot(left, gate[own, :], preferred_element_type=F32)
                up_sum += jnp.dot(left, up[own, :], preferred_element_type=F32)
    scale = lax.rsqrt(jnp.sum(squares, axis=1, keepdims=True) / width + EPS)
    result = (silu(gate_sum * scale) * (up_sum * scale)).astype(BF)
    hidden[...] = result
    for y in range(NY):
        place = pl.multiple_of((2 * y + 1 - index[3]) * block, block)
        part = jnp.dot(result, down[:, pl.ds(place, block)], preferred_element_type=F32)
        away[:, y] = part.reshape(NX, rows, block).astype(BF)
    tokens = NZ * rows
    lane = lax.broadcasted_iota(jnp.int32, (rows, tokens), 1)
    own = lane == lax.broadcasted_iota(jnp.int32, (rows, tokens), 0) + index[2] * rows
    for x in range(NX):
        summed = jnp.zeros((rows, half), F32)
        square = jnp.zeros((8, tokens), F32)
        for y in range(NY):
            for source in (arrived, partner):
                both = source[x, y, 2 * rows : 4 * rows, :].astype(F32)
                summed = summed + jnp.where(index[3] == 0, both[:rows], both[rows:])
                square = square + source[x, y, 4 * rows :, :tokens].astype(F32)
        square = square[0:1, :] + square[1:2, :]
        square = jnp.sum(jnp.where(own, square, 0.0), axis=1, keepdims=True)
        summed = summed * lax.rsqrt(square / width + EPS)
        result = (silu(summed[:, : half // 2]) * summed[:, half // 2 :]).astype(BF)
        dense[x] = result
        away[x, NY, :, :size] = result
        away[x, NY, :, size:] = jnp.zeros((rows, block - size), BF)


def result_body(index, hidden, dense, away, down, out):
    rows, block = away.shape[2:]
    size = dense.shape[2]
    own_place = pl.multiple_of(block + index[3] * size, size)
    far_place = pl.multiple_of(block + (1 - index[3]) * size, size)
    for y in range(NY):
        place = pl.multiple_of((2 * y + index[3]) * block, block)
        part = jnp.dot(hidden[...], down[:, pl.ds(place, block)], preferred_element_type=F32)
        part = part.reshape(NX, rows, block) + away[:, y].astype(F32)
        out[:, y, :, :block] = part.astype(BF)
        out[:, y, :, pl.ds(own_place, size)] = dense[...]
        out[:, y, :, pl.ds(far_place, size)] = away[:, NY, :, :size]


def combine_body(index, arrived, route, d0, d1, d2, d3, mix, out):
    rows = arrived.shape[2]
    block = out.shape[2]
    tokens = NZ * rows
    results = []
    for x in range(NX):
        summed = arrived[x, 0, :, :block].astype(F32)
        for y in range(1, NY):
            summed = summed + arrived[x, y, :, :block].astype(F32)
        results.append(summed)
    results = jnp.concatenate(results, axis=0).astype(BF)
    routing = route[...]
    slot0, slot1 = slots_of(routing, index[0])
    place = lax.broadcasted_iota(jnp.int32, (NX * rows, tokens), 0)
    total = jnp.zeros((tokens, block), F32)
    for k in range(2):
        share = jnp.where(place == slot0, routing[2 + k : 3 + k, :], 0.0)
        share = jnp.where(place == slot1, routing[4 + k : 5 + k, :], share).astype(BF)
        total += lax.dot_general(
            share, results, (((0,), (0,)), ((), ())), preferred_element_type=F32
        )
    gate = 1.0 / (1.0 + jnp.exp(-mix[...]))
    total = total.reshape(NY, 2, rows, block)
    size = (arrived.shape[3] - block) // 2
    for core in range(2):
        lower = jnp.zeros((NY * rows, block // 2), F32)
        upper = jnp.zeros((NY * rows, block // 2), F32)
        lanes = slice(block + core * size, block + (core + 1) * size)
        for step, weight in enumerate((d0, d1, d2, d3)):
            x = wrapped(index[1] + step, NX)
            left = arrived[x, :, :, lanes].astype(F32).reshape(NY * rows, size).astype(BF)
            lower += jnp.dot(left, weight[:size, :], preferred_element_type=F32)
            upper += jnp.dot(left, weight[size:, :], preferred_element_type=F32)
        dense = gate * jnp.concatenate((lower, upper), axis=1)
        for y in range(NY):
            own = dense[y * rows : (y + 1) * rows] + total[y, core]
            out[2 * y + core] = own.astype(BF)


def final_body(index, arrived, middle, out):
    summed = arrived[0].astype(F32)
    for z in range(1, NZ):
        summed = summed + arrived[z].astype(F32)
    out[...] = (middle[...] + summed).astype(BF)


def per_device(
    tokens,
    delta_state,
    attn_gain,
    query_weight,
    key_weight,
    value_weight,
    decay_weight,
    beta_weight,
    decay_rate,
    head_gain,
    output_weight,
    ffn_gain,
    expert_ids,
    group_prob,
    expert_logit,
    expert_gate,
    expert_up,
    expert_down,
    dense_gate,
    dense_up,
    dense_down,
    dense_mix,
):
    rows, width = tokens.shape
    heads, size = delta_state.shape[1:3]
    cols = heads * size
    block = width // NT
    half = block // 2

    def shape(*dims, dtype=BF):
        return jax.ShapeDtypeStruct(dims, dtype)

    def own_block(ref, index):
        place = pl.multiple_of(index[2] * block, block)
        return ref.at[:, pl.ds(place, block)]

    first = (
        shape(NZ, rows + 8, block),
        shape(query_weight.shape[0], 3 * cols),
        shape(rows, 128, dtype=F32),
    )
    message, own_weights, factors = kernel(
        spread_body,
        tuple(pltpu.HBM(made.shape, made.dtype) for made in first),
        tokens,
        attn_gain[None],
        query_weight,
        key_weight,
        value_weight,
        decay_weight.T,
        beta_weight.T,
        decay_rate[None],
        expert_ids.T,
        group_prob[None],
        expert_logit.T,
        far=range(11),
        far_outs=range(3),
        scratch=[pltpu.VMEM(made.shape, made.dtype) for made in first]
        + [pltpu.SemaphoreType.DMA((3,))],
    )
    qkv_weights = from_neighbours(own_weights, "x")
    spread = exchange(message, "z")
    (packed,) = kernel(
        pack_body,
        (shape(block + dense_gate.shape[1] * 2, half),),
        message,
        dense_gate,
        dense_up,
        dense_down,
        plain=(0,),
        far=(1, 2, 3),
    )
    dense_weights = from_neighbours(packed, "x")
    (part,) = kernel(
        project_body,
        (shape(NZ, rows, 3 * cols),),
        spread,
        *qkv_weights,
        held=(1, 2, 3, 4),
        flops=2 * NZ * rows * block * 3 * cols,
    )
    arrived = exchange(part, "z")
    attn_part, keys, changes = kernel(
        recall_body,
        (
            shape(NT, rows, block),
            pltpu.HBM((rows, cols), F32),
            pltpu.HBM((rows, cols), F32),
        ),
        arrived,
        factors,
        delta_state,
        head_gain[None],
        output_weight,
        far=(1, 3, 4),
        flops=2 * rows * cols * width,
    )
    new_state, route_rows = kernel(
        update_body,
        (shape(*delta_state.shape, dtype=F32), pltpu.HBM((8, NZ * rows), F32)),
        keys,
        changes,
        factors,
        delta_state,
        spread,
        far=range(5),
        parts={4: ((NZ, 8, block), lambda ref, index: ref.at[:, rows:])},
        flops=10**8,
        limit=24,
    )
    arrived = exchange(attn_part, ("y", "c"))
    middle, message = kernel(
        middle_body,
        (shape(rows, block, dtype=F32), shape(NZ, rows, block)),
        arrived,
        tokens,
    )

    swap = [(0, 1), (1, 0)]
    arrived = exchange(message, "z")
    (message,) = kernel(
        dispatch_body,
        (shape(NX, NY, 4 * rows + 8, half),),
        arrived,
        ffn_gain[None],
        *dense_weights,
        route_rows,
        far=range(1, 7),
        parts={
            1: ((1, block), own_block),
            **{n: ((block, half), lambda ref, index: ref.at[:block]) for n in range(2, 6)},
        },
        flops=2 * NZ * rows * block * 2 * block,
    )
    sides = ("x", "y")
    arrived = exchange(message.reshape(NX * NY, -1, half), sides)
    partner = lax.ppermute(arrived, "c", swap).reshape(message.shape)
    away, hidden, dense = kernel(
        expert_body,
        (shape(NX, NY + 1, rows, block), shape(NX * rows, 128), shape(NX, rows, 128)),
        arrived.reshape(message.shape),
        partner,
        ffn_gain[None],
        expert_gate[0],
        expert_up[0],
        expert_down[0],
        far=(2,),
        flops=5 * NX * rows * width * 128,
    )
    (message,) = kernel(
        result_body,
        (shape(NX, NY, rows, block + 2 * 128),),
        hidden,
        dense,
        lax.ppermute(away, "c", swap),
        expert_down[0],
        flops=NX * rows * width * 128,
    )
    arrived = exchange(message.reshape(NX * NY, rows, -1), sides)
    (message,) = kernel(
        combine_body,
        (shape(NZ, rows, block),),
        arrived.reshape(message.shape),
        route_rows,
        *dense_weights,
        dense_mix[None],
        far=range(1, 7),
        parts={n: ((half, half), lambda ref, index: ref.at[block:]) for n in range(2, 6)},
        flops=2 * NZ * rows * block * block,
    )
    arrived = exchange(message, "z")
    (mixed_out,) = kernel(final_body, (shape(rows, block),), arrived, middle)
    return (mixed_out, new_state)


def solution(mesh):
    fine = Mesh(mesh.devices.reshape(NZ, NX, 4, 2), ("z", "x", "y", "c"))
    ep, tp = ("z", "x"), ("y", "c")

    return jax.shard_map(
        per_device,
        mesh=fine,
        in_specs=(
            P(ep, None),
            P(ep, tp, None, None),
            P(),
            P(ep, tp),
            P(ep, tp),
            P(ep, tp),
            P(),
            P(),
            P(tp),
            P(),
            P(tp, None),
            P(),
            P(ep, None),
            P(ep),
            P(ep, None),
            P(ep, None, tp),
            P(ep, None, tp),
            P(ep, tp, None),
            P(tp, ep),
            P(tp, ep),
            P(ep, tp),
            P(tp),
        ),
        out_specs=(P(ep, tp), P(ep, tp, None, None)),
        check_vma=False,
    )
```

```python
import jax
import jax.numpy as jnp
from jax import lax
from jax.experimental import pallas as pl
from jax.experimental.pallas import tpu as pltpu
from jax.sharding import Mesh, PartitionSpec as P

EPS = 1e-06
BF = jnp.bfloat16
F32 = jnp.float32
NZ, NX, NY, NT = 8, 4, 4, 8
CAP = 3
MIB = 1 << 20


def exchange(tiles, axes):
    return lax.all_to_all(tiles, axes, split_axis=0, concat_axis=0, tiled=True)


def from_neighbours(shard, axis):
    count = lax.axis_size(axis)
    parts = [shard]
    for step in range(1, count):
        pairs = [(source, (source - step) % count) for source in range(count)]
        parts.append(lax.ppermute(shard, axis, pairs))
    return parts


def unit_rows(values):
    return values * lax.rsqrt(jnp.sum(values * values, axis=-1, keepdims=True) + EPS)


def silu(values):
    return values / (1.0 + jnp.exp(-values))


class Late:
    def __init__(self, source, near, done):
        self.near = near
        self.copy = pltpu.make_async_copy(source, near, done)
        self.copy.start()
        self.waits = True

    def arrive(self):
        if self.waits:
            self.copy.wait()
            self.waits = False
        return self.near

    def __getitem__(self, where):
        return self.arrive()[where]

    @property
    def shape(self):
        return self.near.shape


def kernel(
    body, outs, *args, far=(), plain=(), held=(), parts=None, far_outs=(), scratch=(), flops=0, limit=16
):
    parts = parts or {}
    far, plain, held = tuple(far), tuple(plain), tuple(held)
    nears = [parts[n][0] if n in parts else args[n].shape for n in far]

    def run(*refs):
        sides = [lax.axis_index(name) for name in ("z", "x", "y", "c")]
        index = (sides[0], sides[1], sides[2] * 2 + sides[3], sides[3])
        refs = list(refs)
        ins, refs = refs[: len(args)], refs[len(args) :]
        dones = refs.pop() if far else None
        buffers = refs[len(refs) - len(far) :]
        refs = refs[: len(refs) - len(far)]
        for place, number in enumerate(far):
            source = ins[number]
            if number in parts:
                source = parts[number][1](source, index)
            ins[number] = Late(source, buffers[place], dones.at[place])
        body(index, *ins, *refs)
        for number in far:
            ins[number].arrive()

    specs = [
        pl.BlockSpec(memory_space=pltpu.HBM if number in far or number in plain else pltpu.VMEM)
        for number in range(len(args))
    ]
    out_specs = [
        pl.BlockSpec(memory_space=pltpu.HBM if number in far_outs else pltpu.VMEM)
        for number in range(len(outs))
    ]
    scratches = list(scratch) + [pltpu.VMEM(near, args[n].dtype) for n, near in zip(far, nears)]
    if far:
        scratches.append(pltpu.SemaphoreType.DMA((len(far),)))
    args = [
        pltpu.with_memory_space_constraint(arg, pltpu.HBM) if n in far + plain + held else arg
        for n, arg in enumerate(args)
    ]
    return pl.pallas_call(
        run,
        out_shape=outs,
        in_specs=specs,
        out_specs=out_specs,
        scratch_shapes=scratches,
        cost_estimate=pl.CostEstimate(flops=flops, bytes_accessed=0, transcendentals=0),
        compiler_params=pltpu.CompilerParams(vmem_limit_bytes=limit * MIB),
    )(*args)


def wrapped(value, count):
    return jnp.where(value >= count, value - count, value)


def weights_and_tokens(tokens, gain, query, key, value, out, weights):
    rows = tokens.shape[0]
    cols = query.shape[1]
    for place, weight in enumerate((query, key, value)):
        weights[:, place * cols : (place + 1) * cols] = weight[...]
    block = out.shape[2]
    for z in range(NZ):
        cols = slice(z * block, (z + 1) * block)
        out[z, :rows, :] = (tokens[:, cols].astype(F32) * gain[:, cols]).astype(BF)


def pack_body(index, after, gate, up, down, out):
    block, size = gate.shape
    half = down.shape[1] // 2
    out[:block, :size] = gate[...]
    out[:block, size:] = up[...]
    out[block : block + size, :] = down[:, :half]
    out[block + size :, :] = down[:, half:]


def turned(row, rows):
    shape = (rows, row.shape[1])
    same = lax.broadcasted_iota(jnp.int32, shape, 0) == lax.broadcasted_iota(jnp.int32, shape, 1)
    return jnp.sum(jnp.where(same, row, 0.0), axis=1, keepdims=True)


def spread_body(
    index, tokens, gain, query, key, value, decay_weight, beta_weight, rate, ids, prob, logit,
    far_out, far_weights, far_factors, out, weights, factors, stored,
):
    stores = [
        pltpu.make_async_copy(near, far, stored.at[place])
        for place, (near, far) in enumerate(
            ((weights, far_weights), (out, far_out), (factors, far_factors))
        )
    ]
    weights_and_tokens(tokens, gain, query, key, value, out, weights)
    stores[0].start()
    rows, width = tokens.shape
    block = out.shape[2]
    wide = tokens[...].astype(F32)
    row_scale = lax.rsqrt(jnp.sum(wide * wide, axis=1, keepdims=True) / width + EPS)
    gained = (wide * gain[...]).astype(BF)
    over_width = (((1,), (1,)), ((), ()))
    heads = rate.shape[1]
    factor_lane = lax.broadcasted_iota(jnp.int32, factors.shape, 1)
    table = jnp.where(factor_lane == 0, row_scale, 0.0)

    both = jnp.concatenate((decay_weight[...], beta_weight[...]), axis=0)
    product = lax.dot_general(gained, both, over_width, preferred_element_type=F32)
    product_lane = lax.broadcasted_iota(jnp.int32, product.shape, 1)

    def own_head(place):
        own = jnp.where(product_lane == place, product, 0.0)
        return jnp.sum(own, axis=1, keepdims=True) * row_scale

    for h in range(heads):
        place = index[2] * heads + h
        column = own_head(place)
        soft = jnp.maximum(column, 0.0) + jnp.log1p(jnp.exp(-jnp.abs(column)))
        table = jnp.where(factor_lane == 1 + h, jnp.exp(-rate[:, h : h + 1] * soft), table)
        column = own_head(decay_weight.shape[0] + place)
        table = jnp.where(factor_lane == 1 + heads + h, 1.0 / (1.0 + jnp.exp(-column)), table)
    factors[...] = table

    picks = [ids[k : k + 1, :].astype(F32) for k in range(2)]
    pick_cols = [turned(pick, rows) for pick in picks]
    shape = (rows, rows)
    earlier = lax.broadcasted_iota(jnp.int32, shape, 0) < lax.broadcasted_iota(jnp.int32, shape, 1)
    powers = [jnp.exp(logit[k : k + 1, :]) for k in range(2)]
    total = powers[0] + powers[1]
    lines = []
    for k in range(2):
        named = jnp.zeros(shape, F32)
        for column in pick_cols:
            named = named + jnp.where(earlier & (column == picks[k]), 1.0, 0.0)
        lines.append(picks[k] * CAP + jnp.sum(named, axis=0, keepdims=True))
    for k in range(2):
        route = prob[...] * powers[k] / total
        high = route.astype(BF).astype(F32)
        lines += [high, route - high]
    line = lax.broadcasted_iota(jnp.int32, (8, rows), 0)
    table = jnp.zeros((8, rows), F32)
    for number, values in enumerate(lines):
        table = jnp.where(line == number, values, table)
    shape = (rows, block)
    lane = lax.broadcasted_iota(jnp.int32, shape, 1)
    spot = lane == lax.broadcasted_iota(jnp.int32, shape, 0) + index[0] * rows
    spot = jnp.where(spot, 1.0, 0.0).astype(BF)
    meta = jnp.dot(table.astype(BF), spot, preferred_element_type=F32).astype(BF)
    for z in range(NZ):
        out[z, rows:, :] = meta
    stores[1].start()
    stores[2].start()
    for store in stores:
        store.wait()


def project_body(index, arrived, w0, w1, w2, w3, out):
    groups, rows, _ = out.shape
    tokens = groups * rows
    total = None
    for step, weight in enumerate((w0, w1, w2, w3)):
        size = weight.shape[0]
        place = pl.multiple_of(wrapped(index[1] + step, NX) * size, size)
        left = arrived[:, :rows, pl.ds(place, size)].astype(F32).reshape(tokens, size).astype(BF)
        part = jnp.dot(left, weight[...], preferred_element_type=F32)
        total = part if total is None else total + part
    out[...] = total.reshape(groups, rows, -1).astype(BF)


def recall_body(index, arrived, factors, state, head_gain, weight, out, keys, changes):
    rows, heads, size = state.shape[:3]
    cols = heads * size
    summed = arrived[0].astype(F32)
    for z in range(1, NZ):
        summed = summed + arrived[z].astype(F32)
    summed = summed * factors[:, 0:1]
    line = lax.broadcasted_iota(jnp.int32, (8, size), 0)
    head_rows = []
    for h in range(heads):
        own = slice(h * size, (h + 1) * size)
        query = unit_rows(summed[:, own]) * size ** (-0.5)
        key = unit_rows(summed[:, cols + h * size : cols + (h + 1) * size])
        value = summed[:, 2 * cols + h * size : 2 * cols + (h + 1) * size]
        groups = []
        for first in range(0, rows, 8):
            some = slice(first, first + 8)
            both = jnp.concatenate((key[some], query[some]), axis=0).astype(BF)
            recalled = jnp.zeros((8, size), F32)
            asked = jnp.zeros((8, size), F32)
            for b in range(0, 8, 2):
                pair = (state[first + b, h], state[first + b + 1, h])
                pair = jnp.concatenate(pair, axis=1).astype(BF)
                product = jnp.dot(both, pair, preferred_element_type=F32)
                for side in range(2):
                    lanes = slice(side * size, (side + 1) * size)
                    recalled = jnp.where(line == b + side, product[:8, lanes], recalled)
                    asked = jnp.where(line == b + side, product[8:, lanes], asked)
            groups.append((recalled, asked))
        recalled, asked = (jnp.concatenate(part, axis=0) for part in zip(*groups))
        fade = factors[:, 1 + h : 2 + h]
        gate = factors[:, 1 + heads + h : 2 + heads + h]
        change = gate * (value - fade * recalled)
        keys[:, own] = key
        changes[:, own] = change
        result = fade * asked + jnp.sum(query * key, axis=1, keepdims=True) * change
        mean_sq = jnp.mean(result * result, axis=1, keepdims=True)
        head_rows.append(result * lax.rsqrt(mean_sq + EPS) * head_gain[...])
    left = jnp.concatenate(head_rows, axis=1).astype(BF)
    block = out.shape[2]
    for t in range(NT):
        right = weight[:, t * block : (t + 1) * block]
        out[t] = jnp.dot(left, right, preferred_element_type=F32).astype(BF)


def update_body(index, keys, changes, factors, state, spread, new_state, route):
    rows, heads, size = state.shape[:3]
    tokens = route.shape[1]
    routing = spread[0, :, :tokens].astype(F32)
    for z in range(1, NZ):
        routing = routing + spread[z, :, :tokens].astype(F32)
    route[...] = routing
    line = lax.broadcasted_iota(jnp.int32, (rows, size), 0)
    line = jnp.concatenate((line, line, line), axis=0)
    for h in range(heads):
        own = slice(h * size, (h + 1) * size)
        key, change = keys[:, own], changes[:, own]
        key_high = key.astype(BF).astype(F32)
        high = change.astype(BF).astype(F32)
        left = jnp.concatenate((key_high, key - key_high, key_high), axis=0).T.astype(BF)
        right = jnp.concatenate((high, high, change - high), axis=0)
        for b in range(0, rows, 2):
            pair = [jnp.where(line == b + side, right, 0.0) for side in range(2)]
            pair = jnp.concatenate(pair, axis=1).astype(BF)
            product = jnp.dot(left, pair, preferred_element_type=F32)
            for side in range(2):
                fade = factors[b + side : b + side + 1, 1 + h : 2 + h]
                grown = product[:, side * size : (side + 1) * size]
                new_state[b + side, h] = fade * state[b + side, h] + grown


def middle_body(index, arrived, tokens, middle, out):
    block = middle.shape[1]
    summed = arrived[0].astype(F32)
    for t in range(1, NT):
        summed = summed + arrived[t].astype(F32)
    place = pl.multiple_of(index[2] * block, block)
    total = tokens[:, pl.ds(place, block)].astype(F32) + summed
    middle[...] = total
    narrow = total.astype(BF)
    for z in range(NZ):
        out[z] = narrow


def slots_of(route, zi):
    tokens = route.shape[1]
    lane = lax.broadcasted_iota(jnp.int32, (1, tokens), 1)
    source = jnp.zeros((1, tokens), jnp.int32)
    for z in range(1, NZ):
        source = source + jnp.where(lane >= z * (tokens // NZ), 1, 0)
    slots = []
    for k in range(2):
        code = route[k : k + 1, :].astype(jnp.int32) - zi * (NX * CAP)
        expert = jnp.zeros((1, tokens), jnp.int32)
        for x in range(1, NX):
            expert = expert + jnp.where(code >= x * CAP, 1, 0)
        slot = expert * (NZ * CAP) + source * CAP + (code - expert * CAP)
        slots.append(jnp.where((code >= 0) & (code < NX * CAP), slot, -1))
    return slots


def dispatch_body(index, arrived, gain, g0, g1, g2, g3, route, out):
    rows = arrived.shape[1]
    tokens = NZ * rows
    block = arrived.shape[2]
    half = block // 2
    wide = arrived[...].astype(F32).reshape(tokens, block)
    narrow = wide.astype(BF)
    routing = route[...]
    slot0, slot1 = slots_of(routing, index[0])
    place = lax.broadcasted_iota(jnp.int32, (NX * rows, tokens), 0)
    picks = jnp.where((place == slot0) | (place == slot1), 1.0, 0.0).astype(BF)
    chosen = jnp.dot(picks, narrow, preferred_element_type=F32).astype(BF)
    square = wide * wide
    high = square.astype(BF)
    ones = jnp.ones((8, block), BF)
    over_block = (((1,), (1,)), ((), ()))
    square = sum(
        lax.dot_general(ones, part, over_block, preferred_element_type=F32)
        for part in (high, (square - high.astype(F32)).astype(BF))
    )
    high = square.astype(BF).astype(F32)
    first = lax.broadcasted_iota(jnp.int32, square.shape, 0) == 0
    square = jnp.where(first, high, square - high).astype(BF)
    for x in range(NX):
        own = chosen[x * rows : (x + 1) * rows]
        for y in range(NY):
            out[x, y, :rows, :] = own[:, :half]
            out[x, y, rows : 2 * rows, :] = own[:, half:]
            out[x, y, 4 * rows :, :tokens] = square
            out[x, y, 4 * rows :, tokens:] = jnp.zeros((8, half - tokens), BF)
    scaled = (wide * gain[...]).astype(BF)
    for step, weight in enumerate((g0, g1, g2, g3)):
        part = jnp.dot(scaled, weight[...], preferred_element_type=F32)
        x = wrapped(index[1] + step, NX)
        out[x, :, 2 * rows : 4 * rows, :] = part.reshape(NY, 2 * rows, half).astype(BF)


def expert_body(index, arrived, partner, gain, gate, up, down, away, hidden, dense):
    rows, block = away.shape[2:]
    size = gate.shape[1]
    half = block // 2
    width = gate.shape[0]
    slots = NX * rows
    squares = jnp.zeros((slots, half), F32)
    gate_sum = jnp.zeros((slots, gate.shape[1]), F32)
    up_sum = jnp.zeros((slots, gate.shape[1]), F32)
    for y in range(NY):
        for source, core in ((arrived, index[3]), (partner, 1 - index[3])):
            for part in range(2):
                wide = source[:, y, part * rows : (part + 1) * rows, :].astype(F32)
                wide = wide.reshape(slots, half)
                squares = squares + wide * wide
                place = pl.multiple_of((2 * y + core) * block + part * half, half)
                left = (wide * gain[:, pl.ds(place, half)]).astype(BF)
                own = pl.ds(place, half)
                gate_sum += jnp.dot(left, gate[own, :], preferred_element_type=F32)
                up_sum += jnp.dot(left, up[own, :], preferred_element_type=F32)
    scale = lax.rsqrt(jnp.sum(squares, axis=1, keepdims=True) / width + EPS)
    result = (silu(gate_sum * scale) * (up_sum * scale)).astype(BF)
    hidden[...] = result
    for y in range(NY):
        place = pl.multiple_of((2 * y + 1 - index[3]) * block, block)
        part = jnp.dot(result, down[:, pl.ds(place, block)], preferred_element_type=F32)
        away[:, y] = part.reshape(NX, rows, block).astype(BF)
    tokens = NZ * rows
    lane = lax.broadcasted_iota(jnp.int32, (rows, tokens), 1)
    own = lane == lax.broadcasted_iota(jnp.int32, (rows, tokens), 0) + index[2] * rows
    for x in range(NX):
        summed = jnp.zeros((rows, half), F32)
        square = jnp.zeros((8, tokens), F32)
        for y in range(NY):
            for source in (arrived, partner):
                both = source[x, y, 2 * rows : 4 * rows, :].astype(F32)
                summed = summed + jnp.where(index[3] == 0, both[:rows], both[rows:])
                square = square + source[x, y, 4 * rows :, :tokens].astype(F32)
        square = square[0:1, :] + square[1:2, :]
        square = jnp.sum(jnp.where(own, square, 0.0), axis=1, keepdims=True)
        summed = summed * lax.rsqrt(square / width + EPS)
        result = (silu(summed[:, : half // 2]) * summed[:, half // 2 :]).astype(BF)
        dense[x] = result
        away[x, NY, :, :size] = result
        away[x, NY, :, size:] = jnp.zeros((rows, block - size), BF)


def result_body(index, hidden, dense, away, down, out):
    rows, block = away.shape[2:]
    size = dense.shape[2]
    own_place = pl.multiple_of(block + index[3] * size, size)
    far_place = pl.multiple_of(block + (1 - index[3]) * size, size)
    for y in range(NY):
        place = pl.multiple_of((2 * y + index[3]) * block, block)
        part = jnp.dot(hidden[...], down[:, pl.ds(place, block)], preferred_element_type=F32)
        part = part.reshape(NX, rows, block) + away[:, y].astype(F32)
        out[:, y, :, :block] = part.astype(BF)
        out[:, y, :, pl.ds(own_place, size)] = dense[...]
        out[:, y, :, pl.ds(far_place, size)] = away[:, NY, :, :size]


def combine_body(index, arrived, route, d0, d1, d2, d3, mix, out):
    rows = arrived.shape[2]
    block = out.shape[2]
    tokens = NZ * rows
    results = []
    for x in range(NX):
        summed = arrived[x, 0, :, :block].astype(F32)
        for y in range(1, NY):
            summed = summed + arrived[x, y, :, :block].astype(F32)
        results.append(summed)
    results = jnp.concatenate(results, axis=0).astype(BF)
    routing = route[...]
    slot0, slot1 = slots_of(routing, index[0])
    place = lax.broadcasted_iota(jnp.int32, (NX * rows, tokens), 0)
    total = jnp.zeros((tokens, block), F32)
    for k in range(2):
        share = jnp.where(place == slot0, routing[2 + k : 3 + k, :], 0.0)
        share = jnp.where(place == slot1, routing[4 + k : 5 + k, :], share).astype(BF)
        total += lax.dot_general(
            share, results, (((0,), (0,)), ((), ())), preferred_element_type=F32
        )
    gate = 1.0 / (1.0 + jnp.exp(-mix[...]))
    total = total.reshape(NY, 2, rows, block)
    size = (arrived.shape[3] - block) // 2
    for core in range(2):
        lower = jnp.zeros((NY * rows, block // 2), F32)
        upper = jnp.zeros((NY * rows, block // 2), F32)
        lanes = slice(block + core * size, block + (core + 1) * size)
        for step, weight in enumerate((d0, d1, d2, d3)):
            x = wrapped(index[1] + step, NX)
            left = arrived[x, :, :, lanes].astype(F32).reshape(NY * rows, size).astype(BF)
            lower += jnp.dot(left, weight[:size, :], preferred_element_type=F32)
            upper += jnp.dot(left, weight[size:, :], preferred_element_type=F32)
        dense = gate * jnp.concatenate((lower, upper), axis=1)
        for y in range(NY):
            own = dense[y * rows : (y + 1) * rows] + total[y, core]
            out[2 * y + core] = own.astype(BF)


def final_body(index, arrived, middle, out):
    summed = arrived[0].astype(F32)
    for z in range(1, NZ):
        summed = summed + arrived[z].astype(F32)
    out[...] = (middle[...] + summed).astype(BF)


def per_device(
    tokens,
    delta_state,
    attn_gain,
    query_weight,
    key_weight,
    value_weight,
    decay_weight,
    beta_weight,
    decay_rate,
    head_gain,
    output_weight,
    ffn_gain,
    expert_ids,
    group_prob,
    expert_logit,
    expert_gate,
    expert_up,
    expert_down,
    dense_gate,
    dense_up,
    dense_down,
    dense_mix,
):
    rows, width = tokens.shape
    heads, size = delta_state.shape[1:3]
    cols = heads * size
    block = width // NT
    half = block // 2

    def shape(*dims, dtype=BF):
        return jax.ShapeDtypeStruct(dims, dtype)

    def own_block(ref, index):
        place = pl.multiple_of(index[2] * block, block)
        return ref.at[:, pl.ds(place, block)]

    first = (
        shape(NZ, rows + 8, block),
        shape(query_weight.shape[0], 3 * cols),
        shape(rows, 128, dtype=F32),
    )
    message, own_weights, factors = kernel(
        spread_body,
        tuple(pltpu.HBM(made.shape, made.dtype) for made in first),
        tokens,
        attn_gain[None],
        query_weight,
        key_weight,
        value_weight,
        decay_weight.T,
        beta_weight.T,
        decay_rate[None],
        expert_ids.T,
        group_prob[None],
        expert_logit.T,
        far=range(11),
        far_outs=range(3),
        scratch=[pltpu.VMEM(made.shape, made.dtype) for made in first]
        + [pltpu.SemaphoreType.DMA((3,))],
    )
    qkv_weights = from_neighbours(own_weights, "x")
    spread = exchange(message, "z")
    (packed,) = kernel(
        pack_body,
        (shape(block + dense_gate.shape[1] * 2, half),),
        message,
        dense_gate,
        dense_up,
        dense_down,
        plain=(0,),
        far=(1, 2, 3),
    )
    dense_weights = from_neighbours(packed, "x")
    (part,) = kernel(
        project_body,
        (shape(NZ, rows, 3 * cols),),
        spread,
        *qkv_weights,
        held=(1, 2, 3, 4),
        flops=2 * NZ * rows * block * 3 * cols,
    )
    arrived = exchange(part, "z")
    attn_part, keys, changes = kernel(
        recall_body,
        (
            shape(NT, rows, block),
            pltpu.HBM((rows, cols), F32),
            pltpu.HBM((rows, cols), F32),
        ),
        arrived,
        factors,
        delta_state,
        head_gain[None],
        output_weight,
        far=(1, 3, 4),
        flops=2 * rows * cols * width,
    )
    new_state, route_rows = kernel(
        update_body,
        (shape(*delta_state.shape, dtype=F32), pltpu.HBM((8, NZ * rows), F32)),
        keys,
        changes,
        factors,
        delta_state,
        spread,
        far=range(5),
        parts={4: ((NZ, 8, block), lambda ref, index: ref.at[:, rows:])},
        flops=10**8,
        limit=24,
    )
    arrived = exchange(attn_part, ("y", "c"))
    middle, message = kernel(
        middle_body,
        (shape(rows, block, dtype=F32), shape(NZ, rows, block)),
        arrived,
        tokens,
    )

    swap = [(0, 1), (1, 0)]
    arrived = exchange(message, "z")
    (message,) = kernel(
        dispatch_body,
        (shape(NX, NY, 4 * rows + 8, half),),
        arrived,
        ffn_gain[None],
        *dense_weights,
        route_rows,
        far=range(1, 7),
        parts={
            1: ((1, block), own_block),
            **{n: ((block, half), lambda ref, index: ref.at[:block]) for n in range(2, 6)},
        },
        flops=2 * NZ * rows * block * 2 * block,
    )
    sides = ("x", "y")
    arrived = exchange(message.reshape(NX * NY, -1, half), sides)
    partner = lax.ppermute(arrived, "c", swap).reshape(message.shape)
    away, hidden, dense = kernel(
        expert_body,
        (shape(NX, NY + 1, rows, block), shape(NX * rows, 128), shape(NX, rows, 128)),
        arrived.reshape(message.shape),
        partner,
        ffn_gain[None],
        expert_gate[0],
        expert_up[0],
        expert_down[0],
        far=(2,),
        flops=5 * NX * rows * width * 128,
    )
    (message,) = kernel(
        result_body,
        (shape(NX, NY, rows, block + 2 * 128),),
        hidden,
        dense,
        lax.ppermute(away, "c", swap),
        expert_down[0],
        flops=NX * rows * width * 128,
    )
    arrived = exchange(message.reshape(NX * NY, rows, -1), sides)
    (message,) = kernel(
        combine_body,
        (shape(NZ, rows, block),),
        arrived.reshape(message.shape),
        route_rows,
        *dense_weights,
        dense_mix[None],
        far=range(1, 7),
        parts={n: ((half, half), lambda ref, index: ref.at[block:]) for n in range(2, 6)},
        flops=2 * NZ * rows * block * block,
    )
    arrived = exchange(message, "z")
    (mixed_out,) = kernel(final_body, (shape(rows, block),), arrived, middle)
    return (mixed_out, new_state)


def solution(mesh):
    fine = Mesh(mesh.devices.reshape(NZ, NX, 4, 2), ("z", "x", "y", "c"))
    ep, tp = ("z", "x"), ("y", "c")

    return jax.shard_map(
        per_device,
        mesh=fine,
        in_specs=(
            P(ep, None),
            P(ep, tp, None, None),
            P(),
            P(ep, tp),
            P(ep, tp),
            P(ep, tp),
            P(),
            P(),
            P(tp),
            P(),
            P(tp, None),
            P(),
            P(ep, None),
            P(ep),
            P(ep, None),
            P(ep, None, tp),
            P(ep, None, tp),
            P(ep, tp, None),
            P(tp, ep),
            P(tp, ep),
            P(ep, tp),
            P(tp),
        ),
        out_specs=(P(ep, tp), P(ep, tp, None, None)),
        check_vma=False,
    )
```
